32 devices in a mesh: sp: 4 (over z), fs: 4 (over y, x), tp: 2 (over core).
Axes of the slice: x: 2, y: 2, z: 4, core: 2. Of those that a mesh axis runs over, the one named last changes fastest.
Arguments:
- inputs: bfloat16 [4, 1024, 4096], P('fs', 'sp', 'tp'), may hold values from -6 to 6
- norm_gain: float32 [4096], replicated, may hold values from 0.1 to 1.9
- conv_in_a: bfloat16 [4096, 1024], P(('sp', 'fs'), 'tp'), may hold values from -0.09375 to 0.09375
- conv_in_b: bfloat16 [4096, 1024], P(('sp', 'fs'), 'tp'), may hold values from -0.09375 to 0.09375
- query_w: bfloat16 [4096, 512], P(('sp', 'fs'), 'tp'), may hold values from -0.09375 to 0.09375
- key_w: bfloat16 [4096, 512], P(('sp', 'fs'), 'tp'), may hold values from -0.09375 to 0.09375
- value_w: bfloat16 [4096, 1024], P(('sp', 'fs'), 'tp'), may hold values from -0.09375 to 0.09375
- out_gate_w: bfloat16 [4096, 1024], P(('sp', 'fs'), 'tp'), may hold values from -0.09375 to 0.09375
- pointwise_w: bfloat16 [4096, 1024], P(('sp', 'fs'), 'tp'), may hold values from -0.1875 to 0.1875
- gla_out_w: bfloat16 [4096, 1024], P(('sp', 'fs'), 'tp'), may hold values from -0.1875 to 0.1875
- forget_first_factor: bfloat16 [4096, 64], replicated, may hold values from -0.09375 to 0.09375
- decay_w: bfloat16 [64, 512], replicated, may hold values from -0.75 to 0.75
- decay_bias: float32 [512], replicated, as said below
- decay_extra: float32 [4, 1024, 512], P('fs', 'sp', 'tp'), may hold values from -2.2 to 0, as said below
- conv_kernel: float32 [31, 1024], replicated, may hold values from -7 to 7
- conv_gain: float32 [1024], replicated, may hold values from 0.1 to 1.9
- head_gain: float32 [64], replicated, may hold values from 0.1 to 1.9
Outputs:
- mixed: bfloat16 [4, 1024, 4096], P('fs', 'sp', 'tp')
The draws below stay inside these ranges and needn't reach their ends.
Inputs may be any that keep to these rules, and one draw needn't show every extreme that they name: decay_bias is positive. decay_extra is never positive.
All inputs are finite; a program needn't handle non-finite values.
Results may differ from the reference program's by a relative error of at most 0.015.
Values may be sent and summed in bfloat16 or wider, within the bound.
A program may use at most 192 MiB of HBM per device.

```python
import math
import jax
import jax.numpy as jnp
from jax import lax

D = 4096
C = 1024
GLA_HEADS = 16
DK = 32
DV = 64
RANK = 64
CONV_WIDTH = 31
BLOCK = 64
TOK_DEV = 256
SEQS = 4
LENGTH = 1024
HK = 512
HV = 1024
N_TP = 2


def draw_decay_bias(key, part):
    first_key = jax.random.fold_in(key, 11)
    second_key = jax.random.fold_in(key, 12)
    third_key = jax.random.fold_in(key, 13)
    slow_share = 0.5
    slow_heads = jax.random.bernoulli(first_key, slow_share, (GLA_HEADS,))
    slow_channels = jnp.repeat(slow_heads, DK)
    slow_value = math.log(LENGTH / 16.0) + jax.random.uniform(second_key, (HK,), jnp.float32, 1.0, 1.5)
    fast_value = jax.random.uniform(third_key, (HK,), jnp.float32, 0.5, 1.7)
    return jnp.where(slow_channels, slow_value, fast_value).astype(jnp.float32)


def draw_decay_extra(key, part):
    rate_key = jax.random.fold_in(key, 21)
    spot_key = jax.random.fold_in(key, 22)
    depth_key = jax.random.fold_in(key, 23)
    segment_count = LENGTH // TOK_DEV
    log_rate = jax.random.uniform(rate_key, (SEQS, segment_count, 1, HK), jnp.float32, math.log(0.15), math.log(0.6))
    forget_factors = jnp.broadcast_to(jnp.exp(log_rate) / LENGTH, (SEQS, segment_count, TOK_DEV, HK)).reshape(SEQS, LENGTH, HK)
    spots = jax.random.randint(spot_key, (SEQS, 3), 0, LENGTH)
    tier_heights = jax.random.uniform(depth_key, (SEQS, 3, HK), jnp.float32, math.log(0.5), math.log(0.8))
    agreement_tally = (jnp.arange(LENGTH, dtype=jnp.int32)[None, :, None] == spots[:, None, :]).astype(jnp.float32)
    spurt_sizes_list = jnp.einsum('dqz,dzc->dqc', agreement_tally, tier_heights)
    return (spurt_sizes_list - forget_factors).astype(jnp.float32)


def draw_conv_kernel(key, part):
    base_key = jax.random.fold_in(key, 31)
    base = jax.random.truncated_normal(base_key, -4.0, 4.0, (CONV_WIDTH, C), jnp.float32) * CONV_WIDTH ** (-0.5)
    rising = 3.0 ** (jnp.arange(C, dtype=jnp.float32) / (C - 1))
    return (base * rising).astype(jnp.float32)


def shard_levels(own_key, dims, shards, low, largest):
    level, own = 1.0, jax.random.fold_in(own_key, 6)
    for axis_at, parts in shards:
        heights = jnp.exp(jax.random.uniform(jax.random.fold_in(own, axis_at), (parts,), jnp.float32, low / len(shards), largest / len(shards)))
        level = level * jnp.repeat(heights, dims[axis_at] // parts).reshape([-1 if axis == axis_at else 1 for axis in range(len(dims))])
    return level


def normal_values(rng, extent, scale, limit, split=(), held_as=jnp.bfloat16):
    result = scale * jax.random.normal(rng, extent, jnp.float32)
    if split:
        result = result * shard_levels(rng, extent, split, -0.22, 0.18)
    return jnp.clip(result, -limit, limit).astype(held_as)


def setup_inputs(seed: int = 0) -> dict:
    key_of = jax.random.split(jax.random.key(seed), 18)
    inputs = normal_values(key_of[0], (SEQS, LENGTH, D), 1.0, 6.0, ((0, 4), (1, 4), (2, 2)))
    norm_gain = jnp.clip(1.0 + 0.18 * jax.random.normal(key_of[1], (D,), jnp.float32), 0.1, 1.9)
    conv_in_a = normal_values(key_of[2], (D, C), D ** -0.5, 0.09375, ((0, 16), (1, 2)))
    conv_in_b = normal_values(key_of[3], (D, C), D ** -0.5, 0.09375, ((0, 16), (1, 2)))
    query_w = normal_values(key_of[4], (D, HK), D ** -0.5, 0.09375, ((0, 16), (1, 2)))
    key_w = normal_values(key_of[5], (D, HK), D ** -0.5, 0.09375, ((0, 16), (1, 2)))
    value_w = normal_values(key_of[6], (D, HV), D ** -0.5, 0.09375, ((0, 16), (1, 2)))
    out_gate_w = normal_values(key_of[7], (D, HV), D ** -0.5, 0.09375, ((0, 16), (1, 2)))
    pointwise_w = normal_values(key_of[8], (D, C), C ** -0.5, 0.1875, ((0, 16), (1, 2)))
    gla_out_w = normal_values(key_of[9], (D, HV), HV ** -0.5, 0.1875, ((0, 16), (1, 2)))
    forget_first_factor = normal_values(key_of[10], (D, RANK), D ** -0.5, 0.09375)
    decay_w = normal_values(key_of[11], (RANK, HK), RANK ** -0.5, 0.75)
    decay_bias = draw_decay_bias(jax.random.fold_in(key_of[17], 71), 0)
    decay_extra = draw_decay_extra(jax.random.fold_in(key_of[17], 71), 0)
    conv_kernel = draw_conv_kernel(jax.random.fold_in(key_of[17], 71), 0)
    conv_gain = jnp.clip(1.0 + 0.18 * jax.random.normal(key_of[15], (C,), jnp.float32), 0.1, 1.9)
    head_gain = jnp.clip(1.0 + 0.18 * jax.random.normal(key_of[16], (DV,), jnp.float32), 0.1, 1.9)
    return dict(inputs=inputs, norm_gain=norm_gain, conv_in_a=conv_in_a, conv_in_b=conv_in_b, query_w=query_w, key_w=key_w, value_w=value_w, out_gate_w=out_gate_w, pointwise_w=pointwise_w, gla_out_w=gla_out_w, forget_first_factor=forget_first_factor, decay_w=decay_w, decay_bias=decay_bias, decay_extra=decay_extra, conv_kernel=conv_kernel, conv_gain=conv_gain, head_gain=head_gain)


def reference(inputs, norm_gain, conv_in_a, conv_in_b, query_w, key_w, value_w, out_gate_w, pointwise_w, gla_out_w, forget_first_factor, decay_w, decay_bias, decay_extra, conv_kernel, conv_gain, head_gain):
    position_count = SEQS * LENGTH
    flat_rows = inputs.reshape(position_count, D).astype(jnp.float32)
    row_scale = lax.rsqrt(lax.optimization_barrier(jnp.mean(flat_rows * flat_rows, axis=1, keepdims=True)) + 1e-06)
    scaled = (flat_rows * norm_gain).astype(jnp.bfloat16)

    def project(weight):
        product = jnp.dot(scaled, weight, preferred_element_type=jnp.float32)
        return (product * row_scale).astype(jnp.bfloat16)
    conv_a, conv_b, queries, keys, values, out_gate, low_rank = [project(weight) for weight in (conv_in_a, conv_in_b, query_w, key_w, value_w, out_gate_w, forget_first_factor)]
    gated = (conv_a.astype(jnp.float32) * jax.nn.sigmoid(conv_b.astype(jnp.float32))).astype(jnp.bfloat16)
    padded = jnp.pad(gated.reshape(SEQS, LENGTH, C).astype(jnp.float32), ((0, 0), (CONV_WIDTH - 1, 0), (0, 0)))
    convolved = jnp.zeros((SEQS, LENGTH, C), jnp.float32)
    for offset in range(CONV_WIDTH):
        convolved = convolved + conv_kernel[offset] * padded[:, offset:offset + LENGTH]
    average = lax.optimization_barrier(jnp.mean(convolved, axis=-1, keepdims=True))
    spread_squared_mean = lax.optimization_barrier(jnp.mean(jnp.square(convolved - average), axis=-1, keepdims=True))
    normed = (convolved - average) * lax.rsqrt(spread_squared_mean + 1e-05) * conv_gain
    conv_act = jax.nn.silu(normed).astype(jnp.bfloat16).reshape(position_count, C)
    pre_decay = jnp.dot(low_rank, decay_w, preferred_element_type=jnp.float32) + decay_bias
    log_decay = jax.nn.log_sigmoid(pre_decay) / 16.0 + decay_extra.reshape(position_count, HK)
    block_count = LENGTH // BLOCK

    def split_blocks(array_operand, width):
        return array_operand.reshape(SEQS, block_count, BLOCK, GLA_HEADS, width).transpose(1, 0, 3, 2, 4)
    q_blocks = split_blocks(queries.astype(jnp.float32), DK) * DK ** (-0.5)
    k_blocks = split_blocks(keys.astype(jnp.float32), DK)
    v_blocks = split_blocks(values.astype(jnp.float32), DV)
    cumulative_all = jnp.cumsum(split_blocks(log_decay, DK), axis=3)
    causal = jnp.tril(jnp.ones((BLOCK, BLOCK), dtype=bool))
    highest = lax.Precision.HIGHEST

    def advance(state, block_inputs):
        query_block, key_block, value_block, prefix_running_sum = block_inputs
        spread = prefix_running_sum[..., :, None, :] - prefix_running_sum[..., None, :, :]
        weights_in = jnp.exp(jnp.where(causal[:, :, None], spread, -jnp.inf))
        scores = jnp.einsum('shid,shjd,shijd->shij', query_block, key_block, weights_in, precision=highest)
        inner = jnp.einsum('shij,shjv->shiv', scores, value_block, precision=highest)
        outer = jnp.einsum('shid,shdv->shiv', query_block * jnp.exp(prefix_running_sum), state, precision=highest)
        last_total = prefix_running_sum[..., -1, :]
        added_share_term = jnp.einsum('shjd,shjv->shdv', key_block * jnp.exp(last_total[..., None, :] - prefix_running_sum), value_block, precision=highest)
        return (jnp.exp(last_total)[..., None] * state + added_share_term, inner + outer)
    start_state = jnp.zeros((SEQS, GLA_HEADS, DK, DV), jnp.float32)
    _, outputs = lax.scan(advance, start_state, (q_blocks, k_blocks, v_blocks, cumulative_all))
    outputs = outputs.transpose(1, 0, 3, 2, 4).reshape(position_count, GLA_HEADS, DV)
    normed_heads = outputs * lax.rsqrt(lax.optimization_barrier(jnp.mean(outputs * outputs, axis=-1, keepdims=True)) + 1e-06) * head_gain
    gla_act = (normed_heads.reshape(position_count, HV) * jax.nn.silu(out_gate.astype(jnp.float32))).astype(jnp.bfloat16)
    conv_group = C // N_TP
    head_group = HV // N_TP
    total = flat_rows
    for group_index in range(N_TP):
        convolution_window = slice(group_index * conv_group, (group_index + 1) * conv_group)
        head_slice = slice(group_index * head_group, (group_index + 1) * head_group)
        value_fraction = jnp.dot(conv_act[:, convolution_window], pointwise_w[:, convolution_window].T, preferred_element_type=jnp.float32)
        value_fraction = value_fraction + jnp.dot(gla_act[:, head_slice], gla_out_w[:, head_slice].T, preferred_element_type=jnp.float32)
        total = total + lax.optimization_barrier(value_fraction.astype(jnp.bfloat16)).astype(jnp.float32)
    return total.astype(jnp.bfloat16).reshape(SEQS, LENGTH, D)
```

```python
import jax
import jax.numpy as jnp
from jax import lax
from jax.experimental import pallas as pl
from jax.experimental.pallas import tpu as pltpu
from jax.sharding import PartitionSpec as P


DK = 32
DV = 64
SUB = 16
BLOCK = 64


ROOT = 5
OUT_ITEMS = 2
CHUNK = 128
MESH_IDS = pl.DeviceIdType.MESH


def fused_kernel(
    x_hbm, wa, wb, wq, wk, wv, wg, pw, go, dex_hbm,
    ng_ref, ff_ref, dw_ref, db_ref, ck_ref, cg_ref, hg_ref,
    o_ref,
    xbuf, xs, rs, wbuf, qraw, kraw, qkst, wobuf, debuf, ext, conv, stats, comb, actbuf,
    qkb, vb, ld, raw, qseg, state_ref, base_ref, sfin, tots, stbuf, sin_ref,
    pbuf, prcv, osum, rbuf,
    xl, xsx, xsy, xff, xsd, xi, xd, al, ass, ar, zsu, zsd, zr, ol, dl, dsn, dr,
    hs, hr, tsn, tr, vsn, vr, csn, cr, gsn, gr, psn, pr, osn, orc,
):
    f32, bf16 = jnp.float32, jnp.bfloat16
    z, f, c = lax.axis_index("sp"), lax.axis_index("fs"), lax.axis_index("tp")
    nz, nf, nc = lax.axis_size("sp"), lax.axis_size("fs"), lax.axis_size("tp")
    tok, feat = x_hbm.shape
    half = tok // 2
    rows_w = wa.shape[0]
    layer_rows = nf * rows_w
    cw = wa.shape[1] // nf
    kw = wq.shape[1] // nf
    vw = wv.shape[1] // nf
    total = nf * tok
    kin = wbuf.shape[0]
    pwc = pw.shape[1]
    channels = nc * nf * cw
    other = 1 - c
    xn = f + 1 - 2 * lax.rem(f, 2)
    yn = f + 2 - 4 * (f // 2)
    dg = nf - 1 - f
    peers = (xn, yn, dg)

    def remote(src, dst, send, recv, dev):
        return pltpu.make_async_remote_copy(
            src_ref=src, dst_ref=dst, send_sem=send, recv_sem=recv,
            device_id=dev, device_id_type=MESH_IDS,
        )

    def arrived(dst, recv):
        remote(dst, dst, recv, recv, (z, f, other)).wait_recv()

    def lanes(at, width):
        return pl.ds(pl.multiple_of(at * width, width), width)

    def xr(seq, h):
        row = pl.ds(pl.multiple_of(seq * tok + h * half, half), half)
        return xbuf.at[row, lanes(c, feat)]

    def xr_other(seq, h):
        row = pl.ds(pl.multiple_of(seq * tok + h * half, half), half)
        return xbuf.at[row, lanes(other, feat)]

    def item(i, b):
        if i < ROOT:
            row = pl.ds(pl.multiple_of(b * layer_rows, layer_rows), layer_rows)
            return wbuf.at[row, pl.ds(i * cw, cw)]
        return wobuf.at[b, :, pl.ds((i - ROOT) * pwc, pwc)]

    def up(i, b):
        return remote(item(i, b), item(i, b), zsu.at[i, b], zr.at[i, b], (z + 1, f, c))

    def down(i, b):
        return remote(item(i, b), item(i, b), zsd.at[i, b], zr.at[i, b], (z - 1, f, c))

    items = ROOT + OUT_ITEMS
    sources = {0: wa, 1: wb, 3: wv, 4: wg}
    my_rows = pl.ds(pl.multiple_of((z * nf + f) * rows_w, rows_w), rows_w)

    own_x = [
        pltpu.make_async_copy(x_hbm.at[pl.ds(h * half, half), :], xr(f, h), xl.at[h])
        for h in range(2)
    ]
    qk_load = [
        pltpu.make_async_copy(wq, qraw, ol.at[2]),
        pltpu.make_async_copy(wk, kraw, ol.at[3]),
    ]
    own_w = {
        g: pltpu.make_async_copy(
            w.at[:, lanes(f, cw)], wbuf.at[my_rows, pl.ds(g * cw, cw)], al.at[g]
        )
        for g, w in sources.items()
    }
    own_o = [
        pltpu.make_async_copy(pw, item(ROOT, z), ol.at[0]),
        pltpu.make_async_copy(go, item(ROOT + 1, z), ol.at[1]),
    ]
    own_d = pltpu.make_async_copy(dex_hbm.at[:, lanes(f // 2, 2 * kw)], debuf.at[f], dl)
    for copy in qk_load:
        copy.start()
    for g in sources:
        own_w[g].start()
    for copy in own_x + own_o + [own_d]:
        copy.start()

    barrier = pltpu.get_barrier_semaphore()
    me = f * nc + c
    group = nf * nc
    for k in range(1, group):
        t = lax.rem(me + k, group)
        pl.semaphore_signal(barrier, inc=1, device_id=(z, t // nc, lax.rem(t, nc)), device_id_type=MESH_IDS)
    for k in range(1, nz):
        pl.semaphore_signal(barrier, inc=1, device_id=(lax.rem(z + k, nz), f, c), device_id_type=MESH_IDS)
    pl.semaphore_wait(barrier, group - 1 + nz - 1)

    def exchange(g):
        out = []
        for n, p in enumerate(peers):
            src = qkst.at[p] if g == 2 else sources[g].at[:, lanes(p, cw)]
            dst = wbuf.at[my_rows, pl.ds(g * cw, cw)]
            out.append(remote(src, dst, ass.at[g, n], ar.at[g, f], (z, p, c)))
        return out

    x_to_x = [
        remote(x_hbm.at[pl.ds(h * half, half), :], xr(f, h), xsx.at[h], xi.at[f, h], (z, xn, c))
        for h in range(2)
    ]
    x_to_y = [
        remote(x_hbm.at[pl.ds(h * half, half), :], xr(f, h), xsy.at[h], xi.at[f, h], (z, yn, c))
        for h in range(2)
    ]
    x_over = [
        remote(x_hbm.at[pl.ds(h * half, half), :], xr(f, h), xsd.at[f, h], xd.at[f, h], (z, f, other))
        for h in range(2)
    ]

    def over(seq, h):
        return remote(xr(seq, h), xr(seq, h), xsd.at[seq, h], xd.at[seq, h], (z, f, other))

    decay_out = [
        remote(
            dex_hbm.at[:, lanes(p // 2, 2 * kw)], debuf.at[f], dsn.at[n], dr.at[f], (z, p, c)
        )
        for n, p in enumerate(peers)
    ]

    sends = []

    def start(*copies):
        for copy in copies:
            copy.start()
            sends.append(copy)

    start(*exchange(0))
    start(*exchange(1))
    start(x_to_x[0], x_to_y[1], *x_over)
    start(x_to_x[1], x_to_y[0])
    for copy in qk_load:
        copy.wait()
    for j in range(nf):
        qkst[j] = jnp.concatenate(
            [qraw[:, j * kw : (j + 1) * kw], kraw[:, j * kw : (j + 1) * kw]], axis=1
        )
    wbuf[my_rows, pl.ds(2 * cw, cw)] = qkst[f]

    def own(i):
        if i < ROOT:
            if i in own_w:
                own_w[i].wait()
            for p in peers:
                arrived(
                    wbuf.at[
                        pl.ds(pl.multiple_of((z * nf + p) * rows_w, rows_w), rows_w),
                        pl.ds(i * cw, cw),
                    ],
                    ar.at[i, p],
                )
        else:
            own_o[i - ROOT].wait()

        @pl.when(z < nz - 1)
        def _():
            up(i, z).start()

        @pl.when(z > 0)
        def _():
            down(i, z).start()

    def relay(i, d):
        @pl.when(z >= d)
        def _():
            arrived(item(i, z - d), zr.at[i, z - d])

            @pl.when(z < nz - 1)
            def _():
                up(i, z - d).start()

        @pl.when(z + d < nz)
        def _():
            arrived(item(i, z + d), zr.at[i, z + d])

            @pl.when(z > 0)
            def _():
                down(i, z + d).start()

    own(0)
    start(*exchange(2))
    own(1)
    start(*exchange(3))
    start(*exchange(4))
    start(*decay_out)
    relay(0, 1)

    arrived(xr(xn, 0), xi.at[xn, 0])
    start(
        remote(xr(xn, 0), xr(xn, 0), xff.at[0], xi.at[xn, 0], (z, yn, c)),
        over(xn, 0),
    )
    arrived(xr(yn, 1), xi.at[yn, 1])
    start(
        remote(xr(yn, 1), xr(yn, 1), xff.at[1], xi.at[yn, 1], (z, xn, c)),
        over(yn, 1),
    )
    relay(0, 2)
    own(2)
    arrived(xr(xn, 1), xi.at[xn, 1])
    arrived(xr(yn, 0), xi.at[yn, 0])
    start(over(xn, 1), over(yn, 0))
    relay(1, 1)

    step_rows = 32

    def scale(seq):
        def body(r, carry):
            row = pl.ds(pl.multiple_of(seq * tok + r * step_rows, step_rows), step_rows)
            value = xbuf[row, :].astype(f32)
            square = jnp.sum(value * value, axis=1, keepdims=True)
            rs[row, :] = jnp.broadcast_to(
                lax.rsqrt(square / (nc * feat) + 1e-06), (step_rows, rs.shape[1])
            )
            xs[row, :] = (value * ng_ref[...]).astype(bf16)
            return carry

        lax.fori_loop(0, tok // step_rows, body, 0)

    for copy in own_x:
        copy.wait()
    for h in range(2):
        arrived(xr_other(f, h), xd.at[f, h])
    scale(f)
    relay(1, 2)
    own(3)
    for p in (xn, yn):
        for h in range(2):
            arrived(xr_other(p, h), xd.at[p, h])
        scale(p)
    arrived(xr(dg, 0), xi.at[dg, 0])
    arrived(xr(dg, 1), xi.at[dg, 1])
    start(over(dg, 0), over(dg, 1))
    relay(0, 3)
    relay(1, 3)
    for h in range(2):
        arrived(xr_other(dg, h), xd.at[dg, h])
    scale(dg)
    relay(2, 1)

    def project(seq, first, width):
        row = pl.ds(pl.multiple_of(seq * tok, tok), tok)
        out = jnp.dot(
            xs[row, :], wbuf[:, first : first + width], preferred_element_type=f32
        )
        return (out * rs[row, 0:1]).astype(bf16)

    halo = 32
    taps = ck_ref.shape[0]

    def conv_in(seq, carry):
        both = project(seq, 0, 2 * cw).astype(f32)
        gated = both[:, :cw] * jax.nn.sigmoid(both[:, cw:])
        ext[seq, halo : halo + tok, :] = gated.astype(bf16).astype(f32)
        return carry

    lax.fori_loop(0, nf, conv_in, 0)
    halo_out = remote(
        ext.at[:, pl.ds(tok, halo), :], ext.at[:, pl.ds(0, halo), :], hs, hr, (z + 1, f, c)
    )

    @pl.when(z < nz - 1)
    def _():
        halo_out.start()

    relay(2, 2)
    own(4)

    part = c * (nf // 2) + f // 2
    odd = lax.rem(f, 2) == 1
    dw2 = dw_ref[:, lanes(part, 2 * kw)].astype(f32)
    dw_own = jnp.where(odd, dw2[:, kw:], dw2[:, :kw]).astype(bf16)
    db2 = db_ref[:, lanes(part, 2 * kw)]
    db_own = jnp.where(odd, db2[:, kw:], db2[:, :kw])
    own_d.wait()
    for p in peers:
        arrived(debuf.at[p], dr.at[p])

    def decay(seq, carry):
        row = pl.ds(pl.multiple_of(seq * tok, tok), tok)
        low = jnp.dot(xs[row, :], ff_ref[...], preferred_element_type=f32)
        low = (low * rs[row, 0:1]).astype(bf16)
        pre = jnp.dot(low, dw_own, preferred_element_type=f32) + db_own
        extra = debuf[seq]
        extra = jnp.where(odd, extra[:, kw:], extra[:, :kw])
        ld[row, :] = jax.nn.log_sigmoid(pre) / 16.0 + extra
        return carry

    lax.fori_loop(0, nf, decay, 0)
    relay(2, 3)

    def keys_in(seq, carry):
        qkb[pl.ds(pl.multiple_of(seq * tok, tok), tok), :] = project(seq, 2 * cw, cw)
        return carry

    lax.fori_loop(0, nf, keys_in, 0)

    @pl.when(z > 0)
    def _():
        arrived(ext.at[:, pl.ds(0, halo), :], hr)

    @pl.when(z == 0)
    def _():
        ext[:, 0:halo, :] = jnp.zeros((nf, halo, cw), f32)

    mine = c * nf + f
    tap_rows = 64
    lane = lax.broadcasted_iota(jnp.int32, (tok, cw), 1)

    def tap(seq, carry):
        kernel = ck_ref[:, lanes(mine, cw)]
        for r in range(tok // tap_rows):
            acc = jnp.zeros((tap_rows, cw), f32)
            for j in range(taps):
                at = halo - (taps - 1) + j + r * tap_rows
                acc = acc + kernel[j : j + 1, :] * ext[seq, at : at + tap_rows, :]
            conv[pl.ds(pl.multiple_of(seq * tok + r * tap_rows, tap_rows), tap_rows), :] = acc
        row = pl.ds(pl.multiple_of(seq * tok, tok), tok)
        value = conv[row, :]
        mean = jnp.sum(value, axis=1, keepdims=True) / cw
        spread = value - mean
        second = jnp.sum(spread * spread, axis=1, keepdims=True)
        both = jnp.where(lane == 0, mean, jnp.where(lane == 1, second, 0.0))
        stats[me, :, pl.ds(pl.multiple_of(seq * tok, tok), tok)] = both.T[0:8, :]
        return carry

    lax.fori_loop(0, nf, tap, 0)
    relay(3, 1)
    for k in range(1, group):
        t = lax.rem(me + k, group)
        start(
            remote(
                stats.at[me], stats.at[me], tsn.at[k], tr.at[me], (z, t // nc, lax.rem(t, nc))
            )
        )
    for k in range(1, group):
        t = lax.rem(me + k, group)
        arrived(stats.at[t], tr.at[t])
    every = stats[...]
    means = every[:, 0, :]
    mean = jnp.sum(means, axis=0, keepdims=True) / group
    off = means - mean
    second = jnp.sum(every[:, 1, :] + cw * off * off, axis=0, keepdims=True)
    inverse = lax.rsqrt(second / channels + 1e-05)
    comb[0:1, :] = mean
    comb[1:2, :] = inverse

    def conv_out(seq, carry):
        row = pl.ds(pl.multiple_of(seq * tok, tok), tok)
        flat = comb[0:2, row]
        cols = jnp.concatenate([flat, jnp.zeros((cw - 2, tok), f32)], axis=0).T
        normed = (conv[row, :] - cols[:, 0:1]) * cols[:, 1:2] * cg_ref[:, lanes(mine, cw)]
        actbuf[row, lanes(f, cw)] = (normed * jax.nn.sigmoid(normed)).astype(bf16)
        return carry

    def act_block(at):
        return actbuf.at[:, lanes(at, cw)]

    relay(3, 2)
    own(5)

    def values_in(seq, carry):
        vb[pl.ds(pl.multiple_of(seq * tok, tok), tok), :] = project(seq, 3 * cw, cw)
        return carry

    relay(3, 3)
    lax.fori_loop(0, nf, values_in, 0)
    relay(4, 1)

    spread_m = (
        lax.broadcasted_iota(jnp.int32, (kw, vw), 0) // DK
        == lax.broadcasted_iota(jnp.int32, (kw, vw), 1) // DV
    ).astype(bf16)
    own_mask = (
        lax.broadcasted_iota(jnp.int32, (vw, kw), 1) // DK
        == lax.broadcasted_iota(jnp.int32, (vw, kw), 0) // DV
    )
    place = lax.rem(lax.broadcasted_iota(jnp.int32, (CHUNK, kw), 0), SUB)
    per_seq = tok // CHUNK

    def attend(n, carry):
        at = pl.ds(pl.multiple_of(n * CHUNK, CHUNK), CHUNK)
        qk = qkb[at, :].astype(f32)
        q = qk[:, :kw] * DK ** (-0.5)
        k = qk[:, kw:]
        v = vb[at, :].astype(f32)
        cum = ld[at, :]
        step = 1
        while step < SUB:
            cum = cum + jnp.where(place >= step, pltpu.roll(cum, step, 0), 0.0)
            step *= 2
        acc = jnp.dot((q * k).astype(bf16), spread_m, preferred_element_type=f32) * v
        for lag in range(1, SUB):
            decays = jnp.exp(jnp.where(place >= lag, cum - pltpu.roll(cum, lag, 0), -jnp.inf))
            term = (q * pltpu.roll(k, lag, 0) * decays).astype(bf16)
            score = jnp.dot(term, spread_m, preferred_element_type=f32)
            acc = acc + score * pltpu.roll(v, lag, 0)
        q_f = q * jnp.exp(cum)
        q_in = q_f.astype(bf16)
        v_low = v.astype(bf16)
        first = lax.rem(n, per_seq) == 0
        state = jnp.where(first, 0.0, state_ref[...])
        base = jnp.where(first, 0.0, base_ref[0:1, :])
        outer, seg = [], []
        for m in range(CHUNK // SUB):
            part = slice(m * SUB, (m + 1) * SUB)
            last = cum[(m + 1) * SUB - 1 : (m + 1) * SUB]
            k_out = (k[part] * jnp.exp(last - cum[part])).astype(bf16)
            outer.append(
                lax.dot_general(
                    q_in[part], state.astype(bf16), (((1,), (1,)), ((), ())),
                    preferred_element_type=f32,
                )
            )
            added = lax.dot_general(
                v_low[part], k_out, (((0,), (0,)), ((), ())), preferred_element_type=f32
            )
            seg.append(q_f[part] * jnp.exp(base))
            state = state * jnp.exp(last) + jnp.where(own_mask, added, 0.0)
            base = base + last
        state_ref[...] = state
        base_ref[...] = jnp.broadcast_to(base, base_ref.shape)
        sfin[n // per_seq] = state
        tots[n // per_seq] = jnp.broadcast_to(base, base_ref.shape)
        raw[at, :] = acc + jnp.concatenate(outer, axis=0)
        qseg[at, :] = jnp.concatenate(seg, axis=0).astype(bf16)
        return carry

    lax.fori_loop(0, total // CHUNK, attend, 0)
    vh = vw // 2
    for p in range(nf // 2):
        a, b = sfin[2 * p], sfin[2 * p + 1]
        stbuf[z, p, 0:vh, :] = jnp.concatenate(
            [a[:vh] + a[vh:], b[:vh] + b[vh:]], axis=1
        )
        stbuf[z, p, vh : vh + 8, :] = jnp.concatenate([tots[2 * p], tots[2 * p + 1]], axis=1)
    lax.fori_loop(0, nf, conv_out, 0)
    for d in range(1, nz):
        @pl.when(z + d < nz)
        def _():
            remote(stbuf.at[z], stbuf.at[z], vsn.at[d], vr.at[z], (z + d, f, c)).start()
    for n, p in enumerate(peers):
        start(remote(act_block(f), act_block(f), csn.at[n], cr.at[f], (z, p, c)))
    relay(4, 2)
    own(6)
    relay(4, 3)
    relay(5, 1)

    sin_ref[...] = jnp.zeros_like(sin_ref)
    for b in range(nz - 1):
        @pl.when(z > b)
        def _():
            arrived(stbuf.at[b], vr.at[b])
            sin_ref[...] = (
                sin_ref[...] * jnp.exp(stbuf[b, :, vh : vh + 1, :]) + stbuf[b, :, 0:vh, :]
            )
    head_mean = jnp.where(
        lax.broadcasted_iota(jnp.int32, (vw, vw), 0) // DV
        == lax.broadcasted_iota(jnp.int32, (vw, vw), 1) // DV,
        1.0 / DV,
        0.0,
    ).astype(f32)
    gain = jnp.concatenate([hg_ref[...]] * (vw // DV), axis=1)
    for seq in range(nf):
        row = slice(seq * tok, (seq + 1) * tok)
        lo = (seq % 2) * kw
        packed = sin_ref[seq // 2][:, lo : lo + kw]
        state = jnp.where(own_mask, jnp.concatenate([packed, packed], axis=0), 0.0).astype(bf16)
        full = raw[row, :] + lax.dot_general(
            qseg[row, :], state, (((1,), (1,)), ((), ())), preferred_element_type=f32
        )
        mean = jnp.dot(
            full * full, head_mean, preferred_element_type=f32, precision=lax.Precision.HIGHEST
        )
        gate = project(seq, 4 * cw, cw).astype(f32)
        actbuf[row, lanes(nf + f, cw)] = (
            full * lax.rsqrt(mean + 1e-06) * gain * (gate * jax.nn.sigmoid(gate))
        ).astype(bf16)
    relay(5, 2)
    for n, p in enumerate(peers):
        start(remote(act_block(nf + f), act_block(nf + f), gsn.at[n], gr.at[f], (z, p, c)))
    relay(6, 1)
    relay(5, 3)
    for p in peers:
        arrived(act_block(p), cr.at[p])
        arrived(act_block(nf + p), gr.at[p])

    near = jnp.where(z < nz // 2, z, nz - 1 - z)
    out_rows = pw.shape[0]
    slot_cols = nf * out_rows
    per_core = nz // nc

    def block_of(k):
        o = (near, 1 - near, 2, 3)[k]
        return jnp.where(z < nz // 2, o, nz - 1 - o)

    def over_part(k, slot):
        return remote(pbuf.at[k], prcv.at[slot], psn.at[slot], pr.at[slot], (z, f, other))

    def out_copy(slot, n, p):
        row = pl.ds(pl.multiple_of(p * tok, tok), tok)
        return remote(
            osum.at[slot, row, :],
            rbuf.at[:, lanes(slot * nf + f, out_rows)],
            osn.at[slot, n], orc.at[slot, f], (z, p, c),
        )

    for k in range(nz):
        if k == 1:
            relay(6, 2)
        if k == 3:
            relay(6, 3)
        b = block_of(k)
        slot = lax.rem(b, per_core)
        owner = b // per_core

        def multiply(seq, carry):
            row = pl.ds(pl.multiple_of(seq * tok, tok), tok)
            out = lax.dot_general(
                actbuf[row, :], wobuf[b], (((1,), (1,)), ((), ())), preferred_element_type=f32
            )
            pbuf[k, row, :] = out.astype(bf16)
            return carry

        lax.fori_loop(0, nf, multiply, 0)

        @pl.when(owner != c)
        def _():
            over_part(k, slot).start()

        @pl.when(owner == c)
        def _():
            arrived(prcv.at[slot], pr.at[slot])
            osum[slot] = (pbuf[k].astype(f32) + prcv[slot].astype(f32)).astype(bf16)
            for n, p in enumerate(peers):
                out_copy(slot, n, p).start()
            rbuf[:, lanes(slot * nf + f, out_rows)] = osum[slot, pl.ds(pl.multiple_of(f * tok, tok), tok), :]

    mine_x = xbuf.at[pl.ds(pl.multiple_of(f * tok, tok), tok), lanes(c, feat)]
    for slot in range(per_core):
        for p in peers:
            arrived(rbuf.at[:, lanes(slot * nf + p, out_rows)], orc.at[slot, p])
    o_ref[...] = (mine_x[...].astype(f32) + rbuf[...].astype(f32)).astype(bf16)

    for copy in sends:
        copy.wait_send()
    for i in range(items):
        for b in range(nz):
            @pl.when((z < nz - 1) & (z >= b))
            def _():
                up(i, b).wait_send()

            @pl.when((z > 0) & (z <= b))
            def _():
                down(i, b).wait_send()

    @pl.when(z < nz - 1)
    def _():
        halo_out.wait_send()

    for d in range(1, nz):
        @pl.when(z + d < nz)
        def _():
            remote(stbuf.at[z], stbuf.at[z], vsn.at[d], vr.at[z], (z + d, f, c)).wait_send()
    for k in range(nz):
        b = block_of(k)
        slot = lax.rem(b, per_core)

        @pl.when(b // per_core != c)
        def _():
            over_part(k, slot).wait_send()

        @pl.when(b // per_core == c)
        def _():
            for n, p in enumerate(peers):
                out_copy(slot, n, p).wait_send()


def by_segments(
    inputs, norm_gain, conv_in_a, conv_in_b, query_w, key_w, value_w, out_gate_w,
    pointwise_w, gla_out_w, forget_first_factor, decay_w, decay_bias, decay_extra,
    conv_kernel, conv_gain, head_gain,
):
    f32, bf16 = jnp.float32, jnp.bfloat16
    nz, nf, nc = lax.axis_size("sp"), lax.axis_size("fs"), lax.axis_size("tp")
    x = inputs[0]
    tok, feat = x.shape
    total = nf * tok
    rows_w = conv_in_a.shape[0]
    kin = nz * nf * rows_w
    cw = conv_in_a.shape[1] // nf
    kw = query_w.shape[1] // nf
    vw = value_w.shape[1] // nf
    pwc = pointwise_w.shape[1]
    out_rows = pointwise_w.shape[0]
    group = nf * nc
    dma = pltpu.SemaphoreType.DMA
    items = ROOT + OUT_ITEMS
    any_spec = pl.BlockSpec(memory_space=pl.ANY)
    vmem = pl.BlockSpec(memory_space=pltpu.VMEM)
    V = pltpu.VMEM
    scratch = [
        V((total, nc * feat), bf16), V((total, nc * feat), bf16), V((total, 128), f32),
        V((kin, ROOT * cw), bf16), V((rows_w, nf * kw), bf16), V((rows_w, nf * kw), bf16),
        V((nf, rows_w, cw), bf16), V((nz, out_rows, OUT_ITEMS * pwc), bf16),
        V((nf, tok, 2 * kw), f32), V((nf, tok + 32, cw), f32), V((total, cw), f32),
        V((group, 8, total), f32), V((8, total), f32), V((total, 2 * nf * cw), bf16),
        V((total, cw), bf16), V((total, vw), bf16), V((total, kw), f32), V((total, vw), f32),
        V((total, kw), bf16), V((vw, kw), f32), V((8, kw), f32), V((nf, vw, kw), f32),
        V((nf, 8, kw), f32), V((nz, nf // 2, vw // 2 + 8, 2 * kw), f32),
        V((nf // 2, vw // 2, 2 * kw), f32),
        V((nz, total, out_rows), bf16), V((nz // nc, total, out_rows), bf16),
        V((nz // nc, total, out_rows), bf16), V((tok, feat), bf16),
        dma((2,)), dma((2,)), dma((2,)), dma((2,)), dma((nf, 2)), dma((nf, 2)), dma((nf, 2)),
        dma((ROOT,)), dma((ROOT, nf - 1)), dma((ROOT, nf)),
        dma((items, nz)), dma((items, nz)), dma((items, nz)), dma((4,)), dma,
        dma((nf - 1,)), dma((nf,)), dma, dma, dma((group,)), dma((group,)),
        dma((nz,)), dma((nz,)), dma((nf - 1,)), dma((nf,)), dma((nf - 1,)), dma((nf,)),
        dma((nz // nc,)), dma((nz // nc,)), dma((nz // nc, nf - 1)), dma((nz // nc, nf)),
    ]
    out = pl.pallas_call(
        fused_kernel,
        out_shape=jax.ShapeDtypeStruct((tok, feat), bf16),
        in_specs=[any_spec] * 10 + [vmem] * 7,
        out_specs=vmem,
        scratch_shapes=scratch,
        compiler_params=pltpu.CompilerParams(
            collective_id=0, has_side_effects=True, vmem_limit_bytes=60 * 1024 * 1024
        ),
        name="mixer",
    )(
        x, conv_in_a, conv_in_b, query_w, key_w, value_w, out_gate_w, pointwise_w, gla_out_w,
        decay_extra[0], norm_gain[None], forget_first_factor, decay_w, decay_bias[None],
        conv_kernel, conv_gain[None], head_gain[None],
    )
    return out[None]


def fits(inputs, conv_in_a, query_w, value_w):
    n_sp, n_tp, n_fs = lax.axis_size("sp"), lax.axis_size("tp"), lax.axis_size("fs")
    widths = (conv_in_a.shape[1], 2 * query_w.shape[1], value_w.shape[1])
    return (
        (n_sp, n_fs, n_tp) == (4, 4, 2)
        and inputs.shape[0] == 1
        and inputs.shape[1] % CHUNK == 0
        and all(w == 128 * n_fs for w in widths)
    )


def from_behind(value, axis, by):
    length = lax.axis_size(axis)
    pairs = [(i, i + by) for i in range(length) if 0 <= i + by < length]
    return lax.ppermute(value, axis, pairs)


def by_tokens(
    inputs,
    norm_gain,
    conv_in_a,
    conv_in_b,
    query_w,
    key_w,
    value_w,
    out_gate_w,
    pointwise_w,
    gla_out_w,
    forget_first_factor,
    decay_w,
    decay_bias,
    decay_extra,
    conv_kernel,
    conv_gain,
    head_gain,
):
    collected = (
        lax.all_gather(conv_in_a, ("sp", "fs"), axis=0, tiled=True),
        lax.all_gather(conv_in_b, ("sp", "fs"), axis=0, tiled=True),
        lax.all_gather(query_w, ("sp", "fs"), axis=0, tiled=True),
        lax.all_gather(key_w, ("sp", "fs"), axis=0, tiled=True),
        lax.all_gather(value_w, ("sp", "fs"), axis=0, tiled=True),
        lax.all_gather(out_gate_w, ("sp", "fs"), axis=0, tiled=True),
        lax.all_gather(pointwise_w, ("sp", "fs"), axis=0, tiled=True),
        lax.all_gather(gla_out_w, ("sp", "fs"), axis=0, tiled=True),
    )
    (
        conv_a_full,
        conv_b_full,
        query_full,
        key_full,
        value_full,
        gate_full,
        pointwise_full,
        gla_out_full,
    ) = collected
    tok_rows = inputs[0]
    token_count = tok_rows.shape[0]
    in_weights = (
        conv_a_full,
        conv_b_full,
        query_full,
        key_full,
        value_full,
        gate_full,
        forget_first_factor,
    )
    segment_values = lax.all_gather(tok_rows, "tp", axis=1, tiled=True).astype(jnp.float32)
    scaled = (segment_values * norm_gain).astype(jnp.bfloat16)
    sums = tuple(
        (jnp.dot(scaled, weight, preferred_element_type=jnp.float32) for weight in in_weights)
    )
    sums, squares = (sums, jnp.sum(segment_values * segment_values, axis=1))
    row_scale = lax.rsqrt(squares / norm_gain.shape[0] + 1e-06)[:, None]
    conv_a, conv_b, queries, keys, values, out_gate, low_rank = [
        (running * row_scale).astype(jnp.bfloat16) for running in sums
    ]
    gated = (conv_a.astype(jnp.float32) * jax.nn.sigmoid(conv_b.astype(jnp.float32))).astype(
        jnp.bfloat16
    )
    reach = conv_kernel.shape[0] - 1
    earlier = from_behind(gated[token_count - reach :], "sp", 1)
    extended = jnp.concatenate([earlier, gated], axis=0).astype(jnp.float32)
    tp_index = lax.axis_index("tp")
    channels = gated.shape[1]
    kernel = lax.dynamic_slice_in_dim(conv_kernel, tp_index * channels, channels, 1)
    convolved = jnp.zeros((token_count, channels), jnp.float32)
    for offset in range(reach + 1):
        convolved = convolved + kernel[offset] * extended[offset : offset + token_count]
    channel_sum, channel_squares = lax.psum(
        (jnp.sum(convolved, axis=1), jnp.sum(convolved * convolved, axis=1)), "tp"
    )
    total_channels = conv_gain.shape[0]
    average = channel_sum / total_channels
    spread_squared_mean = channel_squares / total_channels - average * average
    gain_part = lax.dynamic_slice_in_dim(conv_gain, tp_index * channels, channels)
    normed = (
        (convolved - average[:, None]) * lax.rsqrt(spread_squared_mean + 1e-05)[:, None] * gain_part
    )
    conv_act = jax.nn.silu(normed).astype(jnp.bfloat16)
    key_width = keys.shape[1]
    head_count = key_width // DK
    decay_part = lax.dynamic_slice_in_dim(decay_w, tp_index * key_width, key_width, 1)
    bias_part = lax.dynamic_slice_in_dim(decay_bias, tp_index * key_width, key_width)
    pre_decay = jnp.dot(low_rank, decay_part, preferred_element_type=jnp.float32) + bias_part
    log_decay = jax.nn.log_sigmoid(pre_decay) / 16.0 + decay_extra[0]
    block_count = token_count // BLOCK
    highest = lax.Precision.HIGHEST

    def split_blocks(array_operand, width):
        return array_operand.reshape(block_count, BLOCK, head_count, width).transpose(0, 2, 1, 3)

    q_blocks = split_blocks(queries.astype(jnp.float32), DK) * DK ** (-0.5)
    k_blocks = split_blocks(keys.astype(jnp.float32), DK)
    v_blocks = split_blocks(values.astype(jnp.float32), DV)
    prefix_running_sum = jnp.cumsum(split_blocks(log_decay, DK), axis=2)
    causal = jnp.tril(jnp.ones((BLOCK, BLOCK), dtype=bool))
    spread = prefix_running_sum[:, :, :, None, :] - prefix_running_sum[:, :, None, :, :]
    weights_in = jnp.exp(jnp.where(causal[:, :, None], spread, -jnp.inf))
    scores = jnp.einsum("nhid,nhjd,nhijd->nhij", q_blocks, k_blocks, weights_in, precision=highest)
    inner = jnp.einsum("nhij,nhjv->nhiv", scores, v_blocks, precision=highest)
    block_total = prefix_running_sum[:, :, -1]
    block_state = jnp.einsum(
        "nhjd,nhjv->nhdv",
        k_blocks * jnp.exp(block_total[:, :, None] - prefix_running_sum),
        v_blocks,
        precision=highest,
    )

    def advance(state, block_pair):
        decay_row, added_share_term = block_pair
        return (jnp.exp(decay_row)[..., None] * state + added_share_term, state)

    local_final, local_entering = lax.scan(
        advance, jnp.zeros((head_count, DK, DV), jnp.float32), (block_total, block_state)
    )
    device_total = jnp.sum(block_total, axis=0)
    totals = lax.all_gather(device_total[None], "sp", axis=0, tiled=True)
    running_totals = jnp.cumsum(totals, axis=0)
    sp_index = lax.axis_index("sp")
    before = lax.dynamic_index_in_dim(
        running_totals, sp_index, 0, False
    ) - lax.dynamic_index_in_dim(totals, sp_index, 0, False)
    piece = lax.all_gather(local_final[None], "sp", axis=0, tiled=True)
    number = piece.shape[0]
    anchor = jnp.arange(number, dtype=jnp.int32)
    exponent = jnp.where(
        (anchor < sp_index)[:, None, None], before[None] - running_totals, -jnp.inf
    )
    entering = jnp.einsum("nhd,nhdv->hdv", jnp.exp(exponent), piece, precision=highest)
    passed = jnp.exp(jnp.cumsum(block_total, axis=0) - block_total)
    entering_blocks = passed[..., None] * entering[None] + local_entering
    outer = jnp.einsum(
        "nhid,nhdv->nhiv",
        q_blocks * jnp.exp(prefix_running_sum),
        entering_blocks,
        precision=highest,
    )
    head_output = inner + outer
    normed_heads = (
        head_output
        * lax.rsqrt(jnp.mean(head_output * head_output, axis=-1, keepdims=True) + 1e-06)
        * head_gain
    )
    gla_rows = normed_heads.transpose(0, 2, 1, 3).reshape(token_count, head_count * DV)
    gla_act = (gla_rows * jax.nn.silu(out_gate.astype(jnp.float32))).astype(jnp.bfloat16)
    contract = (((1,), (1,)), ((), ()))
    conv_term = lax.dot_general(
        pointwise_full, conv_act, contract, preferred_element_type=jnp.float32
    )
    summed = lax.psum_scatter(
        (
            conv_term
            + lax.dot_general(gla_out_full, gla_act, contract, preferred_element_type=jnp.float32)
        ).astype(jnp.bfloat16),
        "tp",
        scatter_dimension=0,
        tiled=True,
    ).astype(jnp.float32)
    return (tok_rows.astype(jnp.float32) + summed.T).astype(jnp.bfloat16)[None]


def shards(*args):
    if fits(args[0], args[2], args[4], args[6]):
        return by_segments(*args)
    return by_tokens(*args)


def solution(mesh):
    by_rows = P(("sp", "fs"), "tp")
    return jax.shard_map(
        shards,
        mesh=mesh,
        in_specs=(P("fs", "sp", "tp"), P())
        + (by_rows,) * 8
        + (P(), P(), P(), P("fs", "sp", "tp"), P(), P(), P()),
        out_specs=P("fs", "sp", "tp"),
        check_vma=False,
    )
```

```python
import jax
import jax.numpy as jnp
from jax import lax
from jax.experimental import pallas as pl
from jax.experimental.pallas import tpu as pltpu
from jax.sharding import PartitionSpec as P


DK = 32
DV = 64
SUB = 16
BLOCK = 64


ROOT = 5
OUT_ITEMS = 2
CHUNK = 128
MESH_IDS = pl.DeviceIdType.MESH


def fused_kernel(
    x_hbm, wa, wb, wq, wk, wv, wg, pw, go, dex_hbm,
    ng_ref, ff_ref, dw_ref, db_ref, ck_ref, cg_ref, hg_ref,
    o_ref,
    xbuf, xs, rs, wbuf, qraw, kraw, qkst, wobuf, debuf, ext, conv, stats, comb, actbuf,
    qkb, vb, ld, raw, qseg, state_ref, base_ref, sfin, tots, stbuf, sin_ref,
    pbuf, prcv, osum, rbuf,
    xl, xsx, xsy, xff, xsd, xi, xd, al, ass, ar, zsu, zsd, zr, ol, dl, dsn, dr,
    hs, hr, tsn, tr, vsn, vr, csn, cr, gsn, gr, psn, pr, osn, orc,
):
    f32, bf16 = jnp.float32, jnp.bfloat16
    z, f, c = lax.axis_index("sp"), lax.axis_index("fs"), lax.axis_index("tp")
    nz, nf, nc = lax.axis_size("sp"), lax.axis_size("fs"), lax.axis_size("tp")
    tok, feat = x_hbm.shape
    half = tok // 2
    rows_w = wa.shape[0]
    layer_rows = nf * rows_w
    cw = wa.shape[1] // nf
    kw = wq.shape[1] // nf
    vw = wv.shape[1] // nf
    total = nf * tok
    kin = wbuf.shape[0]
    pwc = pw.shape[1]
    channels = nc * nf * cw
    other = 1 - c
    xn = f + 1 - 2 * lax.rem(f, 2)
    yn = f + 2 - 4 * (f // 2)
    dg = nf - 1 - f
    peers = (xn, yn, dg)

    def remote(src, dst, send, recv, dev):
        return pltpu.make_async_remote_copy(
            src_ref=src, dst_ref=dst, send_sem=send, recv_sem=recv,
            device_id=dev, device_id_type=MESH_IDS,
        )

    def arrived(dst, recv):
        remote(dst, dst, recv, recv, (z, f, other)).wait_recv()

    def lanes(at, width):
        return pl.ds(pl.multiple_of(at * width, width), width)

    def xr(seq, h):
        row = pl.ds(pl.multiple_of(seq * tok + h * half, half), half)
        return xbuf.at[row, lanes(c, feat)]

    def xr_other(seq, h):
        row = pl.ds(pl.multiple_of(seq * tok + h * half, half), half)
        return xbuf.at[row, lanes(other, feat)]

    def item(i, b):
        if i < ROOT:
            row = pl.ds(pl.multiple_of(b * layer_rows, layer_rows), layer_rows)
            return wbuf.at[row, pl.ds(i * cw, cw)]
        return wobuf.at[b, :, pl.ds((i - ROOT) * pwc, pwc)]

    def up(i, b):
        return remote(item(i, b), item(i, b), zsu.at[i, b], zr.at[i, b], (z + 1, f, c))

    def down(i, b):
        return remote(item(i, b), item(i, b), zsd.at[i, b], zr.at[i, b], (z - 1, f, c))

    items = ROOT + OUT_ITEMS
    sources = {0: wa, 1: wb, 3: wv, 4: wg}
    my_rows = pl.ds(pl.multiple_of((z * nf + f) * rows_w, rows_w), rows_w)

    own_x = [
        pltpu.make_async_copy(x_hbm.at[pl.ds(h * half, half), :], xr(f, h), xl.at[h])
        for h in range(2)
    ]
    qk_load = [
        pltpu.make_async_copy(wq, qraw, ol.at[2]),
        pltpu.make_async_copy(wk, kraw, ol.at[3]),
    ]
    own_w = {
        g: pltpu.make_async_copy(
            w.at[:, lanes(f, cw)], wbuf.at[my_rows, pl.ds(g * cw, cw)], al.at[g]
        )
        for g, w in sources.items()
    }
    own_o = [
        pltpu.make_async_copy(pw, item(ROOT, z), ol.at[0]),
        pltpu.make_async_copy(go, item(ROOT + 1, z), ol.at[1]),
    ]
    own_d = pltpu.make_async_copy(dex_hbm.at[:, lanes(f // 2, 2 * kw)], debuf.at[f], dl)
    for copy in qk_load:
        copy.start()
    for g in sources:
        own_w[g].start()
    for copy in own_x + own_o + [own_d]:
        copy.start()

    barrier = pltpu.get_barrier_semaphore()
    me = f * nc + c
    group = nf * nc
    for k in range(1, group):
        t = lax.rem(me + k, group)
        pl.semaphore_signal(barrier, inc=1, device_id=(z, t // nc, lax.rem(t, nc)), device_id_type=MESH_IDS)
    for k in range(1, nz):
        pl.semaphore_signal(barrier, inc=1, device_id=(lax.rem(z + k, nz), f, c), device_id_type=MESH_IDS)
    pl.semaphore_wait(barrier, group - 1 + nz - 1)

    def exchange(g):
        out = []
        for n, p in enumerate(peers):
            src = qkst.at[p] if g == 2 else sources[g].at[:, lanes(p, cw)]
            dst = wbuf.at[my_rows, pl.ds(g * cw, cw)]
            out.append(remote(src, dst, ass.at[g, n], ar.at[g, f], (z, p, c)))
        return out

    x_to_x = [
        remote(x_hbm.at[pl.ds(h * half, half), :], xr(f, h), xsx.at[h], xi.at[f, h], (z, xn, c))
        for h in range(2)
    ]
    x_to_y = [
        remote(x_hbm.at[pl.ds(h * half, half), :], xr(f, h), xsy.at[h], xi.at[f, h], (z, yn, c))
        for h in range(2)
    ]
    x_over = [
        remote(x_hbm.at[pl.ds(h * half, half), :], xr(f, h), xsd.at[f, h], xd.at[f, h], (z, f, other))
        for h in range(2)
    ]

    def over(seq, h):
        return remote(xr(seq, h), xr(seq, h), xsd.at[seq, h], xd.at[seq, h], (z, f, other))

    decay_out = [
        remote(
            dex_hbm.at[:, lanes(p // 2, 2 * kw)], debuf.at[f], dsn.at[n], dr.at[f], (z, p, c)
        )
        for n, p in enumerate(peers)
    ]

    sends = []

    def start(*copies):
        for copy in copies:
            copy.start()
            sends.append(copy)

    start(*exchange(0))
    start(*exchange(1))
    start(x_to_x[0], x_to_y[1], *x_over)
    for copy in qk_load:
        copy.wait()
    for j in range(nf):
        qkst[j] = jnp.concatenate(
            [qraw[:, j * kw : (j + 1) * kw], kraw[:, j * kw : (j + 1) * kw]], axis=1
        )
    wbuf[my_rows, pl.ds(2 * cw, cw)] = qkst[f]

    def own(i):
        if i < ROOT:
            if i in own_w:
                own_w[i].wait()
            for p in peers:
                arrived(
                    wbuf.at[
                        pl.ds(pl.multiple_of((z * nf + p) * rows_w, rows_w), rows_w),
                        pl.ds(i * cw, cw),
                    ],
                    ar.at[i, p],
                )
        else:
            own_o[i - ROOT].wait()

        @pl.when(z < nz - 1)
        def _():
            up(i, z).start()

        @pl.when(z > 0)
        def _():
            down(i, z).start()

    def relay(i, d):
        @pl.when(z >= d)
        def _():
            arrived(item(i, z - d), zr.at[i, z - d])

            @pl.when(z < nz - 1)
            def _():
                up(i, z - d).start()

        @pl.when(z + d < nz)
        def _():
            arrived(item(i, z + d), zr.at[i, z + d])

            @pl.when(z > 0)
            def _():
                down(i, z + d).start()

    own(0)
    start(*exchange(2))
    start(x_to_x[1], x_to_y[0])
    start(*exchange(3))
    own(1)
    relay(0, 1)

    arrived(xr(xn, 0), xi.at[xn, 0])
    start(
        remote(xr(xn, 0), xr(xn, 0), xff.at[0], xi.at[xn, 0], (z, yn, c)),
        over(xn, 0),
    )
    arrived(xr(yn, 1), xi.at[yn, 1])
    start(
        remote(xr(yn, 1), xr(yn, 1), xff.at[1], xi.at[yn, 1], (z, xn, c)),
        over(yn, 1),
    )
    start(*exchange(4))
    start(*decay_out)
    relay(0, 2)
    own(2)
    relay(1, 1)

    step_rows = 32

    def scale(seq):
        def body(r, carry):
            row = pl.ds(pl.multiple_of(seq * tok + r * step_rows, step_rows), step_rows)
            value = xbuf[row, :].astype(f32)
            square = jnp.sum(value * value, axis=1, keepdims=True)
            rs[row, :] = jnp.broadcast_to(
                lax.rsqrt(square / (nc * feat) + 1e-06), (step_rows, rs.shape[1])
            )
            xs[row, :] = (value * ng_ref[...]).astype(bf16)
            return carry

        lax.fori_loop(0, tok // step_rows, body, 0)

    for copy in own_x:
        copy.wait()
    for h in range(2):
        arrived(xr_other(f, h), xd.at[f, h])
    scale(f)
    arrived(xr(xn, 1), xi.at[xn, 1])
    arrived(xr(yn, 0), xi.at[yn, 0])
    start(over(xn, 1), over(yn, 0))
    relay(1, 2)
    own(3)
    for p in (xn, yn):
        for h in range(2):
            arrived(xr_other(p, h), xd.at[p, h])
        scale(p)
    relay(0, 3)
    relay(1, 3)
    relay(2, 1)
    arrived(xr(dg, 0), xi.at[dg, 0])
    arrived(xr(dg, 1), xi.at[dg, 1])
    start(over(dg, 0), over(dg, 1))
    for h in range(2):
        arrived(xr_other(dg, h), xd.at[dg, h])
    scale(dg)

    def project(seq, first, width):
        row = pl.ds(pl.multiple_of(seq * tok, tok), tok)
        out = jnp.dot(
            xs[row, :], wbuf[:, first : first + width], preferred_element_type=f32
        )
        return (out * rs[row, 0:1]).astype(bf16)

    halo = 32
    taps = ck_ref.shape[0]

    def conv_in(seq, carry):
        both = project(seq, 0, 2 * cw).astype(f32)
        gated = both[:, :cw] * jax.nn.sigmoid(both[:, cw:])
        ext[seq, halo : halo + tok, :] = gated.astype(bf16).astype(f32)
        return carry

    lax.fori_loop(0, nf, conv_in, 0)
    halo_out = remote(
        ext.at[:, pl.ds(tok, halo), :], ext.at[:, pl.ds(0, halo), :], hs, hr, (z + 1, f, c)
    )

    @pl.when(z < nz - 1)
    def _():
        halo_out.start()

    relay(2, 2)
    own(4)

    part = c * (nf // 2) + f // 2
    odd = lax.rem(f, 2) == 1
    dw2 = dw_ref[:, lanes(part, 2 * kw)].astype(f32)
    dw_own = jnp.where(odd, dw2[:, kw:], dw2[:, :kw]).astype(bf16)
    db2 = db_ref[:, lanes(part, 2 * kw)]
    db_own = jnp.where(odd, db2[:, kw:], db2[:, :kw])
    own_d.wait()
    for p in peers:
        arrived(debuf.at[p], dr.at[p])

    def decay(seq, carry):
        row = pl.ds(pl.multiple_of(seq * tok, tok), tok)
        low = lax.dot_general(
            xs[row, :], ff_ref[...], (((1,), (1,)), ((), ())), preferred_element_type=f32
        )
        low = (low * rs[row, 0:1]).astype(bf16)
        pre = jnp.dot(low, dw_own, preferred_element_type=f32) + db_own
        extra = debuf[seq]
        extra = jnp.where(odd, extra[:, kw:], extra[:, :kw])
        ld[row, :] = jax.nn.log_sigmoid(pre) / 16.0 + extra
        return carry

    lax.fori_loop(0, nf, decay, 0)
    relay(2, 3)

    def keys_in(seq, carry):
        qkb[pl.ds(pl.multiple_of(seq * tok, tok), tok), :] = project(seq, 2 * cw, cw)
        return carry

    lax.fori_loop(0, nf, keys_in, 0)

    @pl.when(z > 0)
    def _():
        arrived(ext.at[:, pl.ds(0, halo), :], hr)

    @pl.when(z == 0)
    def _():
        ext[:, 0:halo, :] = jnp.zeros((nf, halo, cw), f32)

    mine = c * nf + f
    tap_rows = 64
    lane = lax.broadcasted_iota(jnp.int32, (tok, cw), 1)

    def tap(seq, carry):
        kernel = ck_ref[:, lanes(mine, cw)]
        for r in range(tok // tap_rows):
            acc = jnp.zeros((tap_rows, cw), f32)
            for j in range(taps):
                at = halo - (taps - 1) + j + r * tap_rows
                acc = acc + kernel[j : j + 1, :] * ext[seq, at : at + tap_rows, :]
            conv[pl.ds(pl.multiple_of(seq * tok + r * tap_rows, tap_rows), tap_rows), :] = acc
        row = pl.ds(pl.multiple_of(seq * tok, tok), tok)
        value = conv[row, :]
        mean = jnp.sum(value, axis=1, keepdims=True) / cw
        spread = value - mean
        second = jnp.sum(spread * spread, axis=1, keepdims=True)
        both = jnp.where(lane == 0, mean, jnp.where(lane == 1, second, 0.0))
        stats[me, :, pl.ds(pl.multiple_of(seq * tok, tok), tok)] = both.T[0:8, :]
        return carry

    lax.fori_loop(0, nf, tap, 0)
    relay(3, 1)
    for k in range(1, group):
        t = lax.rem(me + k, group)
        start(
            remote(
                stats.at[me], stats.at[me], tsn.at[k], tr.at[me], (z, t // nc, lax.rem(t, nc))
            )
        )
    for k in range(1, group):
        t = lax.rem(me + k, group)
        arrived(stats.at[t], tr.at[t])
    every = stats[...]
    means = every[:, 0, :]
    mean = jnp.sum(means, axis=0, keepdims=True) / group
    off = means - mean
    second = jnp.sum(every[:, 1, :] + cw * off * off, axis=0, keepdims=True)
    inverse = lax.rsqrt(second / channels + 1e-05)
    comb[0:1, :] = mean
    comb[1:2, :] = inverse

    def conv_out(seq, carry):
        row = pl.ds(pl.multiple_of(seq * tok, tok), tok)
        flat = comb[0:2, row]
        cols = jnp.concatenate([flat, jnp.zeros((cw - 2, tok), f32)], axis=0).T
        normed = (conv[row, :] - cols[:, 0:1]) * cols[:, 1:2] * cg_ref[:, lanes(mine, cw)]
        actbuf[row, lanes(f, cw)] = (normed * jax.nn.sigmoid(normed)).astype(bf16)
        return carry

    def act_block(at):
        return actbuf.at[:, lanes(at, cw)]

    relay(3, 2)
    own(5)

    def values_in(seq, carry):
        vb[pl.ds(pl.multiple_of(seq * tok, tok), tok), :] = project(seq, 3 * cw, cw)
        return carry

    relay(3, 3)
    lax.fori_loop(0, nf, values_in, 0)

    spread_m = (
        lax.broadcasted_iota(jnp.int32, (kw, vw), 0) // DK
        == lax.broadcasted_iota(jnp.int32, (kw, vw), 1) // DV
    ).astype(bf16)
    own_mask = (
        lax.broadcasted_iota(jnp.int32, (vw, kw), 1) // DK
        == lax.broadcasted_iota(jnp.int32, (vw, kw), 0) // DV
    )
    place = lax.rem(lax.broadcasted_iota(jnp.int32, (CHUNK, kw), 0), SUB)
    per_seq = tok // CHUNK

    def attend(n, carry):
        at = pl.ds(pl.multiple_of(n * CHUNK, CHUNK), CHUNK)
        qk = qkb[at, :].astype(f32)
        q = qk[:, :kw] * DK ** (-0.5)
        k = qk[:, kw:]
        v = vb[at, :].astype(f32)
        cum = ld[at, :]
        step = 1
        while step < SUB:
            cum = cum + jnp.where(place >= step, pltpu.roll(cum, step, 0), 0.0)
            step *= 2
        acc = jnp.dot((q * k).astype(bf16), spread_m, preferred_element_type=f32) * v
        for lag in range(1, SUB):
            decays = jnp.exp(jnp.where(place >= lag, cum - pltpu.roll(cum, lag, 0), -jnp.inf))
            term = (q * pltpu.roll(k, lag, 0) * decays).astype(bf16)
            score = jnp.dot(term, spread_m, preferred_element_type=f32)
            acc = acc + score * pltpu.roll(v, lag, 0)
        q_f = q * jnp.exp(cum)
        q_in = q_f.astype(bf16)
        v_low = v.astype(bf16)
        first = lax.rem(n, per_seq) == 0
        state = jnp.where(first, 0.0, state_ref[...])
        base = jnp.where(first, 0.0, base_ref[0:1, :])
        outer, seg = [], []
        for m in range(CHUNK // SUB):
            part = slice(m * SUB, (m + 1) * SUB)
            last = cum[(m + 1) * SUB - 1 : (m + 1) * SUB]
            k_out = (k[part] * jnp.exp(last - cum[part])).astype(bf16)
            outer.append(
                lax.dot_general(
                    q_in[part], state.astype(bf16), (((1,), (1,)), ((), ())),
                    preferred_element_type=f32,
                )
            )
            added = lax.dot_general(
                v_low[part], k_out, (((0,), (0,)), ((), ())), preferred_element_type=f32
            )
            seg.append(q_f[part] * jnp.exp(base))
            state = state * jnp.exp(last) + jnp.where(own_mask, added, 0.0)
            base = base + last
        state_ref[...] = state
        base_ref[...] = jnp.broadcast_to(base, base_ref.shape)
        sfin[n // per_seq] = state
        tots[n // per_seq] = jnp.broadcast_to(base, base_ref.shape)
        raw[at, :] = acc + jnp.concatenate(outer, axis=0)
        qseg[at, :] = jnp.concatenate(seg, axis=0).astype(bf16)

        @pl.when(n == 1)
        def _():
            relay(4, 1)

        return carry

    lax.fori_loop(0, total // CHUNK, attend, 0)
    vh = vw // 2
    for p in range(nf // 2):
        a, b = sfin[2 * p], sfin[2 * p + 1]
        stbuf[z, p, 0:vh, :] = jnp.concatenate(
            [a[:vh] + a[vh:], b[:vh] + b[vh:]], axis=1
        )
        stbuf[z, p, vh : vh + 8, :] = jnp.concatenate([tots[2 * p], tots[2 * p + 1]], axis=1)
    for d in range(1, nz):
        @pl.when(z + d < nz)
        def _():
            remote(stbuf.at[z], stbuf.at[z], vsn.at[d], vr.at[z], (z + d, f, c)).start()
    relay(4, 2)
    own(6)
    lax.fori_loop(0, nf, conv_out, 0)
    for n, p in enumerate(peers):
        start(remote(act_block(f), act_block(f), csn.at[n], cr.at[f], (z, p, c)))
    relay(5, 1)
    relay(4, 3)

    sin_ref[...] = jnp.zeros_like(sin_ref)
    for b in range(nz - 1):
        @pl.when(z > b)
        def _():
            arrived(stbuf.at[b], vr.at[b])
            sin_ref[...] = (
                sin_ref[...] * jnp.exp(stbuf[b, :, vh : vh + 1, :]) + stbuf[b, :, 0:vh, :]
            )
    head_mean = jnp.where(
        lax.broadcasted_iota(jnp.int32, (vw, vw), 0) // DV
        == lax.broadcasted_iota(jnp.int32, (vw, vw), 1) // DV,
        1.0 / DV,
        0.0,
    ).astype(f32)
    gain = jnp.concatenate([hg_ref[...]] * (vw // DV), axis=1)
    for seq in range(nf):
        row = slice(seq * tok, (seq + 1) * tok)
        lo = (seq % 2) * kw
        packed = sin_ref[seq // 2][:, lo : lo + kw]
        state = jnp.where(own_mask, jnp.concatenate([packed, packed], axis=0), 0.0).astype(bf16)
        full = raw[row, :] + lax.dot_general(
            qseg[row, :], state, (((1,), (1,)), ((), ())), preferred_element_type=f32
        )
        mean = jnp.dot(
            full * full, head_mean, preferred_element_type=f32, precision=lax.Precision.HIGHEST
        )
        gate = project(seq, 4 * cw, cw).astype(f32)
        actbuf[row, lanes(nf + f, cw)] = (
            full * lax.rsqrt(mean + 1e-06) * gain * (gate * jax.nn.sigmoid(gate))
        ).astype(bf16)
    for n, p in enumerate(peers):
        start(remote(act_block(nf + f), act_block(nf + f), gsn.at[n], gr.at[f], (z, p, c)))
    relay(5, 2)
    relay(6, 1)
    relay(6, 2)
    relay(5, 3)
    for p in peers:
        arrived(act_block(p), cr.at[p])
        arrived(act_block(nf + p), gr.at[p])

    near = jnp.where(z < nz // 2, z, nz - 1 - z)
    out_rows = pw.shape[0]
    slot_cols = nf * out_rows
    per_core = nz // nc

    def block_of(k):
        o = (near, 1 - near, 2, 3)[k]
        return jnp.where(z < nz // 2, o, nz - 1 - o)

    def over_part(k, slot):
        return remote(pbuf.at[k], prcv.at[slot], psn.at[slot], pr.at[slot], (z, f, other))

    def out_copy(slot, n, p):
        row = pl.ds(pl.multiple_of(p * tok, tok), tok)
        return remote(
            osum.at[slot, row, :],
            rbuf.at[:, lanes(slot * nf + f, out_rows)],
            osn.at[slot, n], orc.at[slot, f], (z, p, c),
        )

    for k in range(nz):
        if k == 3:
            relay(6, 3)
        b = block_of(k)
        slot = lax.rem(b, per_core)
        owner = b // per_core

        def multiply(seq, carry):
            row = pl.ds(pl.multiple_of(seq * tok, tok), tok)
            out = lax.dot_general(
                actbuf[row, :], wobuf[b], (((1,), (1,)), ((), ())), preferred_element_type=f32
            )
            pbuf[k, row, :] = out.astype(bf16)
            return carry

        lax.fori_loop(0, nf, multiply, 0)

        @pl.when(owner != c)
        def _():
            over_part(k, slot).start()

        @pl.when(owner == c)
        def _():
            arrived(prcv.at[slot], pr.at[slot])
            osum[slot] = (pbuf[k].astype(f32) + prcv[slot].astype(f32)).astype(bf16)
            for n, p in enumerate(peers):
                out_copy(slot, n, p).start()
            rbuf[:, lanes(slot * nf + f, out_rows)] = osum[slot, pl.ds(pl.multiple_of(f * tok, tok), tok), :]

    mine_x = xbuf.at[pl.ds(pl.multiple_of(f * tok, tok), tok), lanes(c, feat)]
    for slot in range(per_core):
        for p in peers:
            arrived(rbuf.at[:, lanes(slot * nf + p, out_rows)], orc.at[slot, p])
    o_ref[...] = (mine_x[...].astype(f32) + rbuf[...].astype(f32)).astype(bf16)

    for copy in sends:
        copy.wait_send()
    for i in range(items):
        for b in range(nz):
            @pl.when((z < nz - 1) & (z >= b))
            def _():
                up(i, b).wait_send()

            @pl.when((z > 0) & (z <= b))
            def _():
                down(i, b).wait_send()

    @pl.when(z < nz - 1)
    def _():
        halo_out.wait_send()

    for d in range(1, nz):
        @pl.when(z + d < nz)
        def _():
            remote(stbuf.at[z], stbuf.at[z], vsn.at[d], vr.at[z], (z + d, f, c)).wait_send()
    for k in range(nz):
        b = block_of(k)
        slot = lax.rem(b, per_core)

        @pl.when(b // per_core != c)
        def _():
            over_part(k, slot).wait_send()

        @pl.when(b // per_core == c)
        def _():
            for n, p in enumerate(peers):
                out_copy(slot, n, p).wait_send()


def by_segments(
    inputs, norm_gain, conv_in_a, conv_in_b, query_w, key_w, value_w, out_gate_w,
    pointwise_w, gla_out_w, forget_first_factor, decay_w, decay_bias, decay_extra,
    conv_kernel, conv_gain, head_gain,
):
    f32, bf16 = jnp.float32, jnp.bfloat16
    nz, nf, nc = lax.axis_size("sp"), lax.axis_size("fs"), lax.axis_size("tp")
    x = inputs[0]
    tok, feat = x.shape
    total = nf * tok
    rows_w = conv_in_a.shape[0]
    kin = nz * nf * rows_w
    cw = conv_in_a.shape[1] // nf
    kw = query_w.shape[1] // nf
    vw = value_w.shape[1] // nf
    pwc = pointwise_w.shape[1]
    out_rows = pointwise_w.shape[0]
    group = nf * nc
    dma = pltpu.SemaphoreType.DMA
    items = ROOT + OUT_ITEMS
    any_spec = pl.BlockSpec(memory_space=pl.ANY)
    vmem = pl.BlockSpec(memory_space=pltpu.VMEM)
    V = pltpu.VMEM
    scratch = [
        V((total, nc * feat), bf16), V((total, nc * feat), bf16), V((total, 128), f32),
        V((kin, ROOT * cw), bf16), V((rows_w, nf * kw), bf16), V((rows_w, nf * kw), bf16),
        V((nf, rows_w, cw), bf16), V((nz, out_rows, OUT_ITEMS * pwc), bf16),
        V((nf, tok, 2 * kw), f32), V((nf, tok + 32, cw), f32), V((total, cw), f32),
        V((group, 8, total), f32), V((8, total), f32), V((total, 2 * nf * cw), bf16),
        V((total, cw), bf16), V((total, vw), bf16), V((total, kw), f32), V((total, vw), f32),
        V((total, kw), bf16), V((vw, kw), f32), V((8, kw), f32), V((nf, vw, kw), f32),
        V((nf, 8, kw), f32), V((nz, nf // 2, vw // 2 + 8, 2 * kw), f32),
        V((nf // 2, vw // 2, 2 * kw), f32),
        V((nz, total, out_rows), bf16), V((nz // nc, total, out_rows), bf16),
        V((nz // nc, total, out_rows), bf16), V((tok, feat), bf16),
        dma((2,)), dma((2,)), dma((2,)), dma((2,)), dma((nf, 2)), dma((nf, 2)), dma((nf, 2)),
        dma((ROOT,)), dma((ROOT, nf - 1)), dma((ROOT, nf)),
        dma((items, nz)), dma((items, nz)), dma((items, nz)), dma((4,)), dma,
        dma((nf - 1,)), dma((nf,)), dma, dma, dma((group,)), dma((group,)),
        dma((nz,)), dma((nz,)), dma((nf - 1,)), dma((nf,)), dma((nf - 1,)), dma((nf,)),
        dma((nz // nc,)), dma((nz // nc,)), dma((nz // nc, nf - 1)), dma((nz // nc, nf)),
    ]
    out = pl.pallas_call(
        fused_kernel,
        out_shape=jax.ShapeDtypeStruct((tok, feat), bf16),
        in_specs=[any_spec] * 10 + [vmem] * 7,
        out_specs=vmem,
        scratch_shapes=scratch,
        compiler_params=pltpu.CompilerParams(
            collective_id=0, has_side_effects=True, vmem_limit_bytes=60 * 1024 * 1024
        ),
        name="mixer",
    )(
        x, conv_in_a, conv_in_b, query_w, key_w, value_w, out_gate_w, pointwise_w, gla_out_w,
        decay_extra[0], norm_gain[None], forget_first_factor.T, decay_w, decay_bias[None],
        conv_kernel, conv_gain[None], head_gain[None],
    )
    return out[None]


def fits(inputs, conv_in_a, query_w, value_w):
    n_sp, n_tp, n_fs = lax.axis_size("sp"), lax.axis_size("tp"), lax.axis_size("fs")
    widths = (conv_in_a.shape[1], 2 * query_w.shape[1], value_w.shape[1])
    return (
        (n_sp, n_fs, n_tp) == (4, 4, 2)
        and inputs.shape[0] == 1
        and inputs.shape[1] % CHUNK == 0
        and all(w == 128 * n_fs for w in widths)
    )


def from_behind(value, axis, by):
    length = lax.axis_size(axis)
    pairs = [(i, i + by) for i in range(length) if 0 <= i + by < length]
    return lax.ppermute(value, axis, pairs)


def by_tokens(
    inputs,
    norm_gain,
    conv_in_a,
    conv_in_b,
    query_w,
    key_w,
    value_w,
    out_gate_w,
    pointwise_w,
    gla_out_w,
    forget_first_factor,
    decay_w,
    decay_bias,
    decay_extra,
    conv_kernel,
    conv_gain,
    head_gain,
):
    collected = (
        lax.all_gather(conv_in_a, ("sp", "fs"), axis=0, tiled=True),
        lax.all_gather(conv_in_b, ("sp", "fs"), axis=0, tiled=True),
        lax.all_gather(query_w, ("sp", "fs"), axis=0, tiled=True),
        lax.all_gather(key_w, ("sp", "fs"), axis=0, tiled=True),
        lax.all_gather(value_w, ("sp", "fs"), axis=0, tiled=True),
        lax.all_gather(out_gate_w, ("sp", "fs"), axis=0, tiled=True),
        lax.all_gather(pointwise_w, ("sp", "fs"), axis=0, tiled=True),
        lax.all_gather(gla_out_w, ("sp", "fs"), axis=0, tiled=True),
    )
    (
        conv_a_full,
        conv_b_full,
        query_full,
        key_full,
        value_full,
        gate_full,
        pointwise_full,
        gla_out_full,
    ) = collected
    tok_rows = inputs[0]
    token_count = tok_rows.shape[0]
    in_weights = (
        conv_a_full,
        conv_b_full,
        query_full,
        key_full,
        value_full,
        gate_full,
        forget_first_factor,
    )
    segment_values = lax.all_gather(tok_rows, "tp", axis=1, tiled=True).astype(jnp.float32)
    scaled = (segment_values * norm_gain).astype(jnp.bfloat16)
    sums = tuple(
        (jnp.dot(scaled, weight, preferred_element_type=jnp.float32) for weight in in_weights)
    )
    sums, squares = (sums, jnp.sum(segment_values * segment_values, axis=1))
    row_scale = lax.rsqrt(squares / norm_gain.shape[0] + 1e-06)[:, None]
    conv_a, conv_b, queries, keys, values, out_gate, low_rank = [
        (running * row_scale).astype(jnp.bfloat16) for running in sums
    ]
    gated = (conv_a.astype(jnp.float32) * jax.nn.sigmoid(conv_b.astype(jnp.float32))).astype(
        jnp.bfloat16
    )
    reach = conv_kernel.shape[0] - 1
    earlier = from_behind(gated[token_count - reach :], "sp", 1)
    extended = jnp.concatenate([earlier, gated], axis=0).astype(jnp.float32)
    tp_index = lax.axis_index("tp")
    channels = gated.shape[1]
    kernel = lax.dynamic_slice_in_dim(conv_kernel, tp_index * channels, channels, 1)
    convolved = jnp.zeros((token_count, channels), jnp.float32)
    for offset in range(reach + 1):
        convolved = convolved + kernel[offset] * extended[offset : offset + token_count]
    channel_sum, channel_squares = lax.psum(
        (jnp.sum(convolved, axis=1), jnp.sum(convolved * convolved, axis=1)), "tp"
    )
    total_channels = conv_gain.shape[0]
    average = channel_sum / total_channels
    spread_squared_mean = channel_squares / total_channels - average * average
    gain_part = lax.dynamic_slice_in_dim(conv_gain, tp_index * channels, channels)
    normed = (
        (convolved - average[:, None]) * lax.rsqrt(spread_squared_mean + 1e-05)[:, None] * gain_part
    )
    conv_act = jax.nn.silu(normed).astype(jnp.bfloat16)
    key_width = keys.shape[1]
    head_count = key_width // DK
    decay_part = lax.dynamic_slice_in_dim(decay_w, tp_index * key_width, key_width, 1)
    bias_part = lax.dynamic_slice_in_dim(decay_bias, tp_index * key_width, key_width)
    pre_decay = jnp.dot(low_rank, decay_part, preferred_element_type=jnp.float32) + bias_part
    log_decay = jax.nn.log_sigmoid(pre_decay) / 16.0 + decay_extra[0]
    block_count = token_count // BLOCK
    highest = lax.Precision.HIGHEST

    def split_blocks(array_operand, width):
        return array_operand.reshape(block_count, BLOCK, head_count, width).transpose(0, 2, 1, 3)

    q_blocks = split_blocks(queries.astype(jnp.float32), DK) * DK ** (-0.5)
    k_blocks = split_blocks(keys.astype(jnp.float32), DK)
    v_blocks = split_blocks(values.astype(jnp.float32), DV)
    prefix_running_sum = jnp.cumsum(split_blocks(log_decay, DK), axis=2)
    causal = jnp.tril(jnp.ones((BLOCK, BLOCK), dtype=bool))
    spread = prefix_running_sum[:, :, :, None, :] - prefix_running_sum[:, :, None, :, :]
    weights_in = jnp.exp(jnp.where(causal[:, :, None], spread, -jnp.inf))
    scores = jnp.einsum("nhid,nhjd,nhijd->nhij", q_blocks, k_blocks, weights_in, precision=highest)
    inner = jnp.einsum("nhij,nhjv->nhiv", scores, v_blocks, precision=highest)
    block_total = prefix_running_sum[:, :, -1]
    block_state = jnp.einsum(
        "nhjd,nhjv->nhdv",
        k_blocks * jnp.exp(block_total[:, :, None] - prefix_running_sum),
        v_blocks,
        precision=highest,
    )

    def advance(state, block_pair):
        decay_row, added_share_term = block_pair
        return (jnp.exp(decay_row)[..., None] * state + added_share_term, state)

    local_final, local_entering = lax.scan(
        advance, jnp.zeros((head_count, DK, DV), jnp.float32), (block_total, block_state)
    )
    device_total = jnp.sum(block_total, axis=0)
    totals = lax.all_gather(device_total[None], "sp", axis=0, tiled=True)
    running_totals = jnp.cumsum(totals, axis=0)
    sp_index = lax.axis_index("sp")
    before = lax.dynamic_index_in_dim(
        running_totals, sp_index, 0, False
    ) - lax.dynamic_index_in_dim(totals, sp_index, 0, False)
    piece = lax.all_gather(local_final[None], "sp", axis=0, tiled=True)
    number = piece.shape[0]
    anchor = jnp.arange(number, dtype=jnp.int32)
    exponent = jnp.where(
        (anchor < sp_index)[:, None, None], before[None] - running_totals, -jnp.inf
    )
    entering = jnp.einsum("nhd,nhdv->hdv", jnp.exp(exponent), piece, precision=highest)
    passed = jnp.exp(jnp.cumsum(block_total, axis=0) - block_total)
    entering_blocks = passed[..., None] * entering[None] + local_entering
    outer = jnp.einsum(
        "nhid,nhdv->nhiv",
        q_blocks * jnp.exp(prefix_running_sum),
        entering_blocks,
        precision=highest,
    )
    head_output = inner + outer
    normed_heads = (
        head_output
        * lax.rsqrt(jnp.mean(head_output * head_output, axis=-1, keepdims=True) + 1e-06)
        * head_gain
    )
    gla_rows = normed_heads.transpose(0, 2, 1, 3).reshape(token_count, head_count * DV)
    gla_act = (gla_rows * jax.nn.silu(out_gate.astype(jnp.float32))).astype(jnp.bfloat16)
    contract = (((1,), (1,)), ((), ()))
    conv_term = lax.dot_general(
        pointwise_full, conv_act, contract, preferred_element_type=jnp.float32
    )
    summed = lax.psum_scatter(
        (
            conv_term
            + lax.dot_general(gla_out_full, gla_act, contract, preferred_element_type=jnp.float32)
        ).astype(jnp.bfloat16),
        "tp",
        scatter_dimension=0,
        tiled=True,
    ).astype(jnp.float32)
    return (tok_rows.astype(jnp.float32) + summed.T).astype(jnp.bfloat16)[None]


def shards(*args):
    if fits(args[0], args[2], args[4], args[6]):
        return by_segments(*args)
    return by_tokens(*args)


def solution(mesh):
    by_rows = P(("sp", "fs"), "tp")
    return jax.shard_map(
        shards,
        mesh=mesh,
        in_specs=(P("fs", "sp", "tp"), P())
        + (by_rows,) * 8
        + (P(), P(), P(), P("fs", "sp", "tp"), P(), P(), P()),
        out_specs=P("fs", "sp", "tp"),
        check_vma=False,
    )
```

```python
import jax
import jax.numpy as jnp
from jax import lax
from jax.experimental import pallas as pl
from jax.experimental.pallas import tpu as pltpu
from jax.sharding import PartitionSpec as P


DK = 32
DV = 64
SUB = 16
BLOCK = 64


ROOT = 5
OUT_ITEMS = 2
CHUNK = 128
MESH_IDS = pl.DeviceIdType.MESH


def fused_kernel(
    x_hbm, wa, wb, wq, wk, wv, wg, pw, go, dex_hbm,
    ng_ref, ff_ref, dw_ref, db_ref, ck_ref, cg_ref, hg_ref,
    o_ref,
    xbuf, xs, rs, wbuf, qraw, kraw, qkst, wobuf, debuf, ext, hsend, hrecv, conv, stats, comb, actbuf,
    qkb, vb, ld, raw, qseg, state_ref, base_ref, sfin, tots, stbuf, totbuf, sin_ref,
    pbuf, prcv, osum, rbuf,
    xl, xsx, xsy, xff, xsd, xi, xd, al, ass, ar, zsu, zsd, zr, ol, dl, dsn, dr,
    hs, hr, tsn, tr, vsn, vr, csn, cr, gsn, gr, psn, pr, osn, orc,
):
    f32, bf16 = jnp.float32, jnp.bfloat16
    z, f, c = lax.axis_index("sp"), lax.axis_index("fs"), lax.axis_index("tp")
    nz, nf, nc = lax.axis_size("sp"), lax.axis_size("fs"), lax.axis_size("tp")
    tok, feat = x_hbm.shape
    half = tok // 2
    rows_w = wa.shape[0]
    layer_rows = nf * rows_w
    cw = wa.shape[1] // nf
    kw = wq.shape[1] // nf
    vw = wv.shape[1] // nf
    total = nf * tok
    kin = wbuf.shape[0]
    pwc = pw.shape[1]
    channels = nc * nf * cw
    other = 1 - c
    xn = f + 1 - 2 * lax.rem(f, 2)
    yn = f + 2 - 4 * (f // 2)
    dg = nf - 1 - f
    peers = (xn, yn, dg)

    def remote(src, dst, send, recv, dev):
        return pltpu.make_async_remote_copy(
            src_ref=src, dst_ref=dst, send_sem=send, recv_sem=recv,
            device_id=dev, device_id_type=MESH_IDS,
        )

    def arrived(dst, recv):
        remote(dst, dst, recv, recv, (z, f, other)).wait_recv()

    def lanes(at, width):
        return pl.ds(pl.multiple_of(at * width, width), width)

    def xr(seq, h):
        row = pl.ds(pl.multiple_of(seq * tok + h * half, half), half)
        return xbuf.at[row, lanes(c, feat)]

    def xr_other(seq, h):
        row = pl.ds(pl.multiple_of(seq * tok + h * half, half), half)
        return xbuf.at[row, lanes(other, feat)]

    def item(i, b):
        if i < ROOT:
            row = pl.ds(pl.multiple_of(b * layer_rows, layer_rows), layer_rows)
            return wbuf.at[row, pl.ds(i * cw, cw)]
        return wobuf.at[b, :, pl.ds((i - ROOT) * pwc, pwc)]

    def up(i, b):
        return remote(item(i, b), item(i, b), zsu.at[i, b], zr.at[i, b], (z + 1, f, c))

    def down(i, b):
        return remote(item(i, b), item(i, b), zsd.at[i, b], zr.at[i, b], (z - 1, f, c))

    items = ROOT + OUT_ITEMS
    sources = {0: wa, 1: wb, 3: wv, 4: wg}
    my_rows = pl.ds(pl.multiple_of((z * nf + f) * rows_w, rows_w), rows_w)

    own_x = [
        pltpu.make_async_copy(x_hbm.at[pl.ds(h * half, half), :], xr(f, h), xl.at[h])
        for h in range(2)
    ]
    qk_load = [
        pltpu.make_async_copy(wq, qraw, ol.at[2]),
        pltpu.make_async_copy(wk, kraw, ol.at[3]),
    ]
    own_w = {
        g: pltpu.make_async_copy(
            w.at[:, lanes(f, cw)], wbuf.at[my_rows, pl.ds(g * cw, cw)], al.at[g]
        )
        for g, w in sources.items()
    }
    own_o = [
        pltpu.make_async_copy(pw, item(ROOT, z), ol.at[0]),
        pltpu.make_async_copy(go, item(ROOT + 1, z), ol.at[1]),
    ]
    own_d = pltpu.make_async_copy(dex_hbm.at[:, lanes(f // 2, 2 * kw)], debuf.at[f], dl)
    for copy in qk_load:
        copy.start()
    for g in sources:
        own_w[g].start()
    for copy in own_x + own_o + [own_d]:
        copy.start()

    barrier = pltpu.get_barrier_semaphore()
    me = f * nc + c
    group = nf * nc
    for k in range(1, group):
        t = lax.rem(me + k, group)
        pl.semaphore_signal(barrier, inc=1, device_id=(z, t // nc, lax.rem(t, nc)), device_id_type=MESH_IDS)
    for k in range(1, nz):
        pl.semaphore_signal(barrier, inc=1, device_id=(lax.rem(z + k, nz), f, c), device_id_type=MESH_IDS)
    for copy in qk_load:
        copy.wait()
    for j in range(nf):
        qkst[j] = jnp.concatenate(
            [qraw[:, j * kw : (j + 1) * kw], kraw[:, j * kw : (j + 1) * kw]], axis=1
        )
    wbuf[my_rows, pl.ds(2 * cw, cw)] = qkst[f]
    pl.semaphore_wait(barrier, group - 1 + nz - 1)

    def exchange(g):
        out = []
        for n, p in enumerate(peers):
            src = qkst.at[p] if g == 2 else sources[g].at[:, lanes(p, cw)]
            dst = wbuf.at[my_rows, pl.ds(g * cw, cw)]
            out.append(remote(src, dst, ass.at[g, n], ar.at[g, f], (z, p, c)))
        return out

    x_to_x = [
        remote(x_hbm.at[pl.ds(h * half, half), :], xr(f, h), xsx.at[h], xi.at[f, h], (z, xn, c))
        for h in range(2)
    ]
    x_to_y = [
        remote(x_hbm.at[pl.ds(h * half, half), :], xr(f, h), xsy.at[h], xi.at[f, h], (z, yn, c))
        for h in range(2)
    ]
    x_over = [
        remote(x_hbm.at[pl.ds(h * half, half), :], xr(f, h), xsd.at[f, h], xd.at[f, h], (z, f, other))
        for h in range(2)
    ]

    def over(seq, h):
        return remote(xr(seq, h), xr(seq, h), xsd.at[seq, h], xd.at[seq, h], (z, f, other))

    decay_out = [
        remote(
            dex_hbm.at[:, lanes(p // 2, 2 * kw)], debuf.at[f], dsn.at[n], dr.at[f], (z, p, c)
        )
        for n, p in enumerate(peers)
    ]

    sends = []

    def start(*copies):
        for copy in copies:
            copy.start()
            sends.append(copy)


    def own(i):
        if i < ROOT:
            if i in own_w:
                own_w[i].wait()
            for p in peers:
                arrived(
                    wbuf.at[
                        pl.ds(pl.multiple_of((z * nf + p) * rows_w, rows_w), rows_w),
                        pl.ds(i * cw, cw),
                    ],
                    ar.at[i, p],
                )
        else:
            own_o[i - ROOT].wait()

        @pl.when(z < nz - 1)
        def _():
            up(i, z).start()

        @pl.when(z > 0)
        def _():
            down(i, z).start()

    def relay(i, d):
        @pl.when(z >= d)
        def _():
            arrived(item(i, z - d), zr.at[i, z - d])

            @pl.when(z < nz - 1)
            def _():
                up(i, z - d).start()

        @pl.when(z + d < nz)
        def _():
            arrived(item(i, z + d), zr.at[i, z + d])

            @pl.when(z > 0)
            def _():
                down(i, z + d).start()

    start(*exchange(0))
    own(5)
    start(*exchange(1))
    start(x_to_x[0], x_to_y[1], *x_over)
    own(0)
    start(*exchange(2))
    start(x_to_x[1], x_to_y[0])
    start(*exchange(3))
    own(1)
    relay(0, 1)

    arrived(xr(xn, 0), xi.at[xn, 0])
    start(
        remote(xr(xn, 0), xr(xn, 0), xff.at[0], xi.at[xn, 0], (z, yn, c)),
        over(xn, 0),
    )
    arrived(xr(yn, 1), xi.at[yn, 1])
    start(
        remote(xr(yn, 1), xr(yn, 1), xff.at[1], xi.at[yn, 1], (z, xn, c)),
        over(yn, 1),
    )
    start(*exchange(4))
    start(*decay_out)
    relay(0, 2)
    own(2)
    relay(1, 1)

    step_rows = 32

    def scale(seq):
        def body(r, carry):
            row = pl.ds(pl.multiple_of(seq * tok + r * step_rows, step_rows), step_rows)
            value = xbuf[row, :].astype(f32)
            square = jnp.sum(value * value, axis=1, keepdims=True)
            rs[row, :] = jnp.broadcast_to(
                lax.rsqrt(square / (nc * feat) + 1e-06), (step_rows, rs.shape[1])
            )
            xs[row, :] = (value * ng_ref[...]).astype(bf16)
            return carry

        lax.fori_loop(0, tok // step_rows, body, 0)

    for copy in own_x:
        copy.wait()
    for h in range(2):
        arrived(xr_other(f, h), xd.at[f, h])
    scale(f)
    arrived(xr(xn, 1), xi.at[xn, 1])
    arrived(xr(yn, 0), xi.at[yn, 0])
    start(over(xn, 1), over(yn, 0))
    relay(1, 2)
    own(3)
    for p in (xn, yn):
        for h in range(2):
            arrived(xr_other(p, h), xd.at[p, h])
        scale(p)
    relay(0, 3)
    relay(1, 3)
    relay(2, 1)
    arrived(xr(dg, 0), xi.at[dg, 0])
    arrived(xr(dg, 1), xi.at[dg, 1])
    start(over(dg, 0), over(dg, 1))
    for h in range(2):
        arrived(xr_other(dg, h), xd.at[dg, h])
    scale(dg)

    def project(seq, first, width):
        row = pl.ds(pl.multiple_of(seq * tok, tok), tok)
        out = jnp.dot(
            xs[row, :], wbuf[:, first : first + width], preferred_element_type=f32
        )
        return (out * rs[row, 0:1]).astype(bf16)

    halo = 32
    taps = ck_ref.shape[0]

    def conv_in(seq, carry):
        both = project(seq, 0, 2 * cw).astype(f32)
        gated = both[:, :cw] * jax.nn.sigmoid(both[:, cw:])
        low = gated.astype(bf16)
        ext[seq, halo : halo + tok, :] = low.astype(f32)
        hsend[seq] = low[tok - halo :]
        return carry

    lax.fori_loop(0, nf, conv_in, 0)
    halo_out = remote(hsend, hrecv, hs, hr, (z + 1, f, c))

    @pl.when(z < nz - 1)
    def _():
        halo_out.start()

    relay(2, 2)
    own(4)

    part = c * (nf // 2) + f // 2
    odd = lax.rem(f, 2) == 1
    dw2 = dw_ref[:, lanes(part, 2 * kw)].astype(f32)
    dw_own = jnp.where(odd, dw2[:, kw:], dw2[:, :kw]).astype(bf16)
    db2 = db_ref[:, lanes(part, 2 * kw)]
    db_own = jnp.where(odd, db2[:, kw:], db2[:, :kw])
    own_d.wait()
    for p in peers:
        arrived(debuf.at[p], dr.at[p])

    def decay(seq, carry):
        row = pl.ds(pl.multiple_of(seq * tok, tok), tok)
        low = lax.dot_general(
            xs[row, :], ff_ref[...], (((1,), (1,)), ((), ())), preferred_element_type=f32
        )
        low = (low * rs[row, 0:1]).astype(bf16)
        pre = jnp.dot(low, dw_own, preferred_element_type=f32) + db_own
        extra = debuf[seq]
        extra = jnp.where(odd, extra[:, kw:], extra[:, :kw])
        ld[row, :] = jax.nn.log_sigmoid(pre) / 16.0 + extra
        return carry

    lax.fori_loop(0, nf, decay, 0)
    relay(2, 3)

    def keys_in(seq, carry):
        qkb[pl.ds(pl.multiple_of(seq * tok, tok), tok), :] = project(seq, 2 * cw, cw)
        return carry

    lax.fori_loop(0, nf, keys_in, 0)

    @pl.when(z > 0)
    def _():
        arrived(hrecv, hr)
        ext[:, 0:halo, :] = hrecv[...].astype(f32)

    @pl.when(z == 0)
    def _():
        ext[:, 0:halo, :] = jnp.zeros((nf, halo, cw), f32)

    mine = c * nf + f
    tap_rows = 64
    lane = lax.broadcasted_iota(jnp.int32, (tok, cw), 1)

    def tap(seq, carry):
        kernel = ck_ref[:, lanes(mine, cw)]
        for r in range(tok // tap_rows):
            acc = jnp.zeros((tap_rows, cw), f32)
            for j in range(taps):
                at = halo - (taps - 1) + j + r * tap_rows
                acc = acc + kernel[j : j + 1, :] * ext[seq, at : at + tap_rows, :]
            conv[pl.ds(pl.multiple_of(seq * tok + r * tap_rows, tap_rows), tap_rows), :] = acc
        row = pl.ds(pl.multiple_of(seq * tok, tok), tok)
        value = conv[row, :]
        mean = jnp.sum(value, axis=1, keepdims=True) / cw
        spread = value - mean
        second = jnp.sum(spread * spread, axis=1, keepdims=True)
        both = jnp.where(lane == 0, mean, jnp.where(lane == 1, second, 0.0))
        stats[me, :, pl.ds(pl.multiple_of(seq * tok, tok), tok)] = both.T[0:8, :]
        return carry

    lax.fori_loop(0, nf, tap, 0)
    relay(3, 1)
    for k in range(1, group):
        t = lax.rem(me + k, group)
        start(
            remote(
                stats.at[me], stats.at[me], tsn.at[k], tr.at[me], (z, t // nc, lax.rem(t, nc))
            )
        )
    for k in range(1, group):
        t = lax.rem(me + k, group)
        arrived(stats.at[t], tr.at[t])
    every = stats[...]
    means = every[:, 0, :]
    mean = jnp.sum(means, axis=0, keepdims=True) / group
    off = means - mean
    second = jnp.sum(every[:, 1, :] + cw * off * off, axis=0, keepdims=True)
    inverse = lax.rsqrt(second / channels + 1e-05)
    comb[0:1, :] = mean
    comb[1:2, :] = inverse

    def conv_out(seq, carry):
        row = pl.ds(pl.multiple_of(seq * tok, tok), tok)
        flat = comb[0:2, row]
        cols = jnp.concatenate([flat, jnp.zeros((cw - 2, tok), f32)], axis=0).T
        normed = (conv[row, :] - cols[:, 0:1]) * cols[:, 1:2] * cg_ref[:, lanes(mine, cw)]
        actbuf[row, lanes(f, cw)] = (normed * jax.nn.sigmoid(normed)).astype(bf16)
        return carry

    def act_block(at):
        return actbuf.at[:, lanes(at, cw)]

    relay(3, 2)

    def values_in(seq, carry):
        vb[pl.ds(pl.multiple_of(seq * tok, tok), tok), :] = project(seq, 3 * cw, cw)
        return carry

    relay(3, 3)
    lax.fori_loop(0, nf, values_in, 0)

    spread_m = (
        lax.broadcasted_iota(jnp.int32, (kw, vw), 0) // DK
        == lax.broadcasted_iota(jnp.int32, (kw, vw), 1) // DV
    ).astype(bf16)
    own_mask = (
        lax.broadcasted_iota(jnp.int32, (vw, kw), 1) // DK
        == lax.broadcasted_iota(jnp.int32, (vw, kw), 0) // DV
    )
    place = lax.rem(lax.broadcasted_iota(jnp.int32, (CHUNK, kw), 0), SUB)
    per_seq = tok // CHUNK

    def attend(n, carry):
        at = pl.ds(pl.multiple_of(n * CHUNK, CHUNK), CHUNK)
        qk = qkb[at, :].astype(f32)
        q = qk[:, :kw] * DK ** (-0.5)
        k = qk[:, kw:]
        v = vb[at, :].astype(f32)
        cum = ld[at, :]
        step = 1
        while step < SUB:
            cum = cum + jnp.where(place >= step, pltpu.roll(cum, step, 0), 0.0)
            step *= 2
        acc = jnp.dot((q * k).astype(bf16), spread_m, preferred_element_type=f32) * v
        for lag in range(1, SUB):
            decays = jnp.exp(jnp.where(place >= lag, cum - pltpu.roll(cum, lag, 0), -jnp.inf))
            term = (q * pltpu.roll(k, lag, 0) * decays).astype(bf16)
            score = jnp.dot(term, spread_m, preferred_element_type=f32)
            acc = acc + score * pltpu.roll(v, lag, 0)
        q_f = q * jnp.exp(cum)
        q_in = q_f.astype(bf16)
        v_low = v.astype(bf16)
        first = lax.rem(n, per_seq) == 0
        state = jnp.where(first, 0.0, state_ref[...])
        base = jnp.where(first, 0.0, base_ref[0:1, :])
        outer, seg = [], []
        for m in range(CHUNK // SUB):
            part = slice(m * SUB, (m + 1) * SUB)
            last = cum[(m + 1) * SUB - 1 : (m + 1) * SUB]
            k_out = (k[part] * jnp.exp(last - cum[part])).astype(bf16)
            outer.append(
                lax.dot_general(
                    q_in[part], state.astype(bf16), (((1,), (1,)), ((), ())),
                    preferred_element_type=f32,
                )
            )
            added = lax.dot_general(
                v_low[part], k_out, (((0,), (0,)), ((), ())), preferred_element_type=f32
            )
            seg.append(q_f[part] * jnp.exp(base))
            state = state * jnp.exp(last) + jnp.where(own_mask, added, 0.0)
            base = base + last
        state_ref[...] = state
        base_ref[...] = jnp.broadcast_to(base, base_ref.shape)
        sfin[n // per_seq] = state
        tots[n // per_seq] = jnp.broadcast_to(base, base_ref.shape)
        raw[at, :] = acc + jnp.concatenate(outer, axis=0)
        qseg[at, :] = jnp.concatenate(seg, axis=0).astype(bf16)

        @pl.when(n == 1)
        def _():
            relay(4, 1)

        return carry

    lax.fori_loop(0, total // CHUNK, attend, 0)
    vh = vw // 2
    for p in range(nf // 2):
        a, b = sfin[2 * p], sfin[2 * p + 1]
        stbuf[z, p] = jnp.concatenate([a[:vh] + a[vh:], b[:vh] + b[vh:]], axis=1).astype(bf16)
        totbuf[z, p] = jnp.concatenate([tots[2 * p], tots[2 * p + 1]], axis=1)

    def state_out(d):
        dev = (z + d, f, c)
        return (
            remote(stbuf.at[z], stbuf.at[z], vsn.at[0, d], vr.at[0, z], dev),
            remote(totbuf.at[z], totbuf.at[z], vsn.at[1, d], vr.at[1, z], dev),
        )

    for d in range(1, nz):
        @pl.when(z + d < nz)
        def _():
            for copy in state_out(d):
                copy.start()

    relay(4, 2)
    own(6)
    lax.fori_loop(0, nf, conv_out, 0)
    for n, p in enumerate(peers):
        start(remote(act_block(f), act_block(f), csn.at[n], cr.at[f], (z, p, c)))
    relay(5, 1)
    relay(4, 3)

    sin_ref[...] = jnp.zeros_like(sin_ref)
    for b in range(nz - 1):
        @pl.when(z > b)
        def _():
            arrived(stbuf.at[b], vr.at[0, b])
            arrived(totbuf.at[b], vr.at[1, b])
            sin_ref[...] = sin_ref[...] * jnp.exp(totbuf[b, :, 0:1, :]) + stbuf[b].astype(f32)
    head_mean = jnp.where(
        lax.broadcasted_iota(jnp.int32, (vw, vw), 0) // DV
        == lax.broadcasted_iota(jnp.int32, (vw, vw), 1) // DV,
        1.0 / DV,
        0.0,
    ).astype(f32)
    gain = jnp.concatenate([hg_ref[...]] * (vw // DV), axis=1)
    for seq in range(nf):
        row = slice(seq * tok, (seq + 1) * tok)
        lo = (seq % 2) * kw
        packed = sin_ref[seq // 2][:, lo : lo + kw]
        state = jnp.where(own_mask, jnp.concatenate([packed, packed], axis=0), 0.0).astype(bf16)
        full = raw[row, :] + lax.dot_general(
            qseg[row, :], state, (((1,), (1,)), ((), ())), preferred_element_type=f32
        )
        mean = jnp.dot(
            full * full, head_mean, preferred_element_type=f32, precision=lax.Precision.HIGHEST
        )
        gate = project(seq, 4 * cw, cw).astype(f32)
        actbuf[row, lanes(nf + f, cw)] = (
            full * lax.rsqrt(mean + 1e-06) * gain * (gate * jax.nn.sigmoid(gate))
        ).astype(bf16)
    for n, p in enumerate(peers):
        start(remote(act_block(nf + f), act_block(nf + f), gsn.at[n], gr.at[f], (z, p, c)))
    relay(5, 2)

    near = jnp.where(z < nz // 2, z, nz - 1 - z)
    out_rows = pw.shape[0]
    slot_cols = nf * out_rows
    per_core = nz // nc

    def block_of(k):
        o = (near, 1 - near, 2, 3)[k]
        return jnp.where(z < nz // 2, o, nz - 1 - o)

    def rows_of(p):
        return pl.ds(pl.multiple_of(p * tok, tok), tok)

    def turn(j):
        return jnp.where(j == 0, dg, jnp.where(j == 1, xn, jnp.where(j == 2, yn, f)))

    def over_part(k, slot, p):
        return remote(
            pbuf.at[k, rows_of(p), :], prcv.at[slot, rows_of(p), :],
            psn.at[slot, p], pr.at[slot, p], (z, f, other),
        )

    def out_copy(slot, p):
        return remote(
            osum.at[slot, rows_of(p), :],
            rbuf.at[:, lanes(slot * nf + f, out_rows)],
            osn.at[slot, p], orc.at[slot, f], (z, p, c),
        )

    def block(k):
        b = block_of(k)
        slot = lax.rem(b, per_core)
        owner = b // per_core

        def multiply(j, carry):
            p = turn(j)
            out = lax.dot_general(
                actbuf[rows_of(p), :], wobuf[b], (((1,), (1,)), ((), ())),
                preferred_element_type=f32,
            )
            pbuf[k, rows_of(p), :] = out.astype(bf16)

            @pl.when(owner != c)
            def _():
                over_part(k, slot, p).start()

            return carry

        lax.fori_loop(0, nf, multiply, 0)

        def gather(j, carry):
            p = turn(j)
            arrived(prcv.at[slot, rows_of(p), :], pr.at[slot, p])
            osum[slot, rows_of(p), :] = (
                pbuf[k, rows_of(p), :].astype(f32) + prcv[slot, rows_of(p), :].astype(f32)
            ).astype(bf16)

            @pl.when(j < nf - 1)
            def _():
                out_copy(slot, p).start()

            return carry

        @pl.when(owner == c)
        def _():
            lax.fori_loop(0, nf, gather, 0)
            rbuf[:, lanes(slot * nf + f, out_rows)] = osum[slot, rows_of(f), :]

    def acts():
        for p in peers:
            arrived(act_block(p), cr.at[p])
            arrived(act_block(nf + p), gr.at[p])

    ends = (z == 0) | (z == nz - 1)

    @pl.when(ends)
    def _():
        relay(5, 3)
        acts()
        block(0)
        for k in range(1, nz):
            relay(6, k)
            block(k)

    @pl.when(jnp.logical_not(ends))
    def _():
        for k in range(1, nz):
            relay(6, k)
        acts()
        for k in range(nz):
            block(k)

    mine_x = xbuf.at[pl.ds(pl.multiple_of(f * tok, tok), tok), lanes(c, feat)]
    for slot in range(per_core):
        for p in peers:
            arrived(rbuf.at[:, lanes(slot * nf + p, out_rows)], orc.at[slot, p])
    o_ref[...] = (mine_x[...].astype(f32) + rbuf[...].astype(f32)).astype(bf16)

    for copy in sends:
        copy.wait_send()
    for i in range(items):
        for b in range(nz):
            @pl.when((z < nz - 1) & (z >= b))
            def _():
                up(i, b).wait_send()

            @pl.when((z > 0) & (z <= b))
            def _():
                down(i, b).wait_send()

    @pl.when(z < nz - 1)
    def _():
        halo_out.wait_send()

    for d in range(1, nz):
        @pl.when(z + d < nz)
        def _():
            for copy in state_out(d):
                copy.wait_send()
    for k in range(nz):
        b = block_of(k)
        slot = lax.rem(b, per_core)

        @pl.when(b // per_core != c)
        def _():
            for p in range(nf):
                over_part(k, slot, p).wait_send()

        @pl.when(b // per_core == c)
        def _():
            for p in peers:
                out_copy(slot, p).wait_send()


def by_segments(
    inputs, norm_gain, conv_in_a, conv_in_b, query_w, key_w, value_w, out_gate_w,
    pointwise_w, gla_out_w, forget_first_factor, decay_w, decay_bias, decay_extra,
    conv_kernel, conv_gain, head_gain,
):
    f32, bf16 = jnp.float32, jnp.bfloat16
    nz, nf, nc = lax.axis_size("sp"), lax.axis_size("fs"), lax.axis_size("tp")
    x = inputs[0]
    tok, feat = x.shape
    total = nf * tok
    rows_w = conv_in_a.shape[0]
    kin = nz * nf * rows_w
    cw = conv_in_a.shape[1] // nf
    kw = query_w.shape[1] // nf
    vw = value_w.shape[1] // nf
    pwc = pointwise_w.shape[1]
    out_rows = pointwise_w.shape[0]
    group = nf * nc
    dma = pltpu.SemaphoreType.DMA
    items = ROOT + OUT_ITEMS
    any_spec = pl.BlockSpec(memory_space=pl.ANY)
    vmem = pl.BlockSpec(memory_space=pltpu.VMEM)
    V = pltpu.VMEM
    scratch = [
        V((total, nc * feat), bf16), V((total, nc * feat), bf16), V((total, 128), f32),
        V((kin, ROOT * cw), bf16), V((rows_w, nf * kw), bf16), V((rows_w, nf * kw), bf16),
        V((nf, rows_w, cw), bf16), V((nz, out_rows, OUT_ITEMS * pwc), bf16),
        V((nf, tok, 2 * kw), f32), V((nf, tok + 32, cw), f32), V((nf, 32, cw), bf16), V((nf, 32, cw), bf16), V((total, cw), f32),
        V((group, 8, total), f32), V((8, total), f32), V((total, 2 * nf * cw), bf16),
        V((total, cw), bf16), V((total, vw), bf16), V((total, kw), f32), V((total, vw), f32),
        V((total, kw), bf16), V((vw, kw), f32), V((8, kw), f32), V((nf, vw, kw), f32),
        V((nf, 8, kw), f32), V((nz, nf // 2, vw // 2, 2 * kw), bf16),
        V((nz, nf // 2, 8, 2 * kw), f32),
        V((nf // 2, vw // 2, 2 * kw), f32),
        V((nz, total, out_rows), bf16), V((nz // nc, total, out_rows), bf16),
        V((nz // nc, total, out_rows), bf16), V((tok, feat), bf16),
        dma((2,)), dma((2,)), dma((2,)), dma((2,)), dma((nf, 2)), dma((nf, 2)), dma((nf, 2)),
        dma((ROOT,)), dma((ROOT, nf - 1)), dma((ROOT, nf)),
        dma((items, nz)), dma((items, nz)), dma((items, nz)), dma((4,)), dma,
        dma((nf - 1,)), dma((nf,)), dma, dma, dma((group,)), dma((group,)),
        dma((2, nz)), dma((2, nz)), dma((nf - 1,)), dma((nf,)), dma((nf - 1,)), dma((nf,)),
        dma((nz // nc, nf)), dma((nz // nc, nf)), dma((nz // nc, nf)), dma((nz // nc, nf)),
    ]
    out = pl.pallas_call(
        fused_kernel,
        out_shape=jax.ShapeDtypeStruct((tok, feat), bf16),
        in_specs=[any_spec] * 10 + [vmem] * 7,
        out_specs=vmem,
        scratch_shapes=scratch,
        compiler_params=pltpu.CompilerParams(
            collective_id=0, has_side_effects=True, vmem_limit_bytes=60 * 1024 * 1024
        ),
        name="mixer",
    )(
        x, conv_in_a, conv_in_b, query_w, key_w, value_w, out_gate_w, pointwise_w, gla_out_w,
        decay_extra[0], norm_gain[None], forget_first_factor.T, decay_w, decay_bias[None],
        conv_kernel, conv_gain[None], head_gain[None],
    )
    return out[None]


def fits(inputs, conv_in_a, query_w, value_w):
    n_sp, n_tp, n_fs = lax.axis_size("sp"), lax.axis_size("tp"), lax.axis_size("fs")
    widths = (conv_in_a.shape[1], 2 * query_w.shape[1], value_w.shape[1])
    return (
        (n_sp, n_fs, n_tp) == (4, 4, 2)
        and inputs.shape[0] == 1
        and inputs.shape[1] % CHUNK == 0
        and all(w == 128 * n_fs for w in widths)
    )


def from_behind(value, axis, by):
    length = lax.axis_size(axis)
    pairs = [(i, i + by) for i in range(length) if 0 <= i + by < length]
    return lax.ppermute(value, axis, pairs)


def by_tokens(
    inputs,
    norm_gain,
    conv_in_a,
    conv_in_b,
    query_w,
    key_w,
    value_w,
    out_gate_w,
    pointwise_w,
    gla_out_w,
    forget_first_factor,
    decay_w,
    decay_bias,
    decay_extra,
    conv_kernel,
    conv_gain,
    head_gain,
):
    collected = (
        lax.all_gather(conv_in_a, ("sp", "fs"), axis=0, tiled=True),
        lax.all_gather(conv_in_b, ("sp", "fs"), axis=0, tiled=True),
        lax.all_gather(query_w, ("sp", "fs"), axis=0, tiled=True),
        lax.all_gather(key_w, ("sp", "fs"), axis=0, tiled=True),
        lax.all_gather(value_w, ("sp", "fs"), axis=0, tiled=True),
        lax.all_gather(out_gate_w, ("sp", "fs"), axis=0, tiled=True),
        lax.all_gather(pointwise_w, ("sp", "fs"), axis=0, tiled=True),
        lax.all_gather(gla_out_w, ("sp", "fs"), axis=0, tiled=True),
    )
    (
        conv_a_full,
        conv_b_full,
        query_full,
        key_full,
        value_full,
        gate_full,
        pointwise_full,
        gla_out_full,
    ) = collected
    tok_rows = inputs[0]
    token_count = tok_rows.shape[0]
    in_weights = (
        conv_a_full,
        conv_b_full,
        query_full,
        key_full,
        value_full,
        gate_full,
        forget_first_factor,
    )
    segment_values = lax.all_gather(tok_rows, "tp", axis=1, tiled=True).astype(jnp.float32)
    scaled = (segment_values * norm_gain).astype(jnp.bfloat16)
    sums = tuple(
        (jnp.dot(scaled, weight, preferred_element_type=jnp.float32) for weight in in_weights)
    )
    sums, squares = (sums, jnp.sum(segment_values * segment_values, axis=1))
    row_scale = lax.rsqrt(squares / norm_gain.shape[0] + 1e-06)[:, None]
    conv_a, conv_b, queries, keys, values, out_gate, low_rank = [
        (running * row_scale).astype(jnp.bfloat16) for running in sums
    ]
    gated = (conv_a.astype(jnp.float32) * jax.nn.sigmoid(conv_b.astype(jnp.float32))).astype(
        jnp.bfloat16
    )
    reach = conv_kernel.shape[0] - 1
    earlier = from_behind(gated[token_count - reach :], "sp", 1)
    extended = jnp.concatenate([earlier, gated], axis=0).astype(jnp.float32)
    tp_index = lax.axis_index("tp")
    channels = gated.shape[1]
    kernel = lax.dynamic_slice_in_dim(conv_kernel, tp_index * channels, channels, 1)
    convolved = jnp.zeros((token_count, channels), jnp.float32)
    for offset in range(reach + 1):
        convolved = convolved + kernel[offset] * extended[offset : offset + token_count]
    channel_sum, channel_squares = lax.psum(
        (jnp.sum(convolved, axis=1), jnp.sum(convolved * convolved, axis=1)), "tp"
    )
    total_channels = conv_gain.shape[0]
    average = channel_sum / total_channels
    spread_squared_mean = channel_squares / total_channels - average * average
    gain_part = lax.dynamic_slice_in_dim(conv_gain, tp_index * channels, channels)
    normed = (
        (convolved - average[:, None]) * lax.rsqrt(spread_squared_mean + 1e-05)[:, None] * gain_part
    )
    conv_act = jax.nn.silu(normed).astype(jnp.bfloat16)
    key_width = keys.shape[1]
    head_count = key_width // DK
    decay_part = lax.dynamic_slice_in_dim(decay_w, tp_index * key_width, key_width, 1)
    bias_part = lax.dynamic_slice_in_dim(decay_bias, tp_index * key_width, key_width)
    pre_decay = jnp.dot(low_rank, decay_part, preferred_element_type=jnp.float32) + bias_part
    log_decay = jax.nn.log_sigmoid(pre_decay) / 16.0 + decay_extra[0]
    block_count = token_count // BLOCK
    highest = lax.Precision.HIGHEST

    def split_blocks(array_operand, width):
        return array_operand.reshape(block_count, BLOCK, head_count, width).transpose(0, 2, 1, 3)

    q_blocks = split_blocks(queries.astype(jnp.float32), DK) * DK ** (-0.5)
    k_blocks = split_blocks(keys.astype(jnp.float32), DK)
    v_blocks = split_blocks(values.astype(jnp.float32), DV)
    prefix_running_sum = jnp.cumsum(split_blocks(log_decay, DK), axis=2)
    causal = jnp.tril(jnp.ones((BLOCK, BLOCK), dtype=bool))
    spread = prefix_running_sum[:, :, :, None, :] - prefix_running_sum[:, :, None, :, :]
    weights_in = jnp.exp(jnp.where(causal[:, :, None], spread, -jnp.inf))
    scores = jnp.einsum("nhid,nhjd,nhijd->nhij", q_blocks, k_blocks, weights_in, precision=highest)
    inner = jnp.einsum("nhij,nhjv->nhiv", scores, v_blocks, precision=highest)
    block_total = prefix_running_sum[:, :, -1]
    block_state = jnp.einsum(
        "nhjd,nhjv->nhdv",
        k_blocks * jnp.exp(block_total[:, :, None] - prefix_running_sum),
        v_blocks,
        precision=highest,
    )

    def advance(state, block_pair):
        decay_row, added_share_term = block_pair
        return (jnp.exp(decay_row)[..., None] * state + added_share_term, state)

    local_final, local_entering = lax.scan(
        advance, jnp.zeros((head_count, DK, DV), jnp.float32), (block_total, block_state)
    )
    device_total = jnp.sum(block_total, axis=0)
    totals = lax.all_gather(device_total[None], "sp", axis=0, tiled=True)
    running_totals = jnp.cumsum(totals, axis=0)
    sp_index = lax.axis_index("sp")
    before = lax.dynamic_index_in_dim(
        running_totals, sp_index, 0, False
    ) - lax.dynamic_index_in_dim(totals, sp_index, 0, False)
    piece = lax.all_gather(local_final[None], "sp", axis=0, tiled=True)
    number = piece.shape[0]
    anchor = jnp.arange(number, dtype=jnp.int32)
    exponent = jnp.where(
        (anchor < sp_index)[:, None, None], before[None] - running_totals, -jnp.inf
    )
    entering = jnp.einsum("nhd,nhdv->hdv", jnp.exp(exponent), piece, precision=highest)
    passed = jnp.exp(jnp.cumsum(block_total, axis=0) - block_total)
    entering_blocks = passed[..., None] * entering[None] + local_entering
    outer = jnp.einsum(
        "nhid,nhdv->nhiv",
        q_blocks * jnp.exp(prefix_running_sum),
        entering_blocks,
        precision=highest,
    )
    head_output = inner + outer
    normed_heads = (
        head_output
        * lax.rsqrt(jnp.mean(head_output * head_output, axis=-1, keepdims=True) + 1e-06)
        * head_gain
    )
    gla_rows = normed_heads.transpose(0, 2, 1, 3).reshape(token_count, head_count * DV)
    gla_act = (gla_rows * jax.nn.silu(out_gate.astype(jnp.float32))).astype(jnp.bfloat16)
    contract = (((1,), (1,)), ((), ()))
    conv_term = lax.dot_general(
        pointwise_full, conv_act, contract, preferred_element_type=jnp.float32
    )
    summed = lax.psum_scatter(
        (
            conv_term
            + lax.dot_general(gla_out_full, gla_act, contract, preferred_element_type=jnp.float32)
        ).astype(jnp.bfloat16),
        "tp",
        scatter_dimension=0,
        tiled=True,
    ).astype(jnp.float32)
    return (tok_rows.astype(jnp.float32) + summed.T).astype(jnp.bfloat16)[None]


def shards(*args):
    if fits(args[0], args[2], args[4], args[6]):
        return by_segments(*args)
    return by_tokens(*args)


def solution(mesh):
    by_rows = P(("sp", "fs"), "tp")
    return jax.shard_map(
        shards,
        mesh=mesh,
        in_specs=(P("fs", "sp", "tp"), P())
        + (by_rows,) * 8
        + (P(), P(), P(), P("fs", "sp", "tp"), P(), P(), P()),
        out_specs=P("fs", "sp", "tp"),
        check_vma=False,
    )
```

```python
import jax
import jax.numpy as jnp
from jax import lax
from jax.experimental import pallas as pl
from jax.experimental.pallas import tpu as pltpu
from jax.sharding import PartitionSpec as P


DK = 32
DV = 64
SUB = 16
BLOCK = 64


ROOT = 5
OUT_ITEMS = 2
CHUNK = 128
MESH_IDS = pl.DeviceIdType.MESH


def fused_kernel(
    x_hbm, wa, wb, wq, wk, wv, wg, pw, go, dex_hbm,
    ng_hbm, ff_hbm, dw_hbm, db_hbm, ck_hbm, cg_hbm, hg_hbm,
    o_hbm,
    ng_ref, ff_ref, dw_ref, db_ref, ck_ref, cg_ref, hg_ref, obuf,
    xbuf, xs, rs, wbuf, qraw, kraw, qkst, wobuf, debuf, ext, hsend, hrecv, conv, stats, comb, actbuf,
    qkb, vb, ld, raw, qseg, state_ref, base_ref, sfin, tots, stbuf, totbuf, sin_ref,
    pbuf, prcv, osum, rbuf,
    sent, xl, xi, xd, al, ar, zr, ol, dl, dr, pl_in, o_out, hr, tr, vr, cr, gr, pr, orc,
):
    f32, bf16 = jnp.float32, jnp.bfloat16
    z, f, c = lax.axis_index("sp"), lax.axis_index("fs"), lax.axis_index("tp")
    nz, nf, nc = lax.axis_size("sp"), lax.axis_size("fs"), lax.axis_size("tp")
    tok, feat = x_hbm.shape
    half = tok // 2
    rows_w = wa.shape[0]
    layer_rows = nf * rows_w
    cw = wa.shape[1] // nf
    kw = wq.shape[1] // nf
    vw = wv.shape[1] // nf
    total = nf * tok
    kin = wbuf.shape[0]
    pwc = pw.shape[1]
    channels = nc * nf * cw
    other = 1 - c
    xn = f + 1 - 2 * lax.rem(f, 2)
    yn = f + 2 - 4 * (f // 2)
    dg = nf - 1 - f
    peers = (xn, yn, dg)

    def remote(src, dst, recv, dev):
        return pltpu.make_async_remote_copy(
            src_ref=src, dst_ref=dst, send_sem=sent, recv_sem=recv,
            device_id=dev, device_id_type=MESH_IDS,
        )

    def arrived(dst, recv):
        remote(dst, dst, recv, (z, f, other)).wait_recv()

    def lanes(at, width):
        return pl.ds(pl.multiple_of(at * width, width), width)

    def xr(seq, h):
        row = pl.ds(pl.multiple_of(seq * tok + h * half, half), half)
        return xbuf.at[row, lanes(c, feat)]

    def xr_other(seq, h):
        row = pl.ds(pl.multiple_of(seq * tok + h * half, half), half)
        return xbuf.at[row, lanes(other, feat)]

    def item(i, b):
        if i < ROOT:
            row = pl.ds(pl.multiple_of(b * layer_rows, layer_rows), layer_rows)
            return wbuf.at[row, pl.ds(i * cw, cw)]
        return wobuf.at[b, :, pl.ds((i - ROOT) * pwc, pwc)]

    def up(i, b):
        return remote(item(i, b), item(i, b), zr.at[i, b], (z + 1, f, c))

    def down(i, b):
        return remote(item(i, b), item(i, b), zr.at[i, b], (z - 1, f, c))

    items = ROOT + OUT_ITEMS
    sources = {0: wa, 1: wb, 3: wv, 4: wg}
    my_rows = pl.ds(pl.multiple_of((z * nf + f) * rows_w, rows_w), rows_w)

    barrier = pltpu.get_barrier_semaphore()
    me = f * nc + c
    group = nf * nc
    for k in range(1, group):
        t = lax.rem(me + k, group)
        pl.semaphore_signal(barrier, inc=1, device_id=(z, t // nc, lax.rem(t, nc)), device_id_type=MESH_IDS)
    for k in range(1, nz):
        pl.semaphore_signal(barrier, inc=1, device_id=(lax.rem(z + k, nz), f, c), device_id_type=MESH_IDS)
    params = [
        pltpu.make_async_copy(src, dst, pl_in.at[n])
        for n, (src, dst) in enumerate(
            (
                (ng_hbm, ng_ref), (ff_hbm, ff_ref), (dw_hbm, dw_ref), (db_hbm, db_ref),
                (ck_hbm, ck_ref), (cg_hbm, cg_ref), (hg_hbm, hg_ref),
            )
        )
    ]

    own_x = [
        pltpu.make_async_copy(x_hbm.at[pl.ds(h * half, half), :], xr(f, h), xl.at[h])
        for h in range(2)
    ]
    qk_load = [
        pltpu.make_async_copy(wq, qraw, ol.at[2]),
        pltpu.make_async_copy(wk, kraw, ol.at[3]),
    ]
    own_w = {
        g: pltpu.make_async_copy(
            w.at[:, lanes(f, cw)], wbuf.at[my_rows, pl.ds(g * cw, cw)], al.at[g]
        )
        for g, w in sources.items()
    }
    own_o = [
        pltpu.make_async_copy(pw, item(ROOT, z), ol.at[0]),
        pltpu.make_async_copy(go, item(ROOT + 1, z), ol.at[1]),
    ]
    own_d = pltpu.make_async_copy(dex_hbm.at[:, lanes(f // 2, 2 * kw)], debuf.at[f], dl)
    for copy in qk_load:
        copy.start()
    for g in sources:
        own_w[g].start()
    for copy in own_x + own_o + [own_d] + params:
        copy.start()

    for copy in qk_load:
        copy.wait()
    for j in range(nf):
        qkst[j] = jnp.concatenate(
            [qraw[:, j * kw : (j + 1) * kw], kraw[:, j * kw : (j + 1) * kw]], axis=1
        )
    wbuf[my_rows, pl.ds(2 * cw, cw)] = qkst[f]
    pl.semaphore_wait(barrier, group - 1 + nz - 1)

    def exchange(g):
        out = []
        for p in peers:
            src = qkst.at[p] if g == 2 else sources[g].at[:, lanes(p, cw)]
            dst = wbuf.at[my_rows, pl.ds(g * cw, cw)]
            out.append(remote(src, dst, ar.at[g, f], (z, p, c)))
        return out

    x_to_x = [
        remote(x_hbm.at[pl.ds(h * half, half), :], xr(f, h), xi.at[f, h], (z, xn, c))
        for h in range(2)
    ]
    x_to_y = [
        remote(x_hbm.at[pl.ds(h * half, half), :], xr(f, h), xi.at[f, h], (z, yn, c))
        for h in range(2)
    ]
    x_over = [
        remote(x_hbm.at[pl.ds(h * half, half), :], xr(f, h), xd.at[f, h], (z, f, other))
        for h in range(2)
    ]

    def over(seq, h):
        return remote(xr(seq, h), xr(seq, h), xd.at[seq, h], (z, f, other))

    decay_out = [
        remote(
            dex_hbm.at[:, lanes(p // 2, 2 * kw)], debuf.at[f], dr.at[f], (z, p, c)
        )
        for p in peers
    ]

    sends = []

    def start(*copies):
        for copy in copies:
            copy.start()
            sends.append(copy)


    def own(i):
        if i < ROOT:
            if i in own_w:
                own_w[i].wait()
            for p in peers:
                arrived(
                    wbuf.at[
                        pl.ds(pl.multiple_of((z * nf + p) * rows_w, rows_w), rows_w),
                        pl.ds(i * cw, cw),
                    ],
                    ar.at[i, p],
                )
        else:
            own_o[i - ROOT].wait()

        @pl.when(z < nz - 1)
        def _():
            up(i, z).start()

        @pl.when(z > 0)
        def _():
            down(i, z).start()

    def relay(i, d):
        @pl.when(z >= d)
        def _():
            arrived(item(i, z - d), zr.at[i, z - d])

            @pl.when(z < nz - 1)
            def _():
                up(i, z - d).start()

        @pl.when(z + d < nz)
        def _():
            arrived(item(i, z + d), zr.at[i, z + d])

            @pl.when(z > 0)
            def _():
                down(i, z + d).start()

    start(*exchange(0))
    own(5)
    start(*exchange(1))
    start(x_to_x[0], x_to_y[1], *x_over)
    own(0)
    start(*exchange(2))
    start(x_to_x[1], x_to_y[0])
    start(*exchange(3))
    own(1)
    relay(0, 1)

    arrived(xr(xn, 0), xi.at[xn, 0])
    start(
        remote(xr(xn, 0), xr(xn, 0), xi.at[xn, 0], (z, yn, c)),
        over(xn, 0),
    )
    arrived(xr(yn, 1), xi.at[yn, 1])
    start(
        remote(xr(yn, 1), xr(yn, 1), xi.at[yn, 1], (z, xn, c)),
        over(yn, 1),
    )
    start(*exchange(4))
    start(*decay_out)
    own(2)
    relay(0, 2)
    relay(1, 1)

    step_rows = 32

    def scale(seq):
        def body(r, carry):
            row = pl.ds(pl.multiple_of(seq * tok + r * step_rows, step_rows), step_rows)
            value = xbuf[row, :].astype(f32)
            square = jnp.sum(value * value, axis=1, keepdims=True)
            rs[row, :] = jnp.broadcast_to(
                lax.rsqrt(square / (nc * feat) + 1e-06), (step_rows, rs.shape[1])
            )
            xs[row, :] = (value * ng_ref[...]).astype(bf16)
            return carry

        lax.fori_loop(0, tok // step_rows, body, 0)

    for copy in own_x + params:
        copy.wait()
    for h in range(2):
        arrived(xr_other(f, h), xd.at[f, h])
    scale(f)
    arrived(xr(xn, 1), xi.at[xn, 1])
    arrived(xr(yn, 0), xi.at[yn, 0])
    start(over(xn, 1), over(yn, 0))
    relay(1, 2)
    own(3)
    for p in (xn, yn):
        for h in range(2):
            arrived(xr_other(p, h), xd.at[p, h])
        scale(p)
    relay(0, 3)
    relay(1, 3)
    relay(2, 1)
    arrived(xr(dg, 0), xi.at[dg, 0])
    arrived(xr(dg, 1), xi.at[dg, 1])
    start(over(dg, 0), over(dg, 1))
    for h in range(2):
        arrived(xr_other(dg, h), xd.at[dg, h])
    scale(dg)

    def project(seq, first, width):
        row = pl.ds(pl.multiple_of(seq * tok, tok), tok)
        out = jnp.dot(
            xs[row, :], wbuf[:, first : first + width], preferred_element_type=f32
        )
        return (out * rs[row, 0:1]).astype(bf16)

    halo = 32
    taps = ck_ref.shape[0]

    def conv_in(seq, carry):
        both = project(seq, 0, 2 * cw).astype(f32)
        gated = both[:, :cw] * jax.nn.sigmoid(both[:, cw:])
        low = gated.astype(bf16)
        ext[seq, halo : halo + tok, :] = low.astype(f32)
        hsend[seq] = low[tok - halo :]
        return carry

    lax.fori_loop(0, nf, conv_in, 0)
    halo_out = remote(hsend, hrecv, hr, (z + 1, f, c))

    @pl.when(z < nz - 1)
    def _():
        halo_out.start()

    relay(2, 2)
    own(4)

    part = c * (nf // 2) + f // 2
    odd = lax.rem(f, 2) == 1
    dw2 = dw_ref[:, lanes(part, 2 * kw)].astype(f32)
    dw_own = jnp.where(odd, dw2[:, kw:], dw2[:, :kw]).astype(bf16)
    db2 = db_ref[:, lanes(part, 2 * kw)]
    db_own = jnp.where(odd, db2[:, kw:], db2[:, :kw])
    own_d.wait()
    for p in peers:
        arrived(debuf.at[p], dr.at[p])

    def decay(seq, carry):
        row = pl.ds(pl.multiple_of(seq * tok, tok), tok)
        low = lax.dot_general(
            xs[row, :], ff_ref[...], (((1,), (1,)), ((), ())), preferred_element_type=f32
        )
        low = (low * rs[row, 0:1]).astype(bf16)
        pre = jnp.dot(low, dw_own, preferred_element_type=f32) + db_own
        extra = debuf[seq]
        extra = jnp.where(odd, extra[:, kw:], extra[:, :kw])
        ld[row, :] = jax.nn.log_sigmoid(pre) / 16.0 + extra
        return carry

    lax.fori_loop(0, nf, decay, 0)
    relay(2, 3)

    def keys_in(seq, carry):
        qkb[pl.ds(pl.multiple_of(seq * tok, tok), tok), :] = project(seq, 2 * cw, cw)
        return carry

    lax.fori_loop(0, nf, keys_in, 0)

    @pl.when(z > 0)
    def _():
        arrived(hrecv, hr)
        ext[:, 0:halo, :] = hrecv[...].astype(f32)

    @pl.when(z == 0)
    def _():
        ext[:, 0:halo, :] = jnp.zeros((nf, halo, cw), f32)

    mine = c * nf + f
    tap_rows = 64
    lane = lax.broadcasted_iota(jnp.int32, (tok, cw), 1)

    def tap(seq, carry):
        kernel = ck_ref[:, lanes(mine, cw)]
        for r in range(tok // tap_rows):
            acc = jnp.zeros((tap_rows, cw), f32)
            for j in range(taps):
                at = halo - (taps - 1) + j + r * tap_rows
                acc = acc + kernel[j : j + 1, :] * ext[seq, at : at + tap_rows, :]
            conv[pl.ds(pl.multiple_of(seq * tok + r * tap_rows, tap_rows), tap_rows), :] = acc
        row = pl.ds(pl.multiple_of(seq * tok, tok), tok)
        value = conv[row, :]
        mean = jnp.sum(value, axis=1, keepdims=True) / cw
        spread = value - mean
        second = jnp.sum(spread * spread, axis=1, keepdims=True)
        both = jnp.where(lane == 0, mean, jnp.where(lane == 1, second, 0.0))
        stats[me, :, pl.ds(pl.multiple_of(seq * tok, tok), tok)] = both.T[0:8, :]
        return carry

    lax.fori_loop(0, nf, tap, 0)
    relay(3, 1)
    for k in range(1, group):
        t = lax.rem(me + k, group)
        start(
            remote(
                stats.at[me], stats.at[me], tr.at[me], (z, t // nc, lax.rem(t, nc))
            )
        )
    for k in range(1, group):
        t = lax.rem(me + k, group)
        arrived(stats.at[t], tr.at[t])
    every = stats[...]
    means = every[:, 0, :]
    mean = jnp.sum(means, axis=0, keepdims=True) / group
    off = means - mean
    second = jnp.sum(every[:, 1, :] + cw * off * off, axis=0, keepdims=True)
    inverse = lax.rsqrt(second / channels + 1e-05)
    comb[0:1, :] = mean
    comb[1:2, :] = inverse

    def conv_out(seq, carry):
        row = pl.ds(pl.multiple_of(seq * tok, tok), tok)
        flat = comb[0:2, row]
        cols = jnp.concatenate([flat, jnp.zeros((cw - 2, tok), f32)], axis=0).T
        normed = (conv[row, :] - cols[:, 0:1]) * cols[:, 1:2] * cg_ref[:, lanes(mine, cw)]
        actbuf[row, lanes(f, cw)] = (normed * jax.nn.sigmoid(normed)).astype(bf16)
        return carry

    def act_block(at):
        return actbuf.at[:, lanes(at, cw)]

    relay(3, 2)

    def values_in(seq, carry):
        vb[pl.ds(pl.multiple_of(seq * tok, tok), tok), :] = project(seq, 3 * cw, cw)
        return carry

    relay(3, 3)
    lax.fori_loop(0, nf, values_in, 0)

    spread_m = (
        lax.broadcasted_iota(jnp.int32, (kw, vw), 0) // DK
        == lax.broadcasted_iota(jnp.int32, (kw, vw), 1) // DV
    ).astype(bf16)
    own_mask = (
        lax.broadcasted_iota(jnp.int32, (vw, kw), 1) // DK
        == lax.broadcasted_iota(jnp.int32, (vw, kw), 0) // DV
    )
    place = lax.rem(lax.broadcasted_iota(jnp.int32, (CHUNK, kw), 0), SUB)
    per_seq = tok // CHUNK

    def attend(n, carry):
        at = pl.ds(pl.multiple_of(n * CHUNK, CHUNK), CHUNK)
        qk = qkb[at, :].astype(f32)
        q = qk[:, :kw] * DK ** (-0.5)
        k = qk[:, kw:]
        v = vb[at, :].astype(f32)
        cum = ld[at, :]
        step = 1
        while step < SUB:
            cum = cum + jnp.where(place >= step, pltpu.roll(cum, step, 0), 0.0)
            step *= 2
        acc = jnp.dot((q * k).astype(bf16), spread_m, preferred_element_type=f32) * v
        for lag in range(1, SUB):
            decays = jnp.exp(jnp.where(place >= lag, cum - pltpu.roll(cum, lag, 0), -jnp.inf))
            term = (q * pltpu.roll(k, lag, 0) * decays).astype(bf16)
            score = jnp.dot(term, spread_m, preferred_element_type=f32)
            acc = acc + score * pltpu.roll(v, lag, 0)
        q_f = q * jnp.exp(cum)
        q_in = q_f.astype(bf16)
        v_low = v.astype(bf16)
        first = lax.rem(n, per_seq) == 0
        state = jnp.where(first, 0.0, state_ref[...])
        base = jnp.where(first, 0.0, base_ref[0:1, :])
        outer, seg = [], []
        for m in range(CHUNK // SUB):
            part = slice(m * SUB, (m + 1) * SUB)
            last = cum[(m + 1) * SUB - 1 : (m + 1) * SUB]
            k_out = (k[part] * jnp.exp(last - cum[part])).astype(bf16)
            outer.append(
                lax.dot_general(
                    q_in[part], state.astype(bf16), (((1,), (1,)), ((), ())),
                    preferred_element_type=f32,
                )
            )
            added = lax.dot_general(
                v_low[part], k_out, (((0,), (0,)), ((), ())), preferred_element_type=f32
            )
            seg.append(q_f[part] * jnp.exp(base))
            state = state * jnp.exp(last) + jnp.where(own_mask, added, 0.0)
            base = base + last
        state_ref[...] = state
        base_ref[...] = jnp.broadcast_to(base, base_ref.shape)
        sfin[n // per_seq] = state
        tots[n // per_seq] = jnp.broadcast_to(base, base_ref.shape)
        raw[at, :] = acc + jnp.concatenate(outer, axis=0)
        qseg[at, :] = jnp.concatenate(seg, axis=0).astype(bf16)

        @pl.when(n == 1)
        def _():
            relay(4, 1)

        return carry

    lax.fori_loop(0, total // CHUNK, attend, 0)
    vh = vw // 2
    for p in range(nf // 2):
        a, b = sfin[2 * p], sfin[2 * p + 1]
        stbuf[z, p] = jnp.concatenate([a[:vh] + a[vh:], b[:vh] + b[vh:]], axis=1).astype(bf16)
        totbuf[z, p] = jnp.concatenate([tots[2 * p], tots[2 * p + 1]], axis=1)

    def state_out(d):
        dev = (z + d, f, c)
        return (
            remote(stbuf.at[z], stbuf.at[z], vr.at[0, z], dev),
            remote(totbuf.at[z], totbuf.at[z], vr.at[1, z], dev),
        )

    for d in range(1, nz):
        @pl.when(z + d < nz)
        def _():
            for copy in state_out(d):
                copy.start()

    relay(4, 2)
    own(6)
    lax.fori_loop(0, nf, conv_out, 0)
    for n, p in enumerate(peers):
        start(remote(act_block(f), act_block(f), cr.at[f], (z, p, c)))
    relay(5, 1)
    relay(4, 3)

    sin_ref[...] = jnp.zeros_like(sin_ref)
    for b in range(nz - 1):
        @pl.when(z > b)
        def _():
            arrived(stbuf.at[b], vr.at[0, b])
            arrived(totbuf.at[b], vr.at[1, b])
            sin_ref[...] = sin_ref[...] * jnp.exp(totbuf[b, :, 0:1, :]) + stbuf[b].astype(f32)
    head_mean = jnp.where(
        lax.broadcasted_iota(jnp.int32, (vw, vw), 0) // DV
        == lax.broadcasted_iota(jnp.int32, (vw, vw), 1) // DV,
        1.0 / DV,
        0.0,
    ).astype(f32)
    gain = jnp.concatenate([hg_ref[...]] * (vw // DV), axis=1)
    for seq in range(nf):
        row = slice(seq * tok, (seq + 1) * tok)
        lo = (seq % 2) * kw
        packed = sin_ref[seq // 2][:, lo : lo + kw]
        state = jnp.where(own_mask, jnp.concatenate([packed, packed], axis=0), 0.0).astype(bf16)
        full = raw[row, :] + lax.dot_general(
            qseg[row, :], state, (((1,), (1,)), ((), ())), preferred_element_type=f32
        )
        mean = jnp.dot(
            full * full, head_mean, preferred_element_type=f32, precision=lax.Precision.HIGHEST
        )
        gate = project(seq, 4 * cw, cw).astype(f32)
        actbuf[row, lanes(nf + f, cw)] = (
            full * lax.rsqrt(mean + 1e-06) * gain * (gate * jax.nn.sigmoid(gate))
        ).astype(bf16)
    for n, p in enumerate(peers):
        start(remote(act_block(nf + f), act_block(nf + f), gr.at[f], (z, p, c)))
    relay(5, 2)

    near = jnp.where(z < nz // 2, z, nz - 1 - z)
    out_rows = pw.shape[0]
    slot_cols = nf * out_rows
    per_core = nz // nc

    def block_of(k):
        o = (near, 1 - near, 2, 3)[k]
        return jnp.where(z < nz // 2, o, nz - 1 - o)

    def rows_of(p):
        return pl.ds(pl.multiple_of(p * tok, tok), tok)

    def turn(j):
        return jnp.where(j == 0, dg, jnp.where(j == 1, xn, jnp.where(j == 2, yn, f)))

    def over_part(k, slot, p):
        return remote(
            pbuf.at[k, rows_of(p), :], prcv.at[slot, rows_of(p), :],
            pr.at[slot, p], (z, f, other),
        )

    def out_copy(slot, p):
        return remote(
            osum.at[slot, rows_of(p), :],
            rbuf.at[:, lanes(slot * nf + f, out_rows)],
            orc.at[slot, f], (z, p, c),
        )

    def block(k):
        b = block_of(k)
        slot = lax.rem(b, per_core)
        owner = b // per_core

        def multiply(j, carry):
            p = turn(j)
            out = lax.dot_general(
                actbuf[rows_of(p), :], wobuf[b], (((1,), (1,)), ((), ())),
                preferred_element_type=f32,
            )
            pbuf[k, rows_of(p), :] = out.astype(bf16)

            @pl.when(owner != c)
            def _():
                over_part(k, slot, p).start()

            return carry

        lax.fori_loop(0, nf, multiply, 0)

        def gather(j, carry):
            p = turn(j)
            arrived(prcv.at[slot, rows_of(p), :], pr.at[slot, p])
            osum[slot, rows_of(p), :] = (
                pbuf[k, rows_of(p), :].astype(f32) + prcv[slot, rows_of(p), :].astype(f32)
            ).astype(bf16)

            @pl.when(j < nf - 1)
            def _():
                out_copy(slot, p).start()

            return carry

        @pl.when(owner == c)
        def _():
            lax.fori_loop(0, nf, gather, 0)
            rbuf[:, lanes(slot * nf + f, out_rows)] = osum[slot, rows_of(f), :]

    def acts():
        for p in peers:
            arrived(act_block(p), cr.at[p])
            arrived(act_block(nf + p), gr.at[p])

    ends = (z == 0) | (z == nz - 1)

    @pl.when(ends)
    def _():
        relay(5, 3)
        acts()
        block(0)
        for k in range(1, nz):
            relay(6, k)
            block(k)

    @pl.when(jnp.logical_not(ends))
    def _():
        for k in range(1, nz):
            relay(6, k)
        acts()
        for k in range(nz):
            block(k)

    first_slot = lax.rem(block_of(0), per_core)
    first_slot = jnp.where(c == z // per_core, first_slot, lax.rem(block_of(2), per_core))
    wide = nf * out_rows

    def out_half(slot):
        return pltpu.make_async_copy(
            obuf.at[:, lanes(slot, wide)], o_hbm.at[:, lanes(slot, wide)], o_out.at[slot]
        )

    for n in range(per_core):
        slot = first_slot if n == 0 else per_core - 1 - first_slot
        for p in peers:
            arrived(rbuf.at[:, lanes(slot * nf + p, out_rows)], orc.at[slot, p])
        own_part = xbuf[rows_of(f), lanes(c * per_core + slot, wide)].astype(f32)
        obuf[:, lanes(slot, wide)] = (
            own_part + rbuf[:, lanes(slot, wide)].astype(f32)
        ).astype(bf16)
        out_half(slot).start()

    for slot in range(per_core):
        out_half(slot).wait()
    for copy in sends:
        copy.wait_send()
    for i in range(items):
        for b in range(nz):
            @pl.when((z < nz - 1) & (z >= b))
            def _():
                up(i, b).wait_send()

            @pl.when((z > 0) & (z <= b))
            def _():
                down(i, b).wait_send()

    @pl.when(z < nz - 1)
    def _():
        halo_out.wait_send()

    for d in range(1, nz):
        @pl.when(z + d < nz)
        def _():
            for copy in state_out(d):
                copy.wait_send()
    for k in range(nz):
        b = block_of(k)
        slot = lax.rem(b, per_core)

        @pl.when(b // per_core != c)
        def _():
            for p in range(nf):
                over_part(k, slot, p).wait_send()

        @pl.when(b // per_core == c)
        def _():
            for p in peers:
                out_copy(slot, p).wait_send()


def by_segments(
    inputs, norm_gain, conv_in_a, conv_in_b, query_w, key_w, value_w, out_gate_w,
    pointwise_w, gla_out_w, forget_first_factor, decay_w, decay_bias, decay_extra,
    conv_kernel, conv_gain, head_gain,
):
    f32, bf16 = jnp.float32, jnp.bfloat16
    nz, nf, nc = lax.axis_size("sp"), lax.axis_size("fs"), lax.axis_size("tp")
    x = inputs[0]
    tok, feat = x.shape
    total = nf * tok
    rows_w = conv_in_a.shape[0]
    kin = nz * nf * rows_w
    cw = conv_in_a.shape[1] // nf
    kw = query_w.shape[1] // nf
    vw = value_w.shape[1] // nf
    pwc = pointwise_w.shape[1]
    out_rows = pointwise_w.shape[0]
    group = nf * nc
    dma = pltpu.SemaphoreType.DMA
    items = ROOT + OUT_ITEMS
    any_spec = pl.BlockSpec(memory_space=pl.ANY)
    V = pltpu.VMEM
    flat = (
        norm_gain[None], forget_first_factor.T, decay_w, decay_bias[None],
        conv_kernel, conv_gain[None], head_gain[None],
    )
    scratch = [V(a.shape, a.dtype) for a in flat] + [
        V((tok, feat), bf16),
        V((total, nc * feat), bf16), V((total, nc * feat), bf16), V((total, 128), f32),
        V((kin, ROOT * cw), bf16), V((rows_w, nf * kw), bf16), V((rows_w, nf * kw), bf16),
        V((nf, rows_w, cw), bf16), V((nz, out_rows, OUT_ITEMS * pwc), bf16),
        V((nf, tok, 2 * kw), f32), V((nf, tok + 32, cw), f32), V((nf, 32, cw), bf16), V((nf, 32, cw), bf16), V((total, cw), f32),
        V((group, 8, total), f32), V((8, total), f32), V((total, 2 * nf * cw), bf16),
        V((total, cw), bf16), V((total, vw), bf16), V((total, kw), f32), V((total, vw), f32),
        V((total, kw), bf16), V((vw, kw), f32), V((8, kw), f32), V((nf, vw, kw), f32),
        V((nf, 8, kw), f32), V((nz, nf // 2, vw // 2, 2 * kw), bf16),
        V((nz, nf // 2, 8, 2 * kw), f32),
        V((nf // 2, vw // 2, 2 * kw), f32),
        V((nz, total, out_rows), bf16), V((nz // nc, total, out_rows), bf16),
        V((nz // nc, total, out_rows), bf16), V((tok, feat), bf16),
        dma, dma((2,)), dma((nf, 2)), dma((nf, 2)), dma((ROOT,)), dma((ROOT, nf)),
        dma((items, nz)), dma((4,)), dma, dma((nf,)), dma((len(flat),)), dma((nz // nc,)), dma,
        dma((group,)), dma((2, nz)), dma((nf,)), dma((nf,)), dma((nz // nc, nf)),
        dma((nz // nc, nf)),
    ]
    out = pl.pallas_call(
        fused_kernel,
        out_shape=jax.ShapeDtypeStruct((tok, feat), bf16),
        in_specs=[any_spec] * 17,
        out_specs=any_spec,
        scratch_shapes=scratch,
        compiler_params=pltpu.CompilerParams(
            collective_id=0, has_side_effects=True, vmem_limit_bytes=60 * 1024 * 1024
        ),
        name="mixer",
    )(
        x, conv_in_a, conv_in_b, query_w, key_w, value_w, out_gate_w, pointwise_w, gla_out_w,
        decay_extra[0], *flat,
    )
    return out[None]


def fits(inputs, conv_in_a, query_w, value_w):
    n_sp, n_tp, n_fs = lax.axis_size("sp"), lax.axis_size("tp"), lax.axis_size("fs")
    widths = (conv_in_a.shape[1], 2 * query_w.shape[1], value_w.shape[1])
    return (
        (n_sp, n_fs, n_tp) == (4, 4, 2)
        and inputs.shape[0] == 1
        and inputs.shape[1] % CHUNK == 0
        and all(w == 128 * n_fs for w in widths)
    )


def from_behind(value, axis, by):
    length = lax.axis_size(axis)
    pairs = [(i, i + by) for i in range(length) if 0 <= i + by < length]
    return lax.ppermute(value, axis, pairs)


def by_tokens(
    inputs,
    norm_gain,
    conv_in_a,
    conv_in_b,
    query_w,
    key_w,
    value_w,
    out_gate_w,
    pointwise_w,
    gla_out_w,
    forget_first_factor,
    decay_w,
    decay_bias,
    decay_extra,
    conv_kernel,
    conv_gain,
    head_gain,
):
    collected = (
        lax.all_gather(conv_in_a, ("sp", "fs"), axis=0, tiled=True),
        lax.all_gather(conv_in_b, ("sp", "fs"), axis=0, tiled=True),
        lax.all_gather(query_w, ("sp", "fs"), axis=0, tiled=True),
        lax.all_gather(key_w, ("sp", "fs"), axis=0, tiled=True),
        lax.all_gather(value_w, ("sp", "fs"), axis=0, tiled=True),
        lax.all_gather(out_gate_w, ("sp", "fs"), axis=0, tiled=True),
        lax.all_gather(pointwise_w, ("sp", "fs"), axis=0, tiled=True),
        lax.all_gather(gla_out_w, ("sp", "fs"), axis=0, tiled=True),
    )
    (
        conv_a_full,
        conv_b_full,
        query_full,
        key_full,
        value_full,
        gate_full,
        pointwise_full,
        gla_out_full,
    ) = collected
    tok_rows = inputs[0]
    token_count = tok_rows.shape[0]
    in_weights = (
        conv_a_full,
        conv_b_full,
        query_full,
        key_full,
        value_full,
        gate_full,
        forget_first_factor,
    )
    segment_values = lax.all_gather(tok_rows, "tp", axis=1, tiled=True).astype(jnp.float32)
    scaled = (segment_values * norm_gain).astype(jnp.bfloat16)
    sums = tuple(
        (jnp.dot(scaled, weight, preferred_element_type=jnp.float32) for weight in in_weights)
    )
    sums, squares = (sums, jnp.sum(segment_values * segment_values, axis=1))
    row_scale = lax.rsqrt(squares / norm_gain.shape[0] + 1e-06)[:, None]
    conv_a, conv_b, queries, keys, values, out_gate, low_rank = [
        (running * row_scale).astype(jnp.bfloat16) for running in sums
    ]
    gated = (conv_a.astype(jnp.float32) * jax.nn.sigmoid(conv_b.astype(jnp.float32))).astype(
        jnp.bfloat16
    )
    reach = conv_kernel.shape[0] - 1
    earlier = from_behind(gated[token_count - reach :], "sp", 1)
    extended = jnp.concatenate([earlier, gated], axis=0).astype(jnp.float32)
    tp_index = lax.axis_index("tp")
    channels = gated.shape[1]
    kernel = lax.dynamic_slice_in_dim(conv_kernel, tp_index * channels, channels, 1)
    convolved = jnp.zeros((token_count, channels), jnp.float32)
    for offset in range(reach + 1):
        convolved = convolved + kernel[offset] * extended[offset : offset + token_count]
    channel_sum, channel_squares = lax.psum(
        (jnp.sum(convolved, axis=1), jnp.sum(convolved * convolved, axis=1)), "tp"
    )
    total_channels = conv_gain.shape[0]
    average = channel_sum / total_channels
    spread_squared_mean = channel_squares / total_channels - average * average
    gain_part = lax.dynamic_slice_in_dim(conv_gain, tp_index * channels, channels)
    normed = (
        (convolved - average[:, None]) * lax.rsqrt(spread_squared_mean + 1e-05)[:, None] * gain_part
    )
    conv_act = jax.nn.silu(normed).astype(jnp.bfloat16)
    key_width = keys.shape[1]
    head_count = key_width // DK
    decay_part = lax.dynamic_slice_in_dim(decay_w, tp_index * key_width, key_width, 1)
    bias_part = lax.dynamic_slice_in_dim(decay_bias, tp_index * key_width, key_width)
    pre_decay = jnp.dot(low_rank, decay_part, preferred_element_type=jnp.float32) + bias_part
    log_decay = jax.nn.log_sigmoid(pre_decay) / 16.0 + decay_extra[0]
    block_count = token_count // BLOCK
    highest = lax.Precision.HIGHEST

    def split_blocks(array_operand, width):
        return array_operand.reshape(block_count, BLOCK, head_count, width).transpose(0, 2, 1, 3)

    q_blocks = split_blocks(queries.astype(jnp.float32), DK) * DK ** (-0.5)
    k_blocks = split_blocks(keys.astype(jnp.float32), DK)
    v_blocks = split_blocks(values.astype(jnp.float32), DV)
    prefix_running_sum = jnp.cumsum(split_blocks(log_decay, DK), axis=2)
    causal = jnp.tril(jnp.ones((BLOCK, BLOCK), dtype=bool))
    spread = prefix_running_sum[:, :, :, None, :] - prefix_running_sum[:, :, None, :, :]
    weights_in = jnp.exp(jnp.where(causal[:, :, None], spread, -jnp.inf))
    scores = jnp.einsum("nhid,nhjd,nhijd->nhij", q_blocks, k_blocks, weights_in, precision=highest)
    inner = jnp.einsum("nhij,nhjv->nhiv", scores, v_blocks, precision=highest)
    block_total = prefix_running_sum[:, :, -1]
    block_state = jnp.einsum(
        "nhjd,nhjv->nhdv",
        k_blocks * jnp.exp(block_total[:, :, None] - prefix_running_sum),
        v_blocks,
        precision=highest,
    )

    def advance(state, block_pair):
        decay_row, added_share_term = block_pair
        return (jnp.exp(decay_row)[..., None] * state + added_share_term, state)

    local_final, local_entering = lax.scan(
        advance, jnp.zeros((head_count, DK, DV), jnp.float32), (block_total, block_state)
    )
    device_total = jnp.sum(block_total, axis=0)
    totals = lax.all_gather(device_total[None], "sp", axis=0, tiled=True)
    running_totals = jnp.cumsum(totals, axis=0)
    sp_index = lax.axis_index("sp")
    before = lax.dynamic_index_in_dim(
        running_totals, sp_index, 0, False
    ) - lax.dynamic_index_in_dim(totals, sp_index, 0, False)
    piece = lax.all_gather(local_final[None], "sp", axis=0, tiled=True)
    number = piece.shape[0]
    anchor = jnp.arange(number, dtype=jnp.int32)
    exponent = jnp.where(
        (anchor < sp_index)[:, None, None], before[None] - running_totals, -jnp.inf
    )
    entering = jnp.einsum("nhd,nhdv->hdv", jnp.exp(exponent), piece, precision=highest)
    passed = jnp.exp(jnp.cumsum(block_total, axis=0) - block_total)
    entering_blocks = passed[..., None] * entering[None] + local_entering
    outer = jnp.einsum(
        "nhid,nhdv->nhiv",
        q_blocks * jnp.exp(prefix_running_sum),
        entering_blocks,
        precision=highest,
    )
    head_output = inner + outer
    normed_heads = (
        head_output
        * lax.rsqrt(jnp.mean(head_output * head_output, axis=-1, keepdims=True) + 1e-06)
        * head_gain
    )
    gla_rows = normed_heads.transpose(0, 2, 1, 3).reshape(token_count, head_count * DV)
    gla_act = (gla_rows * jax.nn.silu(out_gate.astype(jnp.float32))).astype(jnp.bfloat16)
    contract = (((1,), (1,)), ((), ()))
    conv_term = lax.dot_general(
        pointwise_full, conv_act, contract, preferred_element_type=jnp.float32
    )
    summed = lax.psum_scatter(
        (
            conv_term
            + lax.dot_general(gla_out_full, gla_act, contract, preferred_element_type=jnp.float32)
        ).astype(jnp.bfloat16),
        "tp",
        scatter_dimension=0,
        tiled=True,
    ).astype(jnp.float32)
    return (tok_rows.astype(jnp.float32) + summed.T).astype(jnp.bfloat16)[None]


def shards(*args):
    if fits(args[0], args[2], args[4], args[6]):
        return by_segments(*args)
    return by_tokens(*args)


def solution(mesh):
    by_rows = P(("sp", "fs"), "tp")
    return jax.shard_map(
        shards,
        mesh=mesh,
        in_specs=(P("fs", "sp", "tp"), P())
        + (by_rows,) * 8
        + (P(), P(), P(), P("fs", "sp", "tp"), P(), P(), P()),
        out_specs=P("fs", "sp", "tp"),
        check_vma=False,
    )
```

```python
import jax
import jax.numpy as jnp
from jax import lax
from jax.experimental import pallas as pl
from jax.experimental.pallas import tpu as pltpu
from jax.sharding import PartitionSpec as P


DK = 32
DV = 64
SUB = 16
BLOCK = 64


ROOT = 5
OUT_ITEMS = 3
CHUNK = 128
MESH_IDS = pl.DeviceIdType.MESH


def fused_kernel(
    x_hbm, wa, wb, wq, wk, wv, wg, pw, go, dex_hbm,
    ng_hbm, ff_hbm, dw_hbm, db_hbm, ck_hbm, cg_hbm, hg_hbm,
    o_hbm,
    ng_ref, ff_ref, dw_ref, db_ref, ck_ref, cg_ref, hg_ref,
    xbuf, xs, rs, wbuf, qraw, kraw, qkst, wobuf, debuf, ext, hsend, hrecv, conv, stats, comb, actbuf,
    qkb, vb, ld, raw, qseg, state_ref, base_ref, sfin, tots, stbuf, totbuf, sin_ref,
    pbuf, prcv, osum,
    sent, xl, xi, xd, al, ar, zr, ol, dl, dr, pl_in, o_out, hr, tr, vr, cr, gr, pr, orc,
):
    f32, bf16 = jnp.float32, jnp.bfloat16
    z, f, c = lax.axis_index("sp"), lax.axis_index("fs"), lax.axis_index("tp")
    nz, nf, nc = lax.axis_size("sp"), lax.axis_size("fs"), lax.axis_size("tp")
    tok, feat = x_hbm.shape
    half = tok // 2
    rows_w = wa.shape[0]
    layer_rows = nf * rows_w
    cw = wa.shape[1] // nf
    kw = wq.shape[1] // nf
    vw = wv.shape[1] // nf
    total = nf * tok
    kin = wbuf.shape[0]
    pwc = pw.shape[1]
    half_rows = pw.shape[0] // 2
    channels = nc * nf * cw
    other = 1 - c
    xn = f + 1 - 2 * lax.rem(f, 2)
    yn = f + 2 - 4 * (f // 2)
    dg = nf - 1 - f
    peers = (xn, yn, dg)

    def remote(src, dst, recv, dev):
        return pltpu.make_async_remote_copy(
            src_ref=src, dst_ref=dst, send_sem=sent, recv_sem=recv,
            device_id=dev, device_id_type=MESH_IDS,
        )

    def arrived(dst, recv):
        remote(dst, dst, recv, (z, f, other)).wait_recv()

    def lanes(at, width):
        return pl.ds(pl.multiple_of(at * width, width), width)

    def xr(seq, h):
        row = pl.ds(pl.multiple_of(seq * tok + h * half, half), half)
        return xbuf.at[row, lanes(c, feat)]

    def xr_other(seq, h):
        row = pl.ds(pl.multiple_of(seq * tok + h * half, half), half)
        return xbuf.at[row, lanes(other, feat)]

    def item(i, b):
        if i < ROOT:
            row = pl.ds(pl.multiple_of(b * layer_rows, layer_rows), layer_rows)
            return wbuf.at[row, pl.ds(i * cw, cw)]
        if i == ROOT:
            return wobuf.at[b, :, pl.ds(0, pwc)]
        part = pl.ds((i - ROOT - 1) * half_rows, half_rows)
        return wobuf.at[b, part, pl.ds(pwc, pwc)]

    def up(i, b):
        return remote(item(i, b), item(i, b), zr.at[i, b], (z + 1, f, c))

    def down(i, b):
        return remote(item(i, b), item(i, b), zr.at[i, b], (z - 1, f, c))

    items = ROOT + OUT_ITEMS
    sources = {0: wa, 1: wb, 3: wv, 4: wg}
    my_rows = pl.ds(pl.multiple_of((z * nf + f) * rows_w, rows_w), rows_w)

    barrier = pltpu.get_barrier_semaphore()
    me = f * nc + c
    group = nf * nc
    for k in range(1, group):
        t = lax.rem(me + k, group)
        pl.semaphore_signal(barrier, inc=1, device_id=(z, t // nc, lax.rem(t, nc)), device_id_type=MESH_IDS)
    for k in range(1, nz):
        pl.semaphore_signal(barrier, inc=1, device_id=(lax.rem(z + k, nz), f, c), device_id_type=MESH_IDS)
    params = [
        pltpu.make_async_copy(src, dst, pl_in.at[n])
        for n, (src, dst) in enumerate(
            (
                (ng_hbm, ng_ref), (ff_hbm, ff_ref), (dw_hbm, dw_ref), (db_hbm, db_ref),
                (ck_hbm, ck_ref), (cg_hbm, cg_ref), (hg_hbm, hg_ref),
            )
        )
    ]

    own_x = [
        pltpu.make_async_copy(x_hbm.at[pl.ds(h * half, half), :], xr(f, h), xl.at[h])
        for h in range(2)
    ]
    qk_load = [
        pltpu.make_async_copy(wq, qraw, ol.at[2]),
        pltpu.make_async_copy(wk, kraw, ol.at[3]),
    ]
    own_w = {
        g: pltpu.make_async_copy(
            w.at[:, lanes(f, cw)], wbuf.at[my_rows, pl.ds(g * cw, cw)], al.at[g]
        )
        for g, w in sources.items()
    }
    own_o = [
        pltpu.make_async_copy(pw, item(ROOT, z), ol.at[0]),
        pltpu.make_async_copy(go, wobuf.at[z, :, pl.ds(pwc, pwc)], ol.at[1]),
    ]
    own_d = pltpu.make_async_copy(dex_hbm.at[:, lanes(f // 2, 2 * kw)], debuf.at[f], dl)
    for copy in qk_load:
        copy.start()
    for g in sources:
        own_w[g].start()
    for copy in own_x + own_o + [own_d] + params:
        copy.start()

    for copy in qk_load:
        copy.wait()
    for j in range(nf):
        qkst[j] = jnp.concatenate(
            [qraw[:, j * kw : (j + 1) * kw], kraw[:, j * kw : (j + 1) * kw]], axis=1
        )
    wbuf[my_rows, pl.ds(2 * cw, cw)] = qkst[f]
    pl.semaphore_wait(barrier, group - 1 + nz - 1)

    def exchange(g):
        out = []
        for p in peers:
            src = qkst.at[p] if g == 2 else sources[g].at[:, lanes(p, cw)]
            dst = wbuf.at[my_rows, pl.ds(g * cw, cw)]
            out.append(remote(src, dst, ar.at[g, f], (z, p, c)))
        return out

    x_to_x = [
        remote(x_hbm.at[pl.ds(h * half, half), :], xr(f, h), xi.at[f, h], (z, xn, c))
        for h in range(2)
    ]
    x_to_y = [
        remote(x_hbm.at[pl.ds(h * half, half), :], xr(f, h), xi.at[f, h], (z, yn, c))
        for h in range(2)
    ]
    x_over = [
        remote(x_hbm.at[pl.ds(h * half, half), :], xr(f, h), xd.at[f, h], (z, f, other))
        for h in range(2)
    ]

    def over(seq, h):
        return remote(xr(seq, h), xr(seq, h), xd.at[seq, h], (z, f, other))

    decay_out = [
        remote(
            dex_hbm.at[:, lanes(p // 2, 2 * kw)], debuf.at[f], dr.at[f], (z, p, c)
        )
        for p in peers
    ]

    sends = []

    def start(*copies):
        for copy in copies:
            copy.start()
            sends.append(copy)


    def own(i):
        if i < ROOT:
            if i in own_w:
                own_w[i].wait()
            for p in peers:
                arrived(
                    wbuf.at[
                        pl.ds(pl.multiple_of((z * nf + p) * rows_w, rows_w), rows_w),
                        pl.ds(i * cw, cw),
                    ],
                    ar.at[i, p],
                )
        else:
            if i - ROOT < len(own_o):
                own_o[i - ROOT].wait()

        @pl.when(z < nz - 1)
        def _():
            up(i, z).start()

        @pl.when(z > 0)
        def _():
            down(i, z).start()

    def relay(i, d):
        @pl.when(z >= d)
        def _():
            arrived(item(i, z - d), zr.at[i, z - d])

            @pl.when(z < nz - 1)
            def _():
                up(i, z - d).start()

        @pl.when(z + d < nz)
        def _():
            arrived(item(i, z + d), zr.at[i, z + d])

            @pl.when(z > 0)
            def _():
                down(i, z + d).start()

    start(*exchange(0))
    own(5)
    start(*exchange(1))
    start(*exchange(2))
    start(x_to_x[0], x_to_y[1], *x_over)
    own(0)
    start(x_to_x[1], x_to_y[0])
    start(*exchange(3))
    own(1)
    relay(0, 1)

    arrived(xr(xn, 0), xi.at[xn, 0])
    start(
        remote(xr(xn, 0), xr(xn, 0), xi.at[xn, 0], (z, yn, c)),
        over(xn, 0),
    )
    arrived(xr(yn, 1), xi.at[yn, 1])
    start(
        remote(xr(yn, 1), xr(yn, 1), xi.at[yn, 1], (z, xn, c)),
        over(yn, 1),
    )
    start(*exchange(4))
    start(*decay_out)
    own(2)
    relay(0, 2)
    relay(1, 1)

    step_rows = 32

    def scale(seq):
        def body(r, carry):
            row = pl.ds(pl.multiple_of(seq * tok + r * step_rows, step_rows), step_rows)
            value = xbuf[row, :].astype(f32)
            square = jnp.sum(value * value, axis=1, keepdims=True)
            rs[row, :] = jnp.broadcast_to(
                lax.rsqrt(square / (nc * feat) + 1e-06), (step_rows, rs.shape[1])
            )
            xs[row, :] = (value * ng_ref[...]).astype(bf16)
            return carry

        lax.fori_loop(0, tok // step_rows, body, 0)

    for copy in own_x + params:
        copy.wait()
    for h in range(2):
        arrived(xr_other(f, h), xd.at[f, h])
    scale(f)
    arrived(xr(xn, 1), xi.at[xn, 1])
    arrived(xr(yn, 0), xi.at[yn, 0])
    start(over(xn, 1), over(yn, 0))
    relay(1, 2)
    own(3)
    for p in (xn, yn):
        for h in range(2):
            arrived(xr_other(p, h), xd.at[p, h])
        scale(p)
    relay(0, 3)
    relay(1, 3)
    relay(2, 1)
    arrived(xr(dg, 0), xi.at[dg, 0])
    arrived(xr(dg, 1), xi.at[dg, 1])
    start(over(dg, 0), over(dg, 1))
    for h in range(2):
        arrived(xr_other(dg, h), xd.at[dg, h])
    scale(dg)

    def project(seq, first, width):
        row = pl.ds(pl.multiple_of(seq * tok, tok), tok)
        out = jnp.dot(
            xs[row, :], wbuf[:, first : first + width], preferred_element_type=f32
        )
        return (out * rs[row, 0:1]).astype(bf16)

    halo = 32
    taps = ck_ref.shape[0]

    def conv_in(seq, carry):
        both = project(seq, 0, 2 * cw).astype(f32)
        gated = both[:, :cw] * jax.nn.sigmoid(both[:, cw:])
        low = gated.astype(bf16)
        ext[seq, halo : halo + tok, :] = low.astype(f32)
        hsend[seq] = low[tok - halo :]
        return carry

    lax.fori_loop(0, nf, conv_in, 0)
    halo_out = remote(hsend, hrecv, hr, (z + 1, f, c))

    @pl.when(z < nz - 1)
    def _():
        halo_out.start()

    relay(2, 2)
    own(4)

    part = c * (nf // 2) + f // 2
    odd = lax.rem(f, 2) == 1
    dw2 = dw_ref[:, lanes(part, 2 * kw)].astype(f32)
    dw_own = jnp.where(odd, dw2[:, kw:], dw2[:, :kw]).astype(bf16)
    db2 = db_ref[:, lanes(part, 2 * kw)]
    db_own = jnp.where(odd, db2[:, kw:], db2[:, :kw])
    own_d.wait()
    for p in peers:
        arrived(debuf.at[p], dr.at[p])

    def decay(seq, carry):
        row = pl.ds(pl.multiple_of(seq * tok, tok), tok)
        low = lax.dot_general(
            xs[row, :], ff_ref[...], (((1,), (1,)), ((), ())), preferred_element_type=f32
        )
        low = (low * rs[row, 0:1]).astype(bf16)
        pre = jnp.dot(low, dw_own, preferred_element_type=f32) + db_own
        extra = debuf[seq]
        extra = jnp.where(odd, extra[:, kw:], extra[:, :kw])
        ld[row, :] = jax.nn.log_sigmoid(pre) / 16.0 + extra
        return carry

    lax.fori_loop(0, nf, decay, 0)
    relay(2, 3)

    def keys_in(seq, carry):
        qkb[pl.ds(pl.multiple_of(seq * tok, tok), tok), :] = project(seq, 2 * cw, cw)
        return carry

    lax.fori_loop(0, nf, keys_in, 0)

    @pl.when(z > 0)
    def _():
        arrived(hrecv, hr)
        ext[:, 0:halo, :] = hrecv[...].astype(f32)

    @pl.when(z == 0)
    def _():
        ext[:, 0:halo, :] = jnp.zeros((nf, halo, cw), f32)

    mine = c * nf + f
    tap_rows = 64
    lane = lax.broadcasted_iota(jnp.int32, (tok, cw), 1)

    def tap(seq, carry):
        kernel = ck_ref[:, lanes(mine, cw)]
        for r in range(tok // tap_rows):
            acc = jnp.zeros((tap_rows, cw), f32)
            for j in range(taps):
                at = halo - (taps - 1) + j + r * tap_rows
                acc = acc + kernel[j : j + 1, :] * ext[seq, at : at + tap_rows, :]
            conv[pl.ds(pl.multiple_of(seq * tok + r * tap_rows, tap_rows), tap_rows), :] = acc
        row = pl.ds(pl.multiple_of(seq * tok, tok), tok)
        value = conv[row, :]
        mean = jnp.sum(value, axis=1, keepdims=True) / cw
        spread = value - mean
        second = jnp.sum(spread * spread, axis=1, keepdims=True)
        both = jnp.where(lane == 0, mean, jnp.where(lane == 1, second, 0.0))
        stats[me, :, pl.ds(pl.multiple_of(seq * tok, tok), tok)] = both.T[0:8, :]
        return carry

    lax.fori_loop(0, nf, tap, 0)
    relay(3, 1)
    for k in range(1, group):
        t = lax.rem(me + k, group)
        start(
            remote(
                stats.at[me], stats.at[me], tr.at[me], (z, t // nc, lax.rem(t, nc))
            )
        )
    for k in range(1, group):
        t = lax.rem(me + k, group)
        arrived(stats.at[t], tr.at[t])
    every = stats[...]
    means = every[:, 0, :]
    mean = jnp.sum(means, axis=0, keepdims=True) / group
    off = means - mean
    second = jnp.sum(every[:, 1, :] + cw * off * off, axis=0, keepdims=True)
    inverse = lax.rsqrt(second / channels + 1e-05)
    comb[0:1, :] = mean
    comb[1:2, :] = inverse

    def conv_out(seq, carry):
        row = pl.ds(pl.multiple_of(seq * tok, tok), tok)
        flat = comb[0:2, row]
        cols = jnp.concatenate([flat, jnp.zeros((cw - 2, tok), f32)], axis=0).T
        normed = (conv[row, :] - cols[:, 0:1]) * cols[:, 1:2] * cg_ref[:, lanes(mine, cw)]
        actbuf[row, lanes(f, cw)] = (normed * jax.nn.sigmoid(normed)).astype(bf16)
        return carry

    def act_block(at):
        return actbuf.at[:, lanes(at, cw)]

    relay(3, 2)
    lax.fori_loop(0, nf, conv_out, 0)
    for p in peers:
        start(remote(act_block(f), act_block(f), cr.at[f], (z, p, c)))

    def values_in(seq, carry):
        vb[pl.ds(pl.multiple_of(seq * tok, tok), tok), :] = project(seq, 3 * cw, cw)
        return carry

    relay(3, 3)
    lax.fori_loop(0, nf, values_in, 0)

    spread_m = (
        lax.broadcasted_iota(jnp.int32, (kw, vw), 0) // DK
        == lax.broadcasted_iota(jnp.int32, (kw, vw), 1) // DV
    ).astype(bf16)
    own_mask = (
        lax.broadcasted_iota(jnp.int32, (vw, kw), 1) // DK
        == lax.broadcasted_iota(jnp.int32, (vw, kw), 0) // DV
    )
    place = lax.rem(lax.broadcasted_iota(jnp.int32, (CHUNK, kw), 0), SUB)
    per_seq = tok // CHUNK

    def attend(n, carry):
        at = pl.ds(pl.multiple_of(n * CHUNK, CHUNK), CHUNK)
        qk = qkb[at, :].astype(f32)
        q = qk[:, :kw] * DK ** (-0.5)
        k = qk[:, kw:]
        v = vb[at, :].astype(f32)
        cum = ld[at, :]
        step = 1
        while step < SUB:
            cum = cum + jnp.where(place >= step, pltpu.roll(cum, step, 0), 0.0)
            step *= 2
        acc = jnp.dot((q * k).astype(bf16), spread_m, preferred_element_type=f32) * v
        for lag in range(1, SUB):
            decays = jnp.exp(jnp.where(place >= lag, cum - pltpu.roll(cum, lag, 0), -jnp.inf))
            term = (q * pltpu.roll(k, lag, 0) * decays).astype(bf16)
            score = jnp.dot(term, spread_m, preferred_element_type=f32)
            acc = acc + score * pltpu.roll(v, lag, 0)
        q_f = q * jnp.exp(cum)
        q_in = q_f.astype(bf16)
        v_low = v.astype(bf16)
        first = lax.rem(n, per_seq) == 0
        state = jnp.where(first, 0.0, state_ref[...])
        base = jnp.where(first, 0.0, base_ref[0:1, :])
        outer, seg = [], []
        for m in range(CHUNK // SUB):
            part = slice(m * SUB, (m + 1) * SUB)
            last = cum[(m + 1) * SUB - 1 : (m + 1) * SUB]
            k_out = (k[part] * jnp.exp(last - cum[part])).astype(bf16)
            outer.append(
                lax.dot_general(
                    q_in[part], state.astype(bf16), (((1,), (1,)), ((), ())),
                    preferred_element_type=f32,
                )
            )
            added = lax.dot_general(
                v_low[part], k_out, (((0,), (0,)), ((), ())), preferred_element_type=f32
            )
            seg.append(q_f[part] * jnp.exp(base))
            state = state * jnp.exp(last) + jnp.where(own_mask, added, 0.0)
            base = base + last
        state_ref[...] = state
        base_ref[...] = jnp.broadcast_to(base, base_ref.shape)
        sfin[n // per_seq] = state
        tots[n // per_seq] = jnp.broadcast_to(base, base_ref.shape)
        raw[at, :] = acc + jnp.concatenate(outer, axis=0)
        qseg[at, :] = jnp.concatenate(seg, axis=0).astype(bf16)

        @pl.when(n == 1)
        def _():
            relay(4, 1)

        return carry

    lax.fori_loop(0, total // CHUNK, attend, 0)
    vh = vw // 2
    for p in range(nf // 2):
        a, b = sfin[2 * p], sfin[2 * p + 1]
        stbuf[z, p] = jnp.concatenate([a[:vh] + a[vh:], b[:vh] + b[vh:]], axis=1).astype(bf16)
        totbuf[z, p] = jnp.concatenate([tots[2 * p], tots[2 * p + 1]], axis=1)

    def state_out(d):
        dev = (z + d, f, c)
        return (
            remote(stbuf.at[z], stbuf.at[z], vr.at[0, z], dev),
            remote(totbuf.at[z], totbuf.at[z], vr.at[1, z], dev),
        )

    for d in range(1, nz):
        @pl.when(z + d < nz)
        def _():
            for copy in state_out(d):
                copy.start()

    relay(4, 2)
    own(6)
    own(7)
    relay(5, 1)
    relay(4, 3)

    sin_ref[...] = jnp.zeros_like(sin_ref)
    for b in range(nz - 1):
        @pl.when(z > b)
        def _():
            arrived(stbuf.at[b], vr.at[0, b])
            arrived(totbuf.at[b], vr.at[1, b])
            sin_ref[...] = sin_ref[...] * jnp.exp(totbuf[b, :, 0:1, :]) + stbuf[b].astype(f32)
    head_mean = jnp.where(
        lax.broadcasted_iota(jnp.int32, (vw, vw), 0) // DV
        == lax.broadcasted_iota(jnp.int32, (vw, vw), 1) // DV,
        1.0 / DV,
        0.0,
    ).astype(f32)
    gain = jnp.concatenate([hg_ref[...]] * (vw // DV), axis=1)
    for seq in range(nf):
        row = slice(seq * tok, (seq + 1) * tok)
        lo = (seq % 2) * kw
        packed = sin_ref[seq // 2][:, lo : lo + kw]
        state = jnp.where(own_mask, jnp.concatenate([packed, packed], axis=0), 0.0).astype(bf16)
        full = raw[row, :] + lax.dot_general(
            qseg[row, :], state, (((1,), (1,)), ((), ())), preferred_element_type=f32
        )
        mean = jnp.dot(
            full * full, head_mean, preferred_element_type=f32, precision=lax.Precision.HIGHEST
        )
        gate = project(seq, 4 * cw, cw).astype(f32)
        actbuf[row, lanes(nf + f, cw)] = (
            full * lax.rsqrt(mean + 1e-06) * gain * (gate * jax.nn.sigmoid(gate))
        ).astype(bf16)
    for p in peers:
        start(remote(act_block(nf + f), act_block(nf + f), gr.at[f], (z, p, c)))
    relay(5, 2)

    near = jnp.where(z < nz // 2, z, nz - 1 - z)
    out_rows = pw.shape[0]
    per_core = nz // nc

    def block_of(k):
        o = (near, 1 - near, 2, 3)[k]
        return jnp.where(z < nz // 2, o, nz - 1 - o)

    def rows_of(p):
        return pl.ds(pl.multiple_of(p * tok, tok), tok)

    def turn(j):
        return jnp.where(j == 0, dg, jnp.where(j == 1, xn, jnp.where(j == 2, yn, f)))

    def over_part(k, slot, p, lo, width, n):
        at = pl.ds(lo, width)
        return remote(
            pbuf.at[k, rows_of(p), at], prcv.at[slot, rows_of(p), at],
            pr.at[n, slot, p], (z, f, other),
        )

    def landing(slot, source, lo, width):
        first = pl.multiple_of((slot * nf + source) * out_rows + lo, width)
        return o_hbm.at[:, pl.ds(first, width)]

    def out_copy(slot, p, lo, width, n):
        return remote(
            osum.at[slot, rows_of(p), pl.ds(lo, width)], landing(slot, f, lo, width),
            orc.at[n, slot, f], (z, p, c),
        )

    def out_own(slot, lo, width, n):
        return pltpu.make_async_copy(
            osum.at[slot, rows_of(f), pl.ds(lo, width)], landing(slot, f, lo, width),
            o_out.at[n, slot],
        )

    def block(k, lo, width, n):
        b = block_of(k)
        slot = lax.rem(b, per_core)
        owner = b // per_core
        at = pl.ds(lo, width)

        def multiply(j, carry):
            p = turn(j)
            out = lax.dot_general(
                actbuf[rows_of(p), :], wobuf[b, lo : lo + width, :], (((1,), (1,)), ((), ())),
                preferred_element_type=f32,
            )
            pbuf[k, rows_of(p), at] = out.astype(bf16)

            @pl.when(owner != c)
            def _():
                over_part(k, slot, p, lo, width, n).start()

            return carry

        lax.fori_loop(0, nf, multiply, 0)

        def gather(j, carry):
            p = turn(j)
            arrived(prcv.at[slot, rows_of(p), at], pr.at[n, slot, p])
            osum[slot, rows_of(p), at] = (
                pbuf[k, rows_of(p), at].astype(f32) + prcv[slot, rows_of(p), at].astype(f32)
            ).astype(bf16)

            @pl.when(j < nf - 1)
            def _():
                out_copy(slot, p, lo, width, n).start()

            return carry

        @pl.when(owner == c)
        def _():
            lax.fori_loop(0, nf, gather, 0)
            out_own(slot, lo, width, n).start()

    def block_end(k, lo, width, n):
        b = block_of(k)
        slot = lax.rem(b, per_core)

        @pl.when(b // per_core != c)
        def _():
            for p in range(nf):
                over_part(k, slot, p, lo, width, n).wait_send()

        @pl.when(b // per_core == c)
        def _():
            for p in peers:
                arrived(landing(slot, p, lo, width), orc.at[n, slot, p])
            out_own(slot, lo, width, n).wait()
            for p in peers:
                out_copy(slot, p, lo, width, n).wait_send()

    def acts():
        for p in peers:
            arrived(act_block(p), cr.at[p])
            arrived(act_block(nf + p), gr.at[p])

    ends = (z == 0) | (z == nz - 1)
    halves = [(0, half_rows, 0), (half_rows, half_rows, 1)]
    whole = (0, out_rows, 0)

    @pl.when(ends)
    def _():
        relay(5, 3)
        acts()
        block(0, *whole)
        for k in range(1, nz):
            relay(6, k)
            if k == nz - 1:
                block(k, *halves[0])
            relay(7, k)
            block(k, *(halves[1] if k == nz - 1 else whole))
        for k in range(nz - 1):
            block_end(k, *whole)
        for part in halves:
            block_end(nz - 1, *part)

    @pl.when(jnp.logical_not(ends))
    def _():
        for k in range(1, nz):
            relay(6, k)
            relay(7, k)
        acts()
        for k in range(nz):
            block(k, *whole)
        for k in range(nz):
            block_end(k, *whole)

    for copy in sends:
        copy.wait_send()
    for i in range(items):
        for b in range(nz):
            @pl.when((z < nz - 1) & (z >= b))
            def _():
                up(i, b).wait_send()

            @pl.when((z > 0) & (z <= b))
            def _():
                down(i, b).wait_send()

    @pl.when(z < nz - 1)
    def _():
        halo_out.wait_send()

    for d in range(1, nz):
        @pl.when(z + d < nz)
        def _():
            for copy in state_out(d):
                copy.wait_send()


def by_segments(
    inputs, norm_gain, conv_in_a, conv_in_b, query_w, key_w, value_w, out_gate_w,
    pointwise_w, gla_out_w, forget_first_factor, decay_w, decay_bias, decay_extra,
    conv_kernel, conv_gain, head_gain,
):
    f32, bf16 = jnp.float32, jnp.bfloat16
    nz, nf, nc = lax.axis_size("sp"), lax.axis_size("fs"), lax.axis_size("tp")
    x = inputs[0]
    tok, feat = x.shape
    total = nf * tok
    rows_w = conv_in_a.shape[0]
    kin = nz * nf * rows_w
    cw = conv_in_a.shape[1] // nf
    kw = query_w.shape[1] // nf
    vw = value_w.shape[1] // nf
    pwc = pointwise_w.shape[1]
    out_rows = pointwise_w.shape[0]
    group = nf * nc
    dma = pltpu.SemaphoreType.DMA
    items = ROOT + OUT_ITEMS
    any_spec = pl.BlockSpec(memory_space=pl.ANY)
    V = pltpu.VMEM
    flat = (
        norm_gain[None], forget_first_factor.T, decay_w, decay_bias[None],
        conv_kernel, conv_gain[None], head_gain[None],
    )
    scratch = [V(a.shape, a.dtype) for a in flat] + [
        V((total, nc * feat), bf16), V((total, nc * feat), bf16), V((total, 128), f32),
        V((kin, ROOT * cw), bf16), V((rows_w, nf * kw), bf16), V((rows_w, nf * kw), bf16),
        V((nf, rows_w, cw), bf16), V((nz, out_rows, 2 * pwc), bf16),
        V((nf, tok, 2 * kw), f32), V((nf, tok + 32, cw), f32), V((nf, 32, cw), bf16), V((nf, 32, cw), bf16), V((total, cw), f32),
        V((group, 8, total), f32), V((8, total), f32), V((total, 2 * nf * cw), bf16),
        V((total, cw), bf16), V((total, vw), bf16), V((total, kw), f32), V((total, vw), f32),
        V((total, kw), bf16), V((vw, kw), f32), V((8, kw), f32), V((nf, vw, kw), f32),
        V((nf, 8, kw), f32), V((nz, nf // 2, vw // 2, 2 * kw), bf16),
        V((nz, nf // 2, 8, 2 * kw), f32),
        V((nf // 2, vw // 2, 2 * kw), f32),
        V((nz, total, out_rows), bf16), V((nz // nc, total, out_rows), bf16),
        V((nz // nc, total, out_rows), bf16),
        dma, dma((2,)), dma((nf, 2)), dma((nf, 2)), dma((ROOT,)), dma((ROOT, nf)),
        dma((items, nz)), dma((4,)), dma, dma((nf,)), dma((len(flat),)), dma((2, nz // nc)), dma,
        dma((group,)), dma((2, nz)), dma((nf,)), dma((nf,)), dma((2, nz // nc, nf)),
        dma((2, nz // nc, nf)),
    ]
    out = pl.pallas_call(
        fused_kernel,
        out_shape=jax.ShapeDtypeStruct((tok, feat), bf16),
        in_specs=[any_spec] * 17,
        out_specs=any_spec,
        scratch_shapes=scratch,
        compiler_params=pltpu.CompilerParams(
            collective_id=0, has_side_effects=True, vmem_limit_bytes=60 * 1024 * 1024
        ),
        name="mixer",
    )(
        x, conv_in_a, conv_in_b, query_w, key_w, value_w, out_gate_w, pointwise_w, gla_out_w,
        decay_extra[0], *flat,
    )
    return (x.astype(f32) + out.astype(f32)).astype(bf16)[None]


def fits(inputs, conv_in_a, query_w, value_w):
    n_sp, n_tp, n_fs = lax.axis_size("sp"), lax.axis_size("tp"), lax.axis_size("fs")
    widths = (conv_in_a.shape[1], 2 * query_w.shape[1], value_w.shape[1])
    return (
        (n_sp, n_fs, n_tp) == (4, 4, 2)
        and inputs.shape[0] == 1
        and inputs.shape[1] % CHUNK == 0
        and all(w == 128 * n_fs for w in widths)
    )


def from_behind(value, axis, by):
    length = lax.axis_size(axis)
    pairs = [(i, i + by) for i in range(length) if 0 <= i + by < length]
    return lax.ppermute(value, axis, pairs)


def by_tokens(
    inputs,
    norm_gain,
    conv_in_a,
    conv_in_b,
    query_w,
    key_w,
    value_w,
    out_gate_w,
    pointwise_w,
    gla_out_w,
    forget_first_factor,
    decay_w,
    decay_bias,
    decay_extra,
    conv_kernel,
    conv_gain,
    head_gain,
):
    collected = (
        lax.all_gather(conv_in_a, ("sp", "fs"), axis=0, tiled=True),
        lax.all_gather(conv_in_b, ("sp", "fs"), axis=0, tiled=True),
        lax.all_gather(query_w, ("sp", "fs"), axis=0, tiled=True),
        lax.all_gather(key_w, ("sp", "fs"), axis=0, tiled=True),
        lax.all_gather(value_w, ("sp", "fs"), axis=0, tiled=True),
        lax.all_gather(out_gate_w, ("sp", "fs"), axis=0, tiled=True),
        lax.all_gather(pointwise_w, ("sp", "fs"), axis=0, tiled=True),
        lax.all_gather(gla_out_w, ("sp", "fs"), axis=0, tiled=True),
    )
    (
        conv_a_full,
        conv_b_full,
        query_full,
        key_full,
        value_full,
        gate_full,
        pointwise_full,
        gla_out_full,
    ) = collected
    tok_rows = inputs[0]
    token_count = tok_rows.shape[0]
    in_weights = (
        conv_a_full,
        conv_b_full,
        query_full,
        key_full,
        value_full,
        gate_full,
        forget_first_factor,
    )
    segment_values = lax.all_gather(tok_rows, "tp", axis=1, tiled=True).astype(jnp.float32)
    scaled = (segment_values * norm_gain).astype(jnp.bfloat16)
    sums = tuple(
        (jnp.dot(scaled, weight, preferred_element_type=jnp.float32) for weight in in_weights)
    )
    sums, squares = (sums, jnp.sum(segment_values * segment_values, axis=1))
    row_scale = lax.rsqrt(squares / norm_gain.shape[0] + 1e-06)[:, None]
    conv_a, conv_b, queries, keys, values, out_gate, low_rank = [
        (running * row_scale).astype(jnp.bfloat16) for running in sums
    ]
    gated = (conv_a.astype(jnp.float32) * jax.nn.sigmoid(conv_b.astype(jnp.float32))).astype(
        jnp.bfloat16
    )
    reach = conv_kernel.shape[0] - 1
    earlier = from_behind(gated[token_count - reach :], "sp", 1)
    extended = jnp.concatenate([earlier, gated], axis=0).astype(jnp.float32)
    tp_index = lax.axis_index("tp")
    channels = gated.shape[1]
    kernel = lax.dynamic_slice_in_dim(conv_kernel, tp_index * channels, channels, 1)
    convolved = jnp.zeros((token_count, channels), jnp.float32)
    for offset in range(reach + 1):
        convolved = convolved + kernel[offset] * extended[offset : offset + token_count]
    channel_sum, channel_squares = lax.psum(
        (jnp.sum(convolved, axis=1), jnp.sum(convolved * convolved, axis=1)), "tp"
    )
    total_channels = conv_gain.shape[0]
    average = channel_sum / total_channels
    spread_squared_mean = channel_squares / total_channels - average * average
    gain_part = lax.dynamic_slice_in_dim(conv_gain, tp_index * channels, channels)
    normed = (
        (convolved - average[:, None]) * lax.rsqrt(spread_squared_mean + 1e-05)[:, None] * gain_part
    )
    conv_act = jax.nn.silu(normed).astype(jnp.bfloat16)
    key_width = keys.shape[1]
    head_count = key_width // DK
    decay_part = lax.dynamic_slice_in_dim(decay_w, tp_index * key_width, key_width, 1)
    bias_part = lax.dynamic_slice_in_dim(decay_bias, tp_index * key_width, key_width)
    pre_decay = jnp.dot(low_rank, decay_part, preferred_element_type=jnp.float32) + bias_part
    log_decay = jax.nn.log_sigmoid(pre_decay) / 16.0 + decay_extra[0]
    block_count = token_count // BLOCK
    highest = lax.Precision.HIGHEST

    def split_blocks(array_operand, width):
        return array_operand.reshape(block_count, BLOCK, head_count, width).transpose(0, 2, 1, 3)

    q_blocks = split_blocks(queries.astype(jnp.float32), DK) * DK ** (-0.5)
    k_blocks = split_blocks(keys.astype(jnp.float32), DK)
    v_blocks = split_blocks(values.astype(jnp.float32), DV)
    prefix_running_sum = jnp.cumsum(split_blocks(log_decay, DK), axis=2)
    causal = jnp.tril(jnp.ones((BLOCK, BLOCK), dtype=bool))
    spread = prefix_running_sum[:, :, :, None, :] - prefix_running_sum[:, :, None, :, :]
    weights_in = jnp.exp(jnp.where(causal[:, :, None], spread, -jnp.inf))
    scores = jnp.einsum("nhid,nhjd,nhijd->nhij", q_blocks, k_blocks, weights_in, precision=highest)
    inner = jnp.einsum("nhij,nhjv->nhiv", scores, v_blocks, precision=highest)
    block_total = prefix_running_sum[:, :, -1]
    block_state = jnp.einsum(
        "nhjd,nhjv->nhdv",
        k_blocks * jnp.exp(block_total[:, :, None] - prefix_running_sum),
        v_blocks,
        precision=highest,
    )

    def advance(state, block_pair):
        decay_row, added_share_term = block_pair
        return (jnp.exp(decay_row)[..., None] * state + added_share_term, state)

    local_final, local_entering = lax.scan(
        advance, jnp.zeros((head_count, DK, DV), jnp.float32), (block_total, block_state)
    )
    device_total = jnp.sum(block_total, axis=0)
    totals = lax.all_gather(device_total[None], "sp", axis=0, tiled=True)
    running_totals = jnp.cumsum(totals, axis=0)
    sp_index = lax.axis_index("sp")
    before = lax.dynamic_index_in_dim(
        running_totals, sp_index, 0, False
    ) - lax.dynamic_index_in_dim(totals, sp_index, 0, False)
    piece = lax.all_gather(local_final[None], "sp", axis=0, tiled=True)
    number = piece.shape[0]
    anchor = jnp.arange(number, dtype=jnp.int32)
    exponent = jnp.where(
        (anchor < sp_index)[:, None, None], before[None] - running_totals, -jnp.inf
    )
    entering = jnp.einsum("nhd,nhdv->hdv", jnp.exp(exponent), piece, precision=highest)
    passed = jnp.exp(jnp.cumsum(block_total, axis=0) - block_total)
    entering_blocks = passed[..., None] * entering[None] + local_entering
    outer = jnp.einsum(
        "nhid,nhdv->nhiv",
        q_blocks * jnp.exp(prefix_running_sum),
        entering_blocks,
        precision=highest,
    )
    head_output = inner + outer
    normed_heads = (
        head_output
        * lax.rsqrt(jnp.mean(head_output * head_output, axis=-1, keepdims=True) + 1e-06)
        * head_gain
    )
    gla_rows = normed_heads.transpose(0, 2, 1, 3).reshape(token_count, head_count * DV)
    gla_act = (gla_rows * jax.nn.silu(out_gate.astype(jnp.float32))).astype(jnp.bfloat16)
    contract = (((1,), (1,)), ((), ()))
    conv_term = lax.dot_general(
        pointwise_full, conv_act, contract, preferred_element_type=jnp.float32
    )
    summed = lax.psum_scatter(
        (
            conv_term
            + lax.dot_general(gla_out_full, gla_act, contract, preferred_element_type=jnp.float32)
        ).astype(jnp.bfloat16),
        "tp",
        scatter_dimension=0,
        tiled=True,
    ).astype(jnp.float32)
    return (tok_rows.astype(jnp.float32) + summed.T).astype(jnp.bfloat16)[None]


def shards(*args):
    if fits(args[0], args[2], args[4], args[6]):
        return by_segments(*args)
    return by_tokens(*args)


def solution(mesh):
    by_rows = P(("sp", "fs"), "tp")
    return jax.shard_map(
        shards,
        mesh=mesh,
        in_specs=(P("fs", "sp", "tp"), P())
        + (by_rows,) * 8
        + (P(), P(), P(), P("fs", "sp", "tp"), P(), P(), P()),
        out_specs=P("fs", "sp", "tp"),
        check_vma=False,
    )
```

```python
import jax
import jax.numpy as jnp
from jax import lax
from jax.experimental import pallas as pl
from jax.experimental.pallas import tpu as pltpu
from jax.sharding import PartitionSpec as P


DK = 32
DV = 64
SUB = 16
BLOCK = 64


ROOT = 5
OUT_ITEMS = 3
CHUNK = 128
MESH_IDS = pl.DeviceIdType.MESH


def fused_kernel(
    x_hbm, wa, wb, wq, wk, wv, wg, pw, go, dex_hbm,
    ng_hbm, ff_hbm, dw_hbm, db_hbm, ck_hbm, cg_hbm, hg_hbm,
    o_hbm,
    ng_ref, ff_ref, dw_ref, db_ref, ck_ref, cg_ref, hg_ref,
    xbuf, xs, rs, wbuf, qraw, kraw, qkst, wobuf, debuf, ext, hsend, hrecv, conv, stats, comb, actbuf,
    qkb, vb, ld, raw, qseg, state_ref, base_ref, sfin, tots, stbuf, totbuf, sin_ref,
    pbuf, prcv, osum,
    sent, xl, xi, xd, al, ar, zr, ol, dl, dr, pl_in, o_out, hr, tr, vr, cr, gr, pr, orc,
):
    f32, bf16 = jnp.float32, jnp.bfloat16
    z, f, c = lax.axis_index("sp"), lax.axis_index("fs"), lax.axis_index("tp")
    nz, nf, nc = lax.axis_size("sp"), lax.axis_size("fs"), lax.axis_size("tp")
    tok, feat = x_hbm.shape
    half = tok // 2
    rows_w = wa.shape[0]
    layer_rows = nf * rows_w
    cw = wa.shape[1] // nf
    kw = wq.shape[1] // nf
    vw = wv.shape[1] // nf
    total = nf * tok
    kin = wbuf.shape[0]
    pwc = pw.shape[1]
    half_rows = pw.shape[0] // 2
    channels = nc * nf * cw
    other = 1 - c
    xn = f + 1 - 2 * lax.rem(f, 2)
    yn = f + 2 - 4 * (f // 2)
    dg = nf - 1 - f
    peers = (xn, yn, dg)

    def remote(src, dst, recv, dev):
        return pltpu.make_async_remote_copy(
            src_ref=src, dst_ref=dst, send_sem=sent, recv_sem=recv,
            device_id=dev, device_id_type=MESH_IDS,
        )

    def arrived(dst, recv):
        remote(dst, dst, recv, (z, f, other)).wait_recv()

    def lanes(at, width):
        return pl.ds(pl.multiple_of(at * width, width), width)

    def xr(seq, h):
        row = pl.ds(pl.multiple_of(seq * tok + h * half, half), half)
        return xbuf.at[row, lanes(c, feat)]

    def xr_other(seq, h):
        row = pl.ds(pl.multiple_of(seq * tok + h * half, half), half)
        return xbuf.at[row, lanes(other, feat)]

    def item(i, b):
        if i < ROOT:
            row = pl.ds(pl.multiple_of(b * layer_rows, layer_rows), layer_rows)
            return wbuf.at[row, pl.ds(i * cw, cw)]
        if i == ROOT:
            return wobuf.at[b, :, pl.ds(0, pwc)]
        part = pl.ds((i - ROOT - 1) * half_rows, half_rows)
        return wobuf.at[b, part, pl.ds(pwc, pwc)]

    def up(i, b):
        return remote(item(i, b), item(i, b), zr.at[i, b], (z + 1, f, c))

    def down(i, b):
        return remote(item(i, b), item(i, b), zr.at[i, b], (z - 1, f, c))

    items = ROOT + OUT_ITEMS
    sources = {0: wa, 1: wb, 3: wv, 4: wg}
    my_rows = pl.ds(pl.multiple_of((z * nf + f) * rows_w, rows_w), rows_w)

    barrier = pltpu.get_barrier_semaphore()
    me = f * nc + c
    group = nf * nc
    for k in range(1, group):
        t = lax.rem(me + k, group)
        pl.semaphore_signal(barrier, inc=1, device_id=(z, t // nc, lax.rem(t, nc)), device_id_type=MESH_IDS)

    @pl.when(z > 0)
    def _():
        pl.semaphore_signal(barrier, inc=1, device_id=(z - 1, f, c), device_id_type=MESH_IDS)

    @pl.when(z < nz - 1)
    def _():
        pl.semaphore_signal(barrier, inc=1, device_id=(z + 1, f, c), device_id_type=MESH_IDS)

    params = [
        pltpu.make_async_copy(src, dst, pl_in.at[n])
        for n, (src, dst) in enumerate(
            (
                (ng_hbm, ng_ref), (ff_hbm, ff_ref), (dw_hbm, dw_ref), (db_hbm, db_ref),
                (ck_hbm, ck_ref), (cg_hbm, cg_ref), (hg_hbm, hg_ref),
            )
        )
    ]

    own_x = [
        pltpu.make_async_copy(x_hbm.at[pl.ds(h * half, half), :], xr(f, h), xl.at[h])
        for h in range(2)
    ]
    qk_load = [
        pltpu.make_async_copy(wq, qraw, ol.at[2]),
        pltpu.make_async_copy(wk, kraw, ol.at[3]),
    ]
    own_w = {
        g: pltpu.make_async_copy(
            w.at[:, lanes(f, cw)], wbuf.at[my_rows, pl.ds(g * cw, cw)], al.at[g]
        )
        for g, w in sources.items()
    }
    own_o = [
        pltpu.make_async_copy(pw, item(ROOT, z), ol.at[0]),
        pltpu.make_async_copy(go, wobuf.at[z, :, pl.ds(pwc, pwc)], ol.at[1]),
    ]
    own_d = pltpu.make_async_copy(dex_hbm.at[:, lanes(f // 2, 2 * kw)], debuf.at[f], dl)
    for copy in qk_load:
        copy.start()
    for g in sources:
        own_w[g].start()
    for copy in own_x + own_o + [own_d] + params:
        copy.start()

    for copy in qk_load:
        copy.wait()
    for j in range(nf):
        qkst[j] = jnp.concatenate(
            [qraw[:, j * kw : (j + 1) * kw], kraw[:, j * kw : (j + 1) * kw]], axis=1
        )
    wbuf[my_rows, pl.ds(2 * cw, cw)] = qkst[f]
    beside = jnp.where((z == 0) | (z == nz - 1), 1, 2)
    pl.semaphore_wait(barrier, group - 1 + beside)

    def exchange(g):
        out = []
        for p in peers:
            src = qkst.at[p] if g == 2 else sources[g].at[:, lanes(p, cw)]
            dst = wbuf.at[my_rows, pl.ds(g * cw, cw)]
            out.append(remote(src, dst, ar.at[g], (z, p, c)))
        return out

    x_to_x = [
        remote(x_hbm.at[pl.ds(h * half, half), :], xr(f, h), xi.at[f, h], (z, xn, c))
        for h in range(2)
    ]
    x_to_y = [
        remote(x_hbm.at[pl.ds(h * half, half), :], xr(f, h), xi.at[f, h], (z, yn, c))
        for h in range(2)
    ]
    x_over = [
        remote(x_hbm.at[pl.ds(h * half, half), :], xr(f, h), xd.at[f, h], (z, f, other))
        for h in range(2)
    ]

    def over(seq, h):
        return remote(xr(seq, h), xr(seq, h), xd.at[seq, h], (z, f, other))

    decay_out = [
        remote(
            dex_hbm.at[:, lanes(p // 2, 2 * kw)], debuf.at[f], dr, (z, p, c)
        )
        for p in peers
    ]

    sends = []

    def start(*copies):
        for copy in copies:
            copy.start()
            sends.append(copy)


    def own(i):
        if i < ROOT:
            if i in own_w:
                own_w[i].wait()
            arrived(wbuf.at[pl.ds(0, (nf - 1) * rows_w), pl.ds(i * cw, cw)], ar.at[i])
        else:
            if i - ROOT < len(own_o):
                own_o[i - ROOT].wait()

        @pl.when(z < nz - 1)
        def _():
            up(i, z).start()

        @pl.when(z > 0)
        def _():
            down(i, z).start()

    def relay(i, d):
        @pl.when(z >= d)
        def _():
            arrived(item(i, z - d), zr.at[i, z - d])

            @pl.when(z < nz - 1)
            def _():
                up(i, z - d).start()

        @pl.when(z + d < nz)
        def _():
            arrived(item(i, z + d), zr.at[i, z + d])

            @pl.when(z > 0)
            def _():
                down(i, z + d).start()

    start(*exchange(0))
    own(5)
    start(*exchange(1))
    start(*exchange(2))
    start(x_to_x[0], x_to_y[1], *x_over)
    own(0)
    start(x_to_x[1], x_to_y[0])
    start(*exchange(3))
    own(1)
    relay(0, 1)
    own(2)

    arrived(xr(xn, 0), xi.at[xn, 0])
    start(
        remote(xr(xn, 0), xr(xn, 0), xi.at[xn, 0], (z, yn, c)),
        over(xn, 0),
    )
    arrived(xr(yn, 1), xi.at[yn, 1])
    start(
        remote(xr(yn, 1), xr(yn, 1), xi.at[yn, 1], (z, xn, c)),
        over(yn, 1),
    )
    start(*exchange(4))
    start(*decay_out)
    relay(0, 2)
    relay(1, 1)

    step_rows = 32

    def scale(seq):
        def body(r, carry):
            row = pl.ds(pl.multiple_of(seq * tok + r * step_rows, step_rows), step_rows)
            value = xbuf[row, :].astype(f32)
            square = jnp.sum(value * value, axis=1, keepdims=True)
            rs[row, :] = jnp.broadcast_to(
                lax.rsqrt(square / (nc * feat) + 1e-06), (step_rows, rs.shape[1])
            )
            xs[row, :] = (value * ng_ref[...]).astype(bf16)
            return carry

        lax.fori_loop(0, tok // step_rows, body, 0)

    for copy in own_x + params:
        copy.wait()
    for h in range(2):
        arrived(xr_other(f, h), xd.at[f, h])
    scale(f)
    arrived(xr(xn, 1), xi.at[xn, 1])
    arrived(xr(yn, 0), xi.at[yn, 0])
    start(over(xn, 1), over(yn, 0))
    relay(1, 2)
    own(3)
    for p in (xn, yn):
        for h in range(2):
            arrived(xr_other(p, h), xd.at[p, h])
        scale(p)
    relay(0, 3)
    relay(1, 3)
    relay(2, 1)
    arrived(xr(dg, 0), xi.at[dg, 0])
    arrived(xr(dg, 1), xi.at[dg, 1])
    start(over(dg, 0), over(dg, 1))
    for h in range(2):
        arrived(xr_other(dg, h), xd.at[dg, h])
    scale(dg)

    def project(seq, first, width):
        row = pl.ds(pl.multiple_of(seq * tok, tok), tok)
        out = jnp.dot(
            xs[row, :], wbuf[:, first : first + width], preferred_element_type=f32
        )
        return (out * rs[row, 0:1]).astype(bf16)

    halo = 32
    taps = ck_ref.shape[0]

    def conv_in(seq, carry):
        both = project(seq, 0, 2 * cw).astype(f32)
        gated = both[:, :cw] * jax.nn.sigmoid(both[:, cw:])
        low = gated.astype(bf16)
        ext[seq, halo : halo + tok, :] = low.astype(f32)
        hsend[seq] = low[tok - halo :]
        return carry

    lax.fori_loop(0, nf, conv_in, 0)
    halo_out = remote(hsend, hrecv, hr, (z + 1, f, c))

    @pl.when(z < nz - 1)
    def _():
        halo_out.start()

    relay(2, 2)
    own(4)

    part = c * (nf // 2) + f // 2
    odd = lax.rem(f, 2) == 1
    dw2 = dw_ref[:, lanes(part, 2 * kw)].astype(f32)
    dw_own = jnp.where(odd, dw2[:, kw:], dw2[:, :kw]).astype(bf16)
    db2 = db_ref[:, lanes(part, 2 * kw)]
    db_own = jnp.where(odd, db2[:, kw:], db2[:, :kw])
    own_d.wait()
    arrived(debuf.at[pl.ds(0, nf - 1)], dr)

    def decay(seq, carry):
        row = pl.ds(pl.multiple_of(seq * tok, tok), tok)
        low = lax.dot_general(
            xs[row, :], ff_ref[...], (((1,), (1,)), ((), ())), preferred_element_type=f32
        )
        low = (low * rs[row, 0:1]).astype(bf16)
        pre = jnp.dot(low, dw_own, preferred_element_type=f32) + db_own
        extra = debuf[seq]
        extra = jnp.where(odd, extra[:, kw:], extra[:, :kw])
        ld[row, :] = jax.nn.log_sigmoid(pre) / 16.0 + extra
        return carry

    lax.fori_loop(0, nf, decay, 0)
    relay(2, 3)

    def keys_in(seq, carry):
        qkb[pl.ds(pl.multiple_of(seq * tok, tok), tok), :] = project(seq, 2 * cw, cw)
        return carry

    lax.fori_loop(0, nf, keys_in, 0)

    @pl.when(z > 0)
    def _():
        arrived(hrecv, hr)
        ext[:, 0:halo, :] = hrecv[...].astype(f32)

    @pl.when(z == 0)
    def _():
        ext[:, 0:halo, :] = jnp.zeros((nf, halo, cw), f32)

    mine = c * nf + f
    tap_rows = 64
    lane = lax.broadcasted_iota(jnp.int32, (tok, cw), 1)

    def tap(seq, carry):
        kernel = ck_ref[:, lanes(mine, cw)]
        for r in range(tok // tap_rows):
            acc = jnp.zeros((tap_rows, cw), f32)
            for j in range(taps):
                at = halo - (taps - 1) + j + r * tap_rows
                acc = acc + kernel[j : j + 1, :] * ext[seq, at : at + tap_rows, :]
            conv[pl.ds(pl.multiple_of(seq * tok + r * tap_rows, tap_rows), tap_rows), :] = acc
        row = pl.ds(pl.multiple_of(seq * tok, tok), tok)
        value = conv[row, :]
        mean = jnp.sum(value, axis=1, keepdims=True) / cw
        spread = value - mean
        second = jnp.sum(spread * spread, axis=1, keepdims=True)
        both = jnp.where(lane == 0, mean, jnp.where(lane == 1, second, 0.0))
        stats[me, :, pl.ds(pl.multiple_of(seq * tok, tok), tok)] = both.T[0:8, :]
        return carry

    lax.fori_loop(0, nf, tap, 0)
    relay(3, 1)
    for k in range(1, group):
        t = lax.rem(me + k, group)
        start(
            remote(
                stats.at[me], stats.at[me], tr, (z, t // nc, lax.rem(t, nc))
            )
        )
    arrived(stats.at[pl.ds(0, group - 1)], tr)
    every = stats[...]
    means = every[:, 0, :]
    mean = jnp.sum(means, axis=0, keepdims=True) / group
    off = means - mean
    second = jnp.sum(every[:, 1, :] + cw * off * off, axis=0, keepdims=True)
    inverse = lax.rsqrt(second / channels + 1e-05)
    comb[0:1, :] = mean
    comb[1:2, :] = inverse

    def conv_out(seq, carry):
        row = pl.ds(pl.multiple_of(seq * tok, tok), tok)
        flat = comb[0:2, row]
        cols = jnp.concatenate([flat, jnp.zeros((cw - 2, tok), f32)], axis=0).T
        normed = (conv[row, :] - cols[:, 0:1]) * cols[:, 1:2] * cg_ref[:, lanes(mine, cw)]
        actbuf[row, lanes(f, cw)] = (normed * jax.nn.sigmoid(normed)).astype(bf16)
        return carry

    def act_block(at):
        return actbuf.at[:, lanes(at, cw)]

    relay(3, 2)
    lax.fori_loop(0, nf, conv_out, 0)
    for p in peers:
        start(remote(act_block(f), act_block(f), cr, (z, p, c)))

    def values_in(seq, carry):
        vb[pl.ds(pl.multiple_of(seq * tok, tok), tok), :] = project(seq, 3 * cw, cw)
        return carry

    relay(3, 3)
    lax.fori_loop(0, nf, values_in, 0)

    spread_m = (
        lax.broadcasted_iota(jnp.int32, (kw, vw), 0) // DK
        == lax.broadcasted_iota(jnp.int32, (kw, vw), 1) // DV
    ).astype(bf16)
    own_mask = (
        lax.broadcasted_iota(jnp.int32, (vw, kw), 1) // DK
        == lax.broadcasted_iota(jnp.int32, (vw, kw), 0) // DV
    )
    place = lax.rem(lax.broadcasted_iota(jnp.int32, (CHUNK, kw), 0), SUB)
    per_seq = tok // CHUNK

    def attend(n, carry):
        at = pl.ds(pl.multiple_of(n * CHUNK, CHUNK), CHUNK)
        qk = qkb[at, :].astype(f32)
        q = qk[:, :kw] * DK ** (-0.5)
        k = qk[:, kw:]
        v = vb[at, :].astype(f32)
        cum = ld[at, :]
        step = 1
        while step < SUB:
            cum = cum + jnp.where(place >= step, pltpu.roll(cum, step, 0), 0.0)
            step *= 2
        acc = jnp.dot((q * k).astype(bf16), spread_m, preferred_element_type=f32) * v
        for lag in range(1, SUB):
            decays = jnp.exp(jnp.where(place >= lag, cum - pltpu.roll(cum, lag, 0), -jnp.inf))
            term = (q * pltpu.roll(k, lag, 0) * decays).astype(bf16)
            score = jnp.dot(term, spread_m, preferred_element_type=f32)
            acc = acc + score * pltpu.roll(v, lag, 0)
        q_f = q * jnp.exp(cum)
        q_in = q_f.astype(bf16)
        v_low = v.astype(bf16)
        first = lax.rem(n, per_seq) == 0
        state = jnp.where(first, 0.0, state_ref[...])
        base = jnp.where(first, 0.0, base_ref[0:1, :])
        outer, seg = [], []
        for m in range(CHUNK // SUB):
            part = slice(m * SUB, (m + 1) * SUB)
            last = cum[(m + 1) * SUB - 1 : (m + 1) * SUB]
            k_out = (k[part] * jnp.exp(last - cum[part])).astype(bf16)
            outer.append(
                lax.dot_general(
                    q_in[part], state.astype(bf16), (((1,), (1,)), ((), ())),
                    preferred_element_type=f32,
                )
            )
            added = lax.dot_general(
                v_low[part], k_out, (((0,), (0,)), ((), ())), preferred_element_type=f32
            )
            seg.append(q_f[part] * jnp.exp(base))
            state = state * jnp.exp(last) + jnp.where(own_mask, added, 0.0)
            base = base + last
        state_ref[...] = state
        base_ref[...] = jnp.broadcast_to(base, base_ref.shape)
        sfin[n // per_seq] = state
        tots[n // per_seq] = jnp.broadcast_to(base, base_ref.shape)
        raw[at, :] = acc + jnp.concatenate(outer, axis=0)
        qseg[at, :] = jnp.concatenate(seg, axis=0).astype(bf16)

        @pl.when(n == 1)
        def _():
            relay(4, 1)

        return carry

    lax.fori_loop(0, total // CHUNK, attend, 0)
    vh = vw // 2
    for p in range(nf // 2):
        a, b = sfin[2 * p], sfin[2 * p + 1]
        stbuf[z, p] = jnp.concatenate([a[:vh] + a[vh:], b[:vh] + b[vh:]], axis=1).astype(bf16)
        totbuf[z, p : p + 1, :] = jnp.concatenate(
            [tots[2 * p][0:1], tots[2 * p + 1][0:1]], axis=1
        )

    def state_out(d):
        dev = (z + d, f, c)
        return (
            remote(stbuf.at[z], stbuf.at[z], vr.at[0, z], dev),
            remote(totbuf.at[z], totbuf.at[z], vr.at[1, z], dev),
        )

    for d in range(1, nz):
        @pl.when(z + d < nz)
        def _():
            for copy in state_out(d):
                copy.start()

    relay(4, 2)
    own(6)
    own(7)
    relay(5, 1)
    relay(4, 3)

    sin_ref[...] = jnp.zeros_like(sin_ref)
    for b in range(nz - 1):
        @pl.when(z > b)
        def _():
            arrived(stbuf.at[b], vr.at[0, b])
            arrived(totbuf.at[b], vr.at[1, b])
            passed = jnp.exp(totbuf[b])
            for p in range(nf // 2):
                sin_ref[p] = sin_ref[p] * passed[p : p + 1, :] + stbuf[b, p].astype(f32)
    head_mean = jnp.where(
        lax.broadcasted_iota(jnp.int32, (vw, vw), 0) // DV
        == lax.broadcasted_iota(jnp.int32, (vw, vw), 1) // DV,
        1.0 / DV,
        0.0,
    ).astype(f32)
    gain = jnp.concatenate([hg_ref[...]] * (vw // DV), axis=1)
    for seq in range(nf):
        row = slice(seq * tok, (seq + 1) * tok)
        lo = (seq % 2) * kw
        packed = sin_ref[seq // 2][:, lo : lo + kw]
        state = jnp.where(own_mask, jnp.concatenate([packed, packed], axis=0), 0.0).astype(bf16)
        full = raw[row, :] + lax.dot_general(
            qseg[row, :], state, (((1,), (1,)), ((), ())), preferred_element_type=f32
        )
        mean = jnp.dot(
            full * full, head_mean, preferred_element_type=f32, precision=lax.Precision.HIGHEST
        )
        gate = project(seq, 4 * cw, cw).astype(f32)
        actbuf[row, lanes(nf + f, cw)] = (
            full * lax.rsqrt(mean + 1e-06) * gain * (gate * jax.nn.sigmoid(gate))
        ).astype(bf16)
    for p in peers:
        start(remote(act_block(nf + f), act_block(nf + f), gr, (z, p, c)))
    relay(5, 2)

    near = jnp.where(z < nz // 2, z, nz - 1 - z)
    out_rows = pw.shape[0]
    per_core = nz // nc

    def block_of(k):
        o = (near, 1 - near, 2, 3)[k]
        return jnp.where(z < nz // 2, o, nz - 1 - o)

    def rows_of(p):
        return pl.ds(pl.multiple_of(p * tok, tok), tok)

    def turn(j):
        return jnp.where(j == 0, dg, jnp.where(j == 1, xn, jnp.where(j == 2, yn, f)))

    def over_part(k, slot, p, lo, width, n):
        at = pl.ds(lo, width)
        return remote(
            pbuf.at[k, rows_of(p), at], prcv.at[slot, rows_of(p), at],
            pr.at[n, slot, p], (z, f, other),
        )

    def landing(slot, source, lo, width):
        first = pl.multiple_of((slot * nf + source) * out_rows + lo, width)
        return o_hbm.at[:, pl.ds(first, width)]

    def out_copy(slot, p, lo, width, n):
        return remote(
            osum.at[slot, rows_of(p), pl.ds(lo, width)], landing(slot, f, lo, width),
            orc.at[n, slot], (z, p, c),
        )

    def out_own(slot, lo, width, n):
        return pltpu.make_async_copy(
            osum.at[slot, rows_of(f), pl.ds(lo, width)], landing(slot, f, lo, width),
            o_out.at[n, slot],
        )

    def block(k, lo, width, n):
        b = block_of(k)
        slot = lax.rem(b, per_core)
        owner = b // per_core
        at = pl.ds(lo, width)

        def multiply(j, carry):
            p = turn(j)
            out = lax.dot_general(
                actbuf[rows_of(p), :], wobuf[b, lo : lo + width, :], (((1,), (1,)), ((), ())),
                preferred_element_type=f32,
            )
            pbuf[k, rows_of(p), at] = out.astype(bf16)

            @pl.when(owner != c)
            def _():
                over_part(k, slot, p, lo, width, n).start()

            return carry

        if width < out_rows:
            pbuf[k, :, at] = lax.dot_general(
                actbuf[...], wobuf[b, lo : lo + width, :], (((1,), (1,)), ((), ())),
                preferred_element_type=f32,
            ).astype(bf16)

            @pl.when(owner != c)
            def _():
                for p in (dg, xn, yn, f):
                    over_part(k, slot, p, lo, width, n).start()
        else:
            lax.fori_loop(0, nf, multiply, 0)

        def gather(j, carry):
            p = turn(j)
            arrived(prcv.at[slot, rows_of(p), at], pr.at[n, slot, p])
            osum[slot, rows_of(p), at] = (
                pbuf[k, rows_of(p), at].astype(f32) + prcv[slot, rows_of(p), at].astype(f32)
            ).astype(bf16)

            @pl.when(j < nf - 1)
            def _():
                out_copy(slot, p, lo, width, n).start()

            return carry

        @pl.when(owner == c)
        def _():
            lax.fori_loop(0, nf, gather, 0)
            out_own(slot, lo, width, n).start()

    def block_end(k, lo, width, n):
        b = block_of(k)
        slot = lax.rem(b, per_core)

        @pl.when(b // per_core != c)
        def _():
            for p in range(nf):
                over_part(k, slot, p, lo, width, n).wait_send()

        @pl.when(b // per_core == c)
        def _():
            arrived(o_hbm.at[:, pl.ds(0, (nf - 1) * width)], orc.at[n, slot])
            out_own(slot, lo, width, n).wait()
            for p in peers:
                out_copy(slot, p, lo, width, n).wait_send()

    def acts():
        arrived(actbuf.at[:, pl.ds(0, (nf - 1) * cw)], cr)
        arrived(actbuf.at[:, pl.ds(nf * cw, (nf - 1) * cw)], gr)

    ends = (z == 0) | (z == nz - 1)
    halves = [(0, half_rows, 0), (half_rows, half_rows, 1)]
    whole = (0, out_rows, 0)

    @pl.when(ends)
    def _():
        relay(5, 3)
        acts()
        block(0, *whole)
        for k in range(1, nz):
            relay(6, k)
            if k == nz - 1:
                block(k, *halves[0])
            relay(7, k)
            block(k, *(halves[1] if k == nz - 1 else whole))
        for k in range(nz - 1):
            block_end(k, *whole)
        for part in halves:
            block_end(nz - 1, *part)

    @pl.when(jnp.logical_not(ends))
    def _():
        for k in range(1, nz):
            relay(6, k)
            relay(7, k)
        acts()
        for k in range(nz):
            block(k, *whole)
        for k in range(nz):
            block_end(k, *whole)

    for copy in sends:
        copy.wait_send()
    for i in range(items):
        for b in range(nz):
            @pl.when((z < nz - 1) & (z >= b))
            def _():
                up(i, b).wait_send()

            @pl.when((z > 0) & (z <= b))
            def _():
                down(i, b).wait_send()

    @pl.when(z < nz - 1)
    def _():
        halo_out.wait_send()

    for d in range(1, nz):
        @pl.when(z + d < nz)
        def _():
            for copy in state_out(d):
                copy.wait_send()


def by_segments(
    inputs, norm_gain, conv_in_a, conv_in_b, query_w, key_w, value_w, out_gate_w,
    pointwise_w, gla_out_w, forget_first_factor, decay_w, decay_bias, decay_extra,
    conv_kernel, conv_gain, head_gain,
):
    f32, bf16 = jnp.float32, jnp.bfloat16
    nz, nf, nc = lax.axis_size("sp"), lax.axis_size("fs"), lax.axis_size("tp")
    x = inputs[0]
    tok, feat = x.shape
    total = nf * tok
    rows_w = conv_in_a.shape[0]
    kin = nz * nf * rows_w
    cw = conv_in_a.shape[1] // nf
    kw = query_w.shape[1] // nf
    vw = value_w.shape[1] // nf
    pwc = pointwise_w.shape[1]
    out_rows = pointwise_w.shape[0]
    group = nf * nc
    dma = pltpu.SemaphoreType.DMA
    items = ROOT + OUT_ITEMS
    any_spec = pl.BlockSpec(memory_space=pl.ANY)
    V = pltpu.VMEM
    flat = (
        norm_gain[None], forget_first_factor.T, decay_w, decay_bias[None],
        conv_kernel, conv_gain[None], head_gain[None],
    )
    scratch = [V(a.shape, a.dtype) for a in flat] + [
        V((total, nc * feat), bf16), V((total, nc * feat), bf16), V((total, 128), f32),
        V((kin, ROOT * cw), bf16), V((rows_w, nf * kw), bf16), V((rows_w, nf * kw), bf16),
        V((nf, rows_w, cw), bf16), V((nz, out_rows, 2 * pwc), bf16),
        V((nf, tok, 2 * kw), f32), V((nf, tok + 32, cw), f32), V((nf, 32, cw), bf16), V((nf, 32, cw), bf16), V((total, cw), f32),
        V((group, 8, total), f32), V((8, total), f32), V((total, 2 * nf * cw), bf16),
        V((total, cw), bf16), V((total, vw), bf16), V((total, kw), f32), V((total, vw), f32),
        V((total, kw), bf16), V((vw, kw), f32), V((8, kw), f32), V((nf, vw, kw), f32),
        V((nf, 8, kw), f32), V((nz, nf // 2, vw // 2, 2 * kw), bf16),
        V((nz, nf // 2, 2 * kw), f32),
        V((nf // 2, vw // 2, 2 * kw), f32),
        V((nz, total, out_rows), bf16), V((nz // nc, total, out_rows), bf16),
        V((nz // nc, total, out_rows), bf16),
        dma, dma((2,)), dma((nf, 2)), dma((nf, 2)), dma((ROOT,)), dma((ROOT,)),
        dma((items, nz)), dma((4,)), dma, dma, dma((len(flat),)), dma((2, nz // nc)), dma,
        dma, dma((2, nz)), dma, dma, dma((2, nz // nc, nf)), dma((2, nz // nc)),
    ]
    out = pl.pallas_call(
        fused_kernel,
        out_shape=jax.ShapeDtypeStruct((tok, feat), bf16),
        in_specs=[any_spec] * 17,
        out_specs=any_spec,
        scratch_shapes=scratch,
        compiler_params=pltpu.CompilerParams(
            collective_id=0, has_side_effects=True, vmem_limit_bytes=60 * 1024 * 1024
        ),
        name="mixer",
    )(
        x, conv_in_a, conv_in_b, query_w, key_w, value_w, out_gate_w, pointwise_w, gla_out_w,
        decay_extra[0], *flat,
    )
    return (x.astype(f32) + out.astype(f32)).astype(bf16)[None]


def fits(inputs, conv_in_a, query_w, value_w):
    n_sp, n_tp, n_fs = lax.axis_size("sp"), lax.axis_size("tp"), lax.axis_size("fs")
    widths = (conv_in_a.shape[1], 2 * query_w.shape[1], value_w.shape[1])
    return (
        (n_sp, n_fs, n_tp) == (4, 4, 2)
        and inputs.shape[0] == 1
        and inputs.shape[1] % CHUNK == 0
        and all(w == 128 * n_fs for w in widths)
    )


def from_behind(value, axis, by):
    length = lax.axis_size(axis)
    pairs = [(i, i + by) for i in range(length) if 0 <= i + by < length]
    return lax.ppermute(value, axis, pairs)


def by_tokens(
    inputs,
    norm_gain,
    conv_in_a,
    conv_in_b,
    query_w,
    key_w,
    value_w,
    out_gate_w,
    pointwise_w,
    gla_out_w,
    forget_first_factor,
    decay_w,
    decay_bias,
    decay_extra,
    conv_kernel,
    conv_gain,
    head_gain,
):
    collected = (
        lax.all_gather(conv_in_a, ("sp", "fs"), axis=0, tiled=True),
        lax.all_gather(conv_in_b, ("sp", "fs"), axis=0, tiled=True),
        lax.all_gather(query_w, ("sp", "fs"), axis=0, tiled=True),
        lax.all_gather(key_w, ("sp", "fs"), axis=0, tiled=True),
        lax.all_gather(value_w, ("sp", "fs"), axis=0, tiled=True),
        lax.all_gather(out_gate_w, ("sp", "fs"), axis=0, tiled=True),
        lax.all_gather(pointwise_w, ("sp", "fs"), axis=0, tiled=True),
        lax.all_gather(gla_out_w, ("sp", "fs"), axis=0, tiled=True),
    )
    (
        conv_a_full,
        conv_b_full,
        query_full,
        key_full,
        value_full,
        gate_full,
        pointwise_full,
        gla_out_full,
    ) = collected
    tok_rows = inputs[0]
    token_count = tok_rows.shape[0]
    in_weights = (
        conv_a_full,
        conv_b_full,
        query_full,
        key_full,
        value_full,
        gate_full,
        forget_first_factor,
    )
    segment_values = lax.all_gather(tok_rows, "tp", axis=1, tiled=True).astype(jnp.float32)
    scaled = (segment_values * norm_gain).astype(jnp.bfloat16)
    sums = tuple(
        (jnp.dot(scaled, weight, preferred_element_type=jnp.float32) for weight in in_weights)
    )
    sums, squares = (sums, jnp.sum(segment_values * segment_values, axis=1))
    row_scale = lax.rsqrt(squares / norm_gain.shape[0] + 1e-06)[:, None]
    conv_a, conv_b, queries, keys, values, out_gate, low_rank = [
        (running * row_scale).astype(jnp.bfloat16) for running in sums
    ]
    gated = (conv_a.astype(jnp.float32) * jax.nn.sigmoid(conv_b.astype(jnp.float32))).astype(
        jnp.bfloat16
    )
    reach = conv_kernel.shape[0] - 1
    earlier = from_behind(gated[token_count - reach :], "sp", 1)
    extended = jnp.concatenate([earlier, gated], axis=0).astype(jnp.float32)
    tp_index = lax.axis_index("tp")
    channels = gated.shape[1]
    kernel = lax.dynamic_slice_in_dim(conv_kernel, tp_index * channels, channels, 1)
    convolved = jnp.zeros((token_count, channels), jnp.float32)
    for offset in range(reach + 1):
        convolved = convolved + kernel[offset] * extended[offset : offset + token_count]
    channel_sum, channel_squares = lax.psum(
        (jnp.sum(convolved, axis=1), jnp.sum(convolved * convolved, axis=1)), "tp"
    )
    total_channels = conv_gain.shape[0]
    average = channel_sum / total_channels
    spread_squared_mean = channel_squares / total_channels - average * average
    gain_part = lax.dynamic_slice_in_dim(conv_gain, tp_index * channels, channels)
    normed = (
        (convolved - average[:, None]) * lax.rsqrt(spread_squared_mean + 1e-05)[:, None] * gain_part
    )
    conv_act = jax.nn.silu(normed).astype(jnp.bfloat16)
    key_width = keys.shape[1]
    head_count = key_width // DK
    decay_part = lax.dynamic_slice_in_dim(decay_w, tp_index * key_width, key_width, 1)
    bias_part = lax.dynamic_slice_in_dim(decay_bias, tp_index * key_width, key_width)
    pre_decay = jnp.dot(low_rank, decay_part, preferred_element_type=jnp.float32) + bias_part
    log_decay = jax.nn.log_sigmoid(pre_decay) / 16.0 + decay_extra[0]
    block_count = token_count // BLOCK
    highest = lax.Precision.HIGHEST

    def split_blocks(array_operand, width):
        return array_operand.reshape(block_count, BLOCK, head_count, width).transpose(0, 2, 1, 3)

    q_blocks = split_blocks(queries.astype(jnp.float32), DK) * DK ** (-0.5)
    k_blocks = split_blocks(keys.astype(jnp.float32), DK)
    v_blocks = split_blocks(values.astype(jnp.float32), DV)
    prefix_running_sum = jnp.cumsum(split_blocks(log_decay, DK), axis=2)
    causal = jnp.tril(jnp.ones((BLOCK, BLOCK), dtype=bool))
    spread = prefix_running_sum[:, :, :, None, :] - prefix_running_sum[:, :, None, :, :]
    weights_in = jnp.exp(jnp.where(causal[:, :, None], spread, -jnp.inf))
    scores = jnp.einsum("nhid,nhjd,nhijd->nhij", q_blocks, k_blocks, weights_in, precision=highest)
    inner = jnp.einsum("nhij,nhjv->nhiv", scores, v_blocks, precision=highest)
    block_total = prefix_running_sum[:, :, -1]
    block_state = jnp.einsum(
        "nhjd,nhjv->nhdv",
        k_blocks * jnp.exp(block_total[:, :, None] - prefix_running_sum),
        v_blocks,
        precision=highest,
    )

    def advance(state, block_pair):
        decay_row, added_share_term = block_pair
        return (jnp.exp(decay_row)[..., None] * state + added_share_term, state)

    local_final, local_entering = lax.scan(
        advance, jnp.zeros((head_count, DK, DV), jnp.float32), (block_total, block_state)
    )
    device_total = jnp.sum(block_total, axis=0)
    totals = lax.all_gather(device_total[None], "sp", axis=0, tiled=True)
    running_totals = jnp.cumsum(totals, axis=0)
    sp_index = lax.axis_index("sp")
    before = lax.dynamic_index_in_dim(
        running_totals, sp_index, 0, False
    ) - lax.dynamic_index_in_dim(totals, sp_index, 0, False)
    piece = lax.all_gather(local_final[None], "sp", axis=0, tiled=True)
    number = piece.shape[0]
    anchor = jnp.arange(number, dtype=jnp.int32)
    exponent = jnp.where(
        (anchor < sp_index)[:, None, None], before[None] - running_totals, -jnp.inf
    )
    entering = jnp.einsum("nhd,nhdv->hdv", jnp.exp(exponent), piece, precision=highest)
    passed = jnp.exp(jnp.cumsum(block_total, axis=0) - block_total)
    entering_blocks = passed[..., None] * entering[None] + local_entering
    outer = jnp.einsum(
        "nhid,nhdv->nhiv",
        q_blocks * jnp.exp(prefix_running_sum),
        entering_blocks,
        precision=highest,
    )
    head_output = inner + outer
    normed_heads = (
        head_output
        * lax.rsqrt(jnp.mean(head_output * head_output, axis=-1, keepdims=True) + 1e-06)
        * head_gain
    )
    gla_rows = normed_heads.transpose(0, 2, 1, 3).reshape(token_count, head_count * DV)
    gla_act = (gla_rows * jax.nn.silu(out_gate.astype(jnp.float32))).astype(jnp.bfloat16)
    contract = (((1,), (1,)), ((), ()))
    conv_term = lax.dot_general(
        pointwise_full, conv_act, contract, preferred_element_type=jnp.float32
    )
    summed = lax.psum_scatter(
        (
            conv_term
            + lax.dot_general(gla_out_full, gla_act, contract, preferred_element_type=jnp.float32)
        ).astype(jnp.bfloat16),
        "tp",
        scatter_dimension=0,
        tiled=True,
    ).astype(jnp.float32)
    return (tok_rows.astype(jnp.float32) + summed.T).astype(jnp.bfloat16)[None]


def shards(*args):
    if fits(args[0], args[2], args[4], args[6]):
        return by_segments(*args)
    return by_tokens(*args)


def solution(mesh):
    by_rows = P(("sp", "fs"), "tp")
    return jax.shard_map(
        shards,
        mesh=mesh,
        in_specs=(P("fs", "sp", "tp"), P())
        + (by_rows,) * 8
        + (P(), P(), P(), P("fs", "sp", "tp"), P(), P(), P()),
        out_specs=P("fs", "sp", "tp"),
        check_vma=False,
    )
```

```python
import jax
import jax.numpy as jnp
from jax import lax
from jax.experimental import pallas as pl
from jax.experimental.pallas import tpu as pltpu
from jax.sharding import PartitionSpec as P


DK = 32
DV = 64
SUB = 16
BLOCK = 64


ROOT = 5
OUT_ITEMS = 3
CHUNK = 128
MESH_IDS = pl.DeviceIdType.MESH


def fused_kernel(
    x_hbm, wa, wb, wq, wk, wv, wg, pw, go, dex_hbm,
    ng_hbm, ff_hbm, dw_hbm, db_hbm, ck_hbm, cg_hbm, hg_hbm,
    o_hbm,
    ng_ref, ff_ref, dw_ref, db_ref, ck_ref, cg_ref, hg_ref,
    xbuf, xs, rs, wbuf, qraw, kraw, qkst, wobuf, debuf, ext, hsend, hrecv, conv, stats, comb, actbuf,
    qkb, vb, ld, raw, qseg, state_ref, base_ref, sfin, tots, stbuf, totbuf, sin_ref,
    pbuf, prcv, osum,
    sent, xl, xi, xd, al, ar, zr, ol, dl, dr, pl_in, o_out, hr, tr, vr, cr, gr, pr, orc,
):
    f32, bf16 = jnp.float32, jnp.bfloat16
    z, f, c = lax.axis_index("sp"), lax.axis_index("fs"), lax.axis_index("tp")
    nz, nf, nc = lax.axis_size("sp"), lax.axis_size("fs"), lax.axis_size("tp")
    tok, feat = x_hbm.shape
    half = tok // 2
    rows_w = wa.shape[0]
    layer_rows = nf * rows_w
    cw = wa.shape[1] // nf
    kw = wq.shape[1] // nf
    vw = wv.shape[1] // nf
    total = nf * tok
    kin = wbuf.shape[0]
    pwc = pw.shape[1]
    half_rows = pw.shape[0] // 2
    channels = nc * nf * cw
    other = 1 - c
    xn = f + 1 - 2 * lax.rem(f, 2)
    yn = f + 2 - 4 * (f // 2)
    dg = nf - 1 - f
    peers = (xn, yn, dg)

    def remote(src, dst, recv, dev):
        return pltpu.make_async_remote_copy(
            src_ref=src, dst_ref=dst, send_sem=sent, recv_sem=recv,
            device_id=dev, device_id_type=MESH_IDS,
        )

    def arrived(dst, recv):
        remote(dst, dst, recv, (z, f, other)).wait_recv()

    def lanes(at, width):
        return pl.ds(pl.multiple_of(at * width, width), width)

    def xr(seq, h):
        row = pl.ds(pl.multiple_of(seq * tok + h * half, half), half)
        return xbuf.at[row, lanes(c, feat)]

    def xr_other(seq):
        row = pl.ds(pl.multiple_of(seq * tok, tok), tok)
        return xbuf.at[row, lanes(other, feat)]

    def item(i, b):
        if i < ROOT:
            row = pl.ds(pl.multiple_of(b * layer_rows, layer_rows), layer_rows)
            return wbuf.at[row, pl.ds(i * cw, cw)]
        if i == ROOT:
            return wobuf.at[b, :, pl.ds(0, pwc)]
        part = pl.ds((i - ROOT - 1) * half_rows, half_rows)
        return wobuf.at[b, part, pl.ds(pwc, pwc)]

    def up(i, b):
        return remote(item(i, b), item(i, b), zr.at[i, b], (z + 1, f, c))

    def down(i, b):
        return remote(item(i, b), item(i, b), zr.at[i, b], (z - 1, f, c))

    items = ROOT + OUT_ITEMS
    sources = {0: wa, 1: wb, 3: wv, 4: wg}
    my_rows = pl.ds(pl.multiple_of((z * nf + f) * rows_w, rows_w), rows_w)

    barrier = pltpu.get_barrier_semaphore()
    me = f * nc + c
    group = nf * nc
    for k in range(1, group):
        t = lax.rem(me + k, group)
        pl.semaphore_signal(barrier, inc=1, device_id=(z, t // nc, lax.rem(t, nc)), device_id_type=MESH_IDS)

    @pl.when(z > 0)
    def _():
        pl.semaphore_signal(barrier, inc=1, device_id=(z - 1, f, c), device_id_type=MESH_IDS)

    @pl.when(z < nz - 1)
    def _():
        pl.semaphore_signal(barrier, inc=1, device_id=(z + 1, f, c), device_id_type=MESH_IDS)

    params = [
        pltpu.make_async_copy(src, dst, pl_in.at[n])
        for n, (src, dst) in enumerate(
            (
                (ng_hbm, ng_ref), (ff_hbm, ff_ref), (dw_hbm, dw_ref), (db_hbm, db_ref),
                (ck_hbm, ck_ref), (cg_hbm, cg_ref), (hg_hbm, hg_ref),
            )
        )
    ]

    own_x = [
        pltpu.make_async_copy(x_hbm.at[pl.ds(h * half, half), :], xr(f, h), xl.at[h])
        for h in range(2)
    ]
    qk_load = [
        pltpu.make_async_copy(wq, qraw, ol.at[2]),
        pltpu.make_async_copy(wk, kraw, ol.at[3]),
    ]
    own_w = {
        g: pltpu.make_async_copy(
            w.at[:, lanes(f, cw)], wbuf.at[my_rows, pl.ds(g * cw, cw)], al.at[g]
        )
        for g, w in sources.items()
    }
    own_o = [
        pltpu.make_async_copy(pw, item(ROOT, z), ol.at[0]),
        pltpu.make_async_copy(go, wobuf.at[z, :, pl.ds(pwc, pwc)], ol.at[1]),
    ]
    own_d = pltpu.make_async_copy(dex_hbm.at[:, lanes(f // 2, 2 * kw)], debuf.at[f], dl)
    for copy in qk_load:
        copy.start()
    for g in sources:
        own_w[g].start()
    for copy in own_x + own_o + [own_d] + params:
        copy.start()

    for copy in qk_load:
        copy.wait()
    for j in range(nf):
        qkst[j] = jnp.concatenate(
            [qraw[:, j * kw : (j + 1) * kw], kraw[:, j * kw : (j + 1) * kw]], axis=1
        )
    wbuf[my_rows, pl.ds(2 * cw, cw)] = qkst[f]
    beside = jnp.where((z == 0) | (z == nz - 1), 1, 2)
    pl.semaphore_wait(barrier, group - 1 + beside)

    def exchange(g):
        out = []
        for p in peers:
            src = qkst.at[p] if g == 2 else sources[g].at[:, lanes(p, cw)]
            dst = wbuf.at[my_rows, pl.ds(g * cw, cw)]
            out.append(remote(src, dst, ar.at[g], (z, p, c)))
        return out

    x_to_x = [
        remote(x_hbm.at[pl.ds(h * half, half), :], xr(f, h), xi.at[f, h], (z, xn, c))
        for h in range(2)
    ]
    x_to_y = [
        remote(x_hbm.at[pl.ds(h * half, half), :], xr(f, h), xi.at[f, h], (z, yn, c))
        for h in range(2)
    ]
    x_over = [
        remote(x_hbm.at[pl.ds(h * half, half), :], xr(f, h), xd.at[f], (z, f, other))
        for h in range(2)
    ]

    def over(seq, h):
        return remote(xr(seq, h), xr(seq, h), xd.at[seq], (z, f, other))

    decay_out = [
        remote(
            dex_hbm.at[:, lanes(p // 2, 2 * kw)], debuf.at[f], dr, (z, p, c)
        )
        for p in peers
    ]

    sends = []

    def start(*copies):
        for copy in copies:
            copy.start()
            sends.append(copy)


    def own(i):
        if i < ROOT:
            if i in own_w:
                own_w[i].wait()
            arrived(wbuf.at[pl.ds(0, (nf - 1) * rows_w), pl.ds(i * cw, cw)], ar.at[i])
        else:
            if i - ROOT < len(own_o):
                own_o[i - ROOT].wait()

        @pl.when(z < nz - 1)
        def _():
            up(i, z).start()

        @pl.when(z > 0)
        def _():
            down(i, z).start()

    def relay(i, d):
        @pl.when(z >= d)
        def _():
            arrived(item(i, z - d), zr.at[i, z - d])

            @pl.when(z < nz - 1)
            def _():
                up(i, z - d).start()

        @pl.when(z + d < nz)
        def _():
            arrived(item(i, z + d), zr.at[i, z + d])

            @pl.when(z > 0)
            def _():
                down(i, z + d).start()

    start(*exchange(0))
    own(5)
    start(*exchange(1))
    start(*exchange(2))
    start(x_to_x[0], x_to_y[1], *x_over)
    own(0)
    start(x_to_x[1], x_to_y[0])
    start(*exchange(3))
    own(1)
    relay(0, 1)
    own(2)

    arrived(xr(xn, 0), xi.at[xn, 0])
    start(
        remote(xr(xn, 0), xr(xn, 0), xi.at[xn, 0], (z, yn, c)),
        over(xn, 0),
    )
    arrived(xr(yn, 1), xi.at[yn, 1])
    start(
        remote(xr(yn, 1), xr(yn, 1), xi.at[yn, 1], (z, xn, c)),
        over(yn, 1),
    )
    start(*exchange(4))
    start(*decay_out)
    relay(0, 2)
    relay(1, 1)

    step_rows = 32

    def scale(seq):
        def body(r, carry):
            row = pl.ds(pl.multiple_of(seq * tok + r * step_rows, step_rows), step_rows)
            value = xbuf[row, :].astype(f32)
            square = jnp.sum(value * value, axis=1, keepdims=True)
            rs[row, :] = jnp.broadcast_to(
                lax.rsqrt(square / (nc * feat) + 1e-06), (step_rows, rs.shape[1])
            )
            xs[row, :] = (value * ng_ref[...]).astype(bf16)
            return carry

        lax.fori_loop(0, tok // step_rows, body, 0)

    for copy in own_x + params:
        copy.wait()
    arrived(xr_other(f), xd.at[f])
    scale(f)
    arrived(xr(xn, 1), xi.at[xn, 1])
    arrived(xr(yn, 0), xi.at[yn, 0])
    start(over(xn, 1), over(yn, 0))
    relay(1, 2)
    own(3)
    for p in (xn, yn):
        arrived(xr_other(p), xd.at[p])
        scale(p)
    relay(0, 3)
    relay(1, 3)
    relay(2, 1)
    arrived(xr(dg, 0), xi.at[dg, 0])
    arrived(xr(dg, 1), xi.at[dg, 1])
    start(over(dg, 0), over(dg, 1))
    arrived(xr_other(dg), xd.at[dg])
    scale(dg)

    def project(seq, first, width):
        row = pl.ds(pl.multiple_of(seq * tok, tok), tok)
        out = jnp.dot(
            xs[row, :], wbuf[:, first : first + width], preferred_element_type=f32
        )
        return (out * rs[row, 0:1]).astype(bf16)

    halo = 32
    taps = ck_ref.shape[0]

    def conv_in(seq, carry):
        both = project(seq, 0, 2 * cw).astype(f32)
        gated = both[:, :cw] * jax.nn.sigmoid(both[:, cw:])
        low = gated.astype(bf16)
        ext[seq, halo : halo + tok, :] = low.astype(f32)
        hsend[seq] = low[tok - halo :]
        return carry

    lax.fori_loop(0, nf, conv_in, 0)
    halo_out = remote(hsend, hrecv, hr, (z + 1, f, c))

    @pl.when(z < nz - 1)
    def _():
        halo_out.start()

    relay(2, 2)
    own(4)

    part = c * (nf // 2) + f // 2
    odd = lax.rem(f, 2) == 1
    dw2 = dw_ref[:, lanes(part, 2 * kw)].astype(f32)
    dw_own = jnp.where(odd, dw2[:, kw:], dw2[:, :kw]).astype(bf16)
    db2 = db_ref[:, lanes(part, 2 * kw)]
    db_own = jnp.where(odd, db2[:, kw:], db2[:, :kw])
    own_d.wait()
    arrived(debuf.at[pl.ds(0, nf - 1)], dr)

    def decay(seq, carry):
        row = pl.ds(pl.multiple_of(seq * tok, tok), tok)
        low = lax.dot_general(
            xs[row, :], ff_ref[...], (((1,), (1,)), ((), ())), preferred_element_type=f32
        )
        low = (low * rs[row, 0:1]).astype(bf16)
        pre = jnp.dot(low, dw_own, preferred_element_type=f32) + db_own
        extra = debuf[seq]
        extra = jnp.where(odd, extra[:, kw:], extra[:, :kw])
        ld[row, :] = jax.nn.log_sigmoid(pre) / 16.0 + extra
        return carry

    lax.fori_loop(0, nf, decay, 0)
    relay(2, 3)

    def keys_in(seq, carry):
        qkb[pl.ds(pl.multiple_of(seq * tok, tok), tok), :] = project(seq, 2 * cw, cw)
        return carry

    lax.fori_loop(0, nf, keys_in, 0)

    @pl.when(z > 0)
    def _():
        arrived(hrecv, hr)
        ext[:, 0:halo, :] = hrecv[...].astype(f32)

    @pl.when(z == 0)
    def _():
        ext[:, 0:halo, :] = jnp.zeros((nf, halo, cw), f32)

    mine = c * nf + f
    tap_rows = 64
    lane = lax.broadcasted_iota(jnp.int32, (tok, cw), 1)

    def tap(seq, carry):
        kernel = ck_ref[:, lanes(mine, cw)]
        for r in range(tok // tap_rows):
            acc = jnp.zeros((tap_rows, cw), f32)
            for j in range(taps):
                at = halo - (taps - 1) + j + r * tap_rows
                acc = acc + kernel[j : j + 1, :] * ext[seq, at : at + tap_rows, :]
            conv[pl.ds(pl.multiple_of(seq * tok + r * tap_rows, tap_rows), tap_rows), :] = acc
        row = pl.ds(pl.multiple_of(seq * tok, tok), tok)
        value = conv[row, :]
        mean = jnp.sum(value, axis=1, keepdims=True) / cw
        spread = value - mean
        second = jnp.sum(spread * spread, axis=1, keepdims=True)
        both = jnp.where(lane == 0, mean, jnp.where(lane == 1, second, 0.0))
        stats[me, :, pl.ds(pl.multiple_of(seq * tok, tok), tok)] = both.T[0:8, :]
        return carry

    lax.fori_loop(0, nf, tap, 0)
    relay(3, 1)
    for k in range(1, group):
        t = lax.rem(me + k, group)
        start(
            remote(
                stats.at[me], stats.at[me], tr, (z, t // nc, lax.rem(t, nc))
            )
        )
    arrived(stats.at[pl.ds(0, group - 1)], tr)
    every = stats[...]
    means = every[:, 0, :]
    mean = jnp.sum(means, axis=0, keepdims=True) / group
    off = means - mean
    second = jnp.sum(every[:, 1, :] + cw * off * off, axis=0, keepdims=True)
    inverse = lax.rsqrt(second / channels + 1e-05)
    comb[0:1, :] = mean
    comb[1:2, :] = inverse

    def conv_out(seq, carry):
        row = pl.ds(pl.multiple_of(seq * tok, tok), tok)
        flat = comb[0:2, row]
        cols = jnp.concatenate([flat, jnp.zeros((cw - 2, tok), f32)], axis=0).T
        normed = (conv[row, :] - cols[:, 0:1]) * cols[:, 1:2] * cg_ref[:, lanes(mine, cw)]
        actbuf[row, lanes(f, cw)] = (normed * jax.nn.sigmoid(normed)).astype(bf16)
        return carry

    def act_block(at):
        return actbuf.at[:, lanes(at, cw)]

    relay(3, 2)
    lax.fori_loop(0, nf, conv_out, 0)
    for p in peers:
        start(remote(act_block(f), act_block(f), cr, (z, p, c)))

    def values_in(seq, carry):
        vb[pl.ds(pl.multiple_of(seq * tok, tok), tok), :] = project(seq, 3 * cw, cw)
        return carry

    relay(3, 3)
    lax.fori_loop(0, nf, values_in, 0)

    spread_m = (
        lax.broadcasted_iota(jnp.int32, (kw, vw), 0) // DK
        == lax.broadcasted_iota(jnp.int32, (kw, vw), 1) // DV
    ).astype(bf16)
    own_mask = (
        lax.broadcasted_iota(jnp.int32, (vw, kw), 1) // DK
        == lax.broadcasted_iota(jnp.int32, (vw, kw), 0) // DV
    )
    place = lax.rem(lax.broadcasted_iota(jnp.int32, (CHUNK, kw), 0), SUB)
    per_seq = tok // CHUNK

    def attend(n, carry):
        at = pl.ds(pl.multiple_of(n * CHUNK, CHUNK), CHUNK)
        qk = qkb[at, :].astype(f32)
        q = qk[:, :kw] * DK ** (-0.5)
        k = qk[:, kw:]
        v = vb[at, :].astype(f32)
        cum = ld[at, :]
        step = 1
        while step < SUB:
            cum = cum + jnp.where(place >= step, pltpu.roll(cum, step, 0), 0.0)
            step *= 2
        acc = jnp.dot((q * k).astype(bf16), spread_m, preferred_element_type=f32) * v
        for lag in range(1, SUB):
            decays = jnp.exp(jnp.where(place >= lag, cum - pltpu.roll(cum, lag, 0), -jnp.inf))
            term = (q * pltpu.roll(k, lag, 0) * decays).astype(bf16)
            score = jnp.dot(term, spread_m, preferred_element_type=f32)
            acc = acc + score * pltpu.roll(v, lag, 0)
        q_f = q * jnp.exp(cum)
        q_in = q_f.astype(bf16)
        v_low = v.astype(bf16)
        first = lax.rem(n, per_seq) == 0
        state = jnp.where(first, 0.0, state_ref[...])
        base = jnp.where(first, 0.0, base_ref[0:1, :])
        outer, seg = [], []
        for m in range(CHUNK // SUB):
            part = slice(m * SUB, (m + 1) * SUB)
            last = cum[(m + 1) * SUB - 1 : (m + 1) * SUB]
            k_out = (k[part] * jnp.exp(last - cum[part])).astype(bf16)
            outer.append(
                lax.dot_general(
                    q_in[part], state.astype(bf16), (((1,), (1,)), ((), ())),
                    preferred_element_type=f32,
                )
            )
            added = lax.dot_general(
                v_low[part], k_out, (((0,), (0,)), ((), ())), preferred_element_type=f32
            )
            seg.append(q_f[part] * jnp.exp(base))
            state = state * jnp.exp(last) + jnp.where(own_mask, added, 0.0)
            base = base + last
        state_ref[...] = state
        base_ref[...] = jnp.broadcast_to(base, base_ref.shape)
        sfin[n // per_seq] = state
        tots[n // per_seq] = jnp.broadcast_to(base, base_ref.shape)
        raw[at, :] = acc + jnp.concatenate(outer, axis=0)
        qseg[at, :] = jnp.concatenate(seg, axis=0).astype(bf16)

        @pl.when(n == 1)
        def _():
            relay(4, 1)

        return carry

    lax.fori_loop(0, total // CHUNK, attend, 0)
    vh = vw // 2
    for p in range(nf // 2):
        a, b = sfin[2 * p], sfin[2 * p + 1]
        stbuf[z, p] = jnp.concatenate([a[:vh] + a[vh:], b[:vh] + b[vh:]], axis=1).astype(bf16)
        totbuf[z, p : p + 1, :] = jnp.concatenate(
            [tots[2 * p][0:1], tots[2 * p + 1][0:1]], axis=1
        )

    def state_out(d):
        dev = (z + d, f, c)
        return (
            remote(stbuf.at[z], stbuf.at[z], vr.at[0, z], dev),
            remote(totbuf.at[z], totbuf.at[z], vr.at[1, z], dev),
        )

    for d in range(1, nz):
        @pl.when(z + d < nz)
        def _():
            for copy in state_out(d):
                copy.start()

    relay(4, 2)
    own(6)
    own(7)
    relay(5, 1)
    relay(4, 3)

    sin_ref[...] = jnp.zeros_like(sin_ref)
    for b in range(nz - 1):
        @pl.when(z > b)
        def _():
            arrived(stbuf.at[b], vr.at[0, b])
            arrived(totbuf.at[b], vr.at[1, b])
            passed = jnp.exp(totbuf[b])
            for p in range(nf // 2):
                sin_ref[p] = sin_ref[p] * passed[p : p + 1, :] + stbuf[b, p].astype(f32)
    head_mean = jnp.where(
        lax.broadcasted_iota(jnp.int32, (vw, vw), 0) // DV
        == lax.broadcasted_iota(jnp.int32, (vw, vw), 1) // DV,
        1.0 / DV,
        0.0,
    ).astype(f32)
    gain = jnp.concatenate([hg_ref[...]] * (vw // DV), axis=1)
    for seq in range(nf):
        row = slice(seq * tok, (seq + 1) * tok)
        lo = (seq % 2) * kw
        packed = sin_ref[seq // 2][:, lo : lo + kw]
        state = jnp.where(own_mask, jnp.concatenate([packed, packed], axis=0), 0.0).astype(bf16)
        full = raw[row, :] + lax.dot_general(
            qseg[row, :], state, (((1,), (1,)), ((), ())), preferred_element_type=f32
        )
        mean = jnp.dot(
            full * full, head_mean, preferred_element_type=f32, precision=lax.Precision.HIGHEST
        )
        gate = project(seq, 4 * cw, cw).astype(f32)
        actbuf[row, lanes(nf + f, cw)] = (
            full * lax.rsqrt(mean + 1e-06) * gain * (gate * jax.nn.sigmoid(gate))
        ).astype(bf16)
    for p in peers:
        start(remote(act_block(nf + f), act_block(nf + f), gr, (z, p, c)))
    relay(5, 2)

    near = jnp.where(z < nz // 2, z, nz - 1 - z)
    out_rows = pw.shape[0]
    per_core = nz // nc

    def block_of(k):
        o = (near, 1 - near, 2, 3)[k]
        return jnp.where(z < nz // 2, o, nz - 1 - o)

    def rows_of(p):
        return pl.ds(pl.multiple_of(p * tok, tok), tok)

    def turn(j):
        return jnp.where(j == 0, dg, jnp.where(j == 1, yn, jnp.where(j == 2, xn, f)))

    def over_part(k, slot, p, lo, width, n):
        at = pl.ds(lo, width)
        return remote(
            pbuf.at[k, rows_of(p), at], prcv.at[slot, rows_of(p), at],
            pr.at[n, slot, p], (z, f, other),
        )

    def landing(slot, source, lo, width):
        first = pl.multiple_of((slot * nf + source) * out_rows + lo, width)
        return o_hbm.at[:, pl.ds(first, width)]

    def out_copy(slot, p, lo, width, n):
        return remote(
            osum.at[slot, rows_of(p), pl.ds(lo, width)], landing(slot, f, lo, width),
            orc.at[n, slot], (z, p, c),
        )

    def out_own(slot, lo, width, n):
        return pltpu.make_async_copy(
            osum.at[slot, rows_of(f), pl.ds(lo, width)], landing(slot, f, lo, width),
            o_out.at[n, slot],
        )

    def block(k, lo, width, n):
        b = block_of(k)
        slot = lax.rem(b, per_core)
        owner = b // per_core
        at = pl.ds(lo, width)

        def multiply(j, carry):
            p = turn(j)
            out = lax.dot_general(
                actbuf[rows_of(p), :], wobuf[b, lo : lo + width, :], (((1,), (1,)), ((), ())),
                preferred_element_type=f32,
            )
            pbuf[k, rows_of(p), at] = out.astype(bf16)

            @pl.when(owner != c)
            def _():
                over_part(k, slot, p, lo, width, n).start()

            return carry

        if width < out_rows:
            pbuf[k, :, at] = lax.dot_general(
                actbuf[...], wobuf[b, lo : lo + width, :], (((1,), (1,)), ((), ())),
                preferred_element_type=f32,
            ).astype(bf16)

            @pl.when(owner != c)
            def _():
                for p in (dg, yn, xn, f):
                    over_part(k, slot, p, lo, width, n).start()
        else:
            lax.fori_loop(0, nf, multiply, 0)

        def gather(j, carry):
            p = turn(j)
            arrived(prcv.at[slot, rows_of(p), at], pr.at[n, slot, p])
            osum[slot, rows_of(p), at] = (
                pbuf[k, rows_of(p), at].astype(f32) + prcv[slot, rows_of(p), at].astype(f32)
            ).astype(bf16)

            @pl.when(j < nf - 1)
            def _():
                out_copy(slot, p, lo, width, n).start()

            return carry

        @pl.when(owner == c)
        def _():
            lax.fori_loop(0, nf, gather, 0)
            out_own(slot, lo, width, n).start()

    def block_end(k, lo, width, n):
        b = block_of(k)
        slot = lax.rem(b, per_core)

        @pl.when(b // per_core != c)
        def _():
            for p in range(nf):
                over_part(k, slot, p, lo, width, n).wait_send()

        @pl.when(b // per_core == c)
        def _():
            arrived(o_hbm.at[:, pl.ds(0, (nf - 1) * width)], orc.at[n, slot])
            out_own(slot, lo, width, n).wait()
            for p in peers:
                out_copy(slot, p, lo, width, n).wait_send()

    def acts():
        arrived(actbuf.at[:, pl.ds(0, (nf - 1) * cw)], cr)
        arrived(actbuf.at[:, pl.ds(nf * cw, (nf - 1) * cw)], gr)

    ends = (z == 0) | (z == nz - 1)
    halves = [(0, half_rows, 0), (half_rows, half_rows, 1)]
    whole = (0, out_rows, 0)

    @pl.when(ends)
    def _():
        relay(5, 3)
        acts()
        block(0, *whole)
        for k in range(1, nz):
            relay(6, k)
            if k == nz - 1:
                block(k, *halves[0])
            relay(7, k)
            block(k, *(halves[1] if k == nz - 1 else whole))

    @pl.when(jnp.logical_not(ends))
    def _():
        for k in range(1, nz):
            relay(6, k)
            relay(7, k)
        acts()
        for k in range(nz):
            block(k, *whole)

    for copy in sends:
        copy.wait_send()
    for i in range(items):
        for b in range(nz):
            @pl.when((z < nz - 1) & (z >= b))
            def _():
                up(i, b).wait_send()

            @pl.when((z > 0) & (z <= b))
            def _():
                down(i, b).wait_send()

    @pl.when(z < nz - 1)
    def _():
        halo_out.wait_send()

    for d in range(1, nz):
        @pl.when(z + d < nz)
        def _():
            for copy in state_out(d):
                copy.wait_send()

    @pl.when(ends)
    def _():
        for k in range(nz - 1):
            block_end(k, *whole)
        for part in halves:
            block_end(nz - 1, *part)

    @pl.when(jnp.logical_not(ends))
    def _():
        for k in range(nz):
            block_end(k, *whole)


def by_segments(
    inputs, norm_gain, conv_in_a, conv_in_b, query_w, key_w, value_w, out_gate_w,
    pointwise_w, gla_out_w, forget_first_factor, decay_w, decay_bias, decay_extra,
    conv_kernel, conv_gain, head_gain,
):
    f32, bf16 = jnp.float32, jnp.bfloat16
    nz, nf, nc = lax.axis_size("sp"), lax.axis_size("fs"), lax.axis_size("tp")
    x = inputs[0]
    tok, feat = x.shape
    total = nf * tok
    rows_w = conv_in_a.shape[0]
    kin = nz * nf * rows_w
    cw = conv_in_a.shape[1] // nf
    kw = query_w.shape[1] // nf
    vw = value_w.shape[1] // nf
    pwc = pointwise_w.shape[1]
    out_rows = pointwise_w.shape[0]
    group = nf * nc
    dma = pltpu.SemaphoreType.DMA
    items = ROOT + OUT_ITEMS
    any_spec = pl.BlockSpec(memory_space=pl.ANY)
    V = pltpu.VMEM
    flat = (
        norm_gain[None], forget_first_factor.T, decay_w, decay_bias[None],
        conv_kernel, conv_gain[None], head_gain[None],
    )
    scratch = [V(a.shape, a.dtype) for a in flat] + [
        V((total, nc * feat), bf16), V((total, nc * feat), bf16), V((total, 128), f32),
        V((kin, ROOT * cw), bf16), V((rows_w, nf * kw), bf16), V((rows_w, nf * kw), bf16),
        V((nf, rows_w, cw), bf16), V((nz, out_rows, 2 * pwc), bf16),
        V((nf, tok, 2 * kw), f32), V((nf, tok + 32, cw), f32), V((nf, 32, cw), bf16), V((nf, 32, cw), bf16), V((total, cw), f32),
        V((group, 8, total), f32), V((8, total), f32), V((total, 2 * nf * cw), bf16),
        V((total, cw), bf16), V((total, vw), bf16), V((total, kw), f32), V((total, vw), f32),
        V((total, kw), bf16), V((vw, kw), f32), V((8, kw), f32), V((nf, vw, kw), f32),
        V((nf, 8, kw), f32), V((nz, nf // 2, vw // 2, 2 * kw), bf16),
        V((nz, nf // 2, 2 * kw), f32),
        V((nf // 2, vw // 2, 2 * kw), f32),
        V((nz, total, out_rows), bf16), V((nz // nc, total, out_rows), bf16),
        V((nz // nc, total, out_rows), bf16),
        dma, dma((2,)), dma((nf, 2)), dma((nf,)), dma((ROOT,)), dma((ROOT,)),
        dma((items, nz)), dma((4,)), dma, dma, dma((len(flat),)), dma((2, nz // nc)), dma,
        dma, dma((2, nz)), dma, dma, dma((2, nz // nc, nf)), dma((2, nz // nc)),
    ]
    out = pl.pallas_call(
        fused_kernel,
        out_shape=jax.ShapeDtypeStruct((tok, feat), bf16),
        in_specs=[any_spec] * 17,
        out_specs=any_spec,
        scratch_shapes=scratch,
        compiler_params=pltpu.CompilerParams(
            collective_id=0, has_side_effects=True, vmem_limit_bytes=60 * 1024 * 1024
        ),
        name="mixer",
    )(
        x, conv_in_a, conv_in_b, query_w, key_w, value_w, out_gate_w, pointwise_w, gla_out_w,
        decay_extra[0], *flat,
    )
    return (x.astype(f32) + out.astype(f32)).astype(bf16)[None]


def fits(inputs, conv_in_a, query_w, value_w):
    n_sp, n_tp, n_fs = lax.axis_size("sp"), lax.axis_size("tp"), lax.axis_size("fs")
    widths = (conv_in_a.shape[1], 2 * query_w.shape[1], value_w.shape[1])
    return (
        (n_sp, n_fs, n_tp) == (4, 4, 2)
        and inputs.shape[0] == 1
        and inputs.shape[1] % CHUNK == 0
        and all(w == 128 * n_fs for w in widths)
    )


def from_behind(value, axis, by):
    length = lax.axis_size(axis)
    pairs = [(i, i + by) for i in range(length) if 0 <= i + by < length]
    return lax.ppermute(value, axis, pairs)


def by_tokens(
    inputs,
    norm_gain,
    conv_in_a,
    conv_in_b,
    query_w,
    key_w,
    value_w,
    out_gate_w,
    pointwise_w,
    gla_out_w,
    forget_first_factor,
    decay_w,
    decay_bias,
    decay_extra,
    conv_kernel,
    conv_gain,
    head_gain,
):
    collected = (
        lax.all_gather(conv_in_a, ("sp", "fs"), axis=0, tiled=True),
        lax.all_gather(conv_in_b, ("sp", "fs"), axis=0, tiled=True),
        lax.all_gather(query_w, ("sp", "fs"), axis=0, tiled=True),
        lax.all_gather(key_w, ("sp", "fs"), axis=0, tiled=True),
        lax.all_gather(value_w, ("sp", "fs"), axis=0, tiled=True),
        lax.all_gather(out_gate_w, ("sp", "fs"), axis=0, tiled=True),
        lax.all_gather(pointwise_w, ("sp", "fs"), axis=0, tiled=True),
        lax.all_gather(gla_out_w, ("sp", "fs"), axis=0, tiled=True),
    )
    (
        conv_a_full,
        conv_b_full,
        query_full,
        key_full,
        value_full,
        gate_full,
        pointwise_full,
        gla_out_full,
    ) = collected
    tok_rows = inputs[0]
    token_count = tok_rows.shape[0]
    in_weights = (
        conv_a_full,
        conv_b_full,
        query_full,
        key_full,
        value_full,
        gate_full,
        forget_first_factor,
    )
    segment_values = lax.all_gather(tok_rows, "tp", axis=1, tiled=True).astype(jnp.float32)
    scaled = (segment_values * norm_gain).astype(jnp.bfloat16)
    sums = tuple(
        (jnp.dot(scaled, weight, preferred_element_type=jnp.float32) for weight in in_weights)
    )
    sums, squares = (sums, jnp.sum(segment_values * segment_values, axis=1))
    row_scale = lax.rsqrt(squares / norm_gain.shape[0] + 1e-06)[:, None]
    conv_a, conv_b, queries, keys, values, out_gate, low_rank = [
        (running * row_scale).astype(jnp.bfloat16) for running in sums
    ]
    gated = (conv_a.astype(jnp.float32) * jax.nn.sigmoid(conv_b.astype(jnp.float32))).astype(
        jnp.bfloat16
    )
    reach = conv_kernel.shape[0] - 1
    earlier = from_behind(gated[token_count - reach :], "sp", 1)
    extended = jnp.concatenate([earlier, gated], axis=0).astype(jnp.float32)
    tp_index = lax.axis_index("tp")
    channels = gated.shape[1]
    kernel = lax.dynamic_slice_in_dim(conv_kernel, tp_index * channels, channels, 1)
    convolved = jnp.zeros((token_count, channels), jnp.float32)
    for offset in range(reach + 1):
        convolved = convolved + kernel[offset] * extended[offset : offset + token_count]
    channel_sum, channel_squares = lax.psum(
        (jnp.sum(convolved, axis=1), jnp.sum(convolved * convolved, axis=1)), "tp"
    )
    total_channels = conv_gain.shape[0]
    average = channel_sum / total_channels
    spread_squared_mean = channel_squares / total_channels - average * average
    gain_part = lax.dynamic_slice_in_dim(conv_gain, tp_index * channels, channels)
    normed = (
        (convolved - average[:, None]) * lax.rsqrt(spread_squared_mean + 1e-05)[:, None] * gain_part
    )
    conv_act = jax.nn.silu(normed).astype(jnp.bfloat16)
    key_width = keys.shape[1]
    head_count = key_width // DK
    decay_part = lax.dynamic_slice_in_dim(decay_w, tp_index * key_width, key_width, 1)
    bias_part = lax.dynamic_slice_in_dim(decay_bias, tp_index * key_width, key_width)
    pre_decay = jnp.dot(low_rank, decay_part, preferred_element_type=jnp.float32) + bias_part
    log_decay = jax.nn.log_sigmoid(pre_decay) / 16.0 + decay_extra[0]
    block_count = token_count // BLOCK
    highest = lax.Precision.HIGHEST

    def split_blocks(array_operand, width):
        return array_operand.reshape(block_count, BLOCK, head_count, width).transpose(0, 2, 1, 3)

    q_blocks = split_blocks(queries.astype(jnp.float32), DK) * DK ** (-0.5)
    k_blocks = split_blocks(keys.astype(jnp.float32), DK)
    v_blocks = split_blocks(values.astype(jnp.float32), DV)
    prefix_running_sum = jnp.cumsum(split_blocks(log_decay, DK), axis=2)
    causal = jnp.tril(jnp.ones((BLOCK, BLOCK), dtype=bool))
    spread = prefix_running_sum[:, :, :, None, :] - prefix_running_sum[:, :, None, :, :]
    weights_in = jnp.exp(jnp.where(causal[:, :, None], spread, -jnp.inf))
    scores = jnp.einsum("nhid,nhjd,nhijd->nhij", q_blocks, k_blocks, weights_in, precision=highest)
    inner = jnp.einsum("nhij,nhjv->nhiv", scores, v_blocks, precision=highest)
    block_total = prefix_running_sum[:, :, -1]
    block_state = jnp.einsum(
        "nhjd,nhjv->nhdv",
        k_blocks * jnp.exp(block_total[:, :, None] - prefix_running_sum),
        v_blocks,
        precision=highest,
    )

    def advance(state, block_pair):
        decay_row, added_share_term = block_pair
        return (jnp.exp(decay_row)[..., None] * state + added_share_term, state)

    local_final, local_entering = lax.scan(
        advance, jnp.zeros((head_count, DK, DV), jnp.float32), (block_total, block_state)
    )
    device_total = jnp.sum(block_total, axis=0)
    totals = lax.all_gather(device_total[None], "sp", axis=0, tiled=True)
    running_totals = jnp.cumsum(totals, axis=0)
    sp_index = lax.axis_index("sp")
    before = lax.dynamic_index_in_dim(
        running_totals, sp_index, 0, False
    ) - lax.dynamic_index_in_dim(totals, sp_index, 0, False)
    piece = lax.all_gather(local_final[None], "sp", axis=0, tiled=True)
    number = piece.shape[0]
    anchor = jnp.arange(number, dtype=jnp.int32)
    exponent = jnp.where(
        (anchor < sp_index)[:, None, None], before[None] - running_totals, -jnp.inf
    )
    entering = jnp.einsum("nhd,nhdv->hdv", jnp.exp(exponent), piece, precision=highest)
    passed = jnp.exp(jnp.cumsum(block_total, axis=0) - block_total)
    entering_blocks = passed[..., None] * entering[None] + local_entering
    outer = jnp.einsum(
        "nhid,nhdv->nhiv",
        q_blocks * jnp.exp(prefix_running_sum),
        entering_blocks,
        precision=highest,
    )
    head_output = inner + outer
    normed_heads = (
        head_output
        * lax.rsqrt(jnp.mean(head_output * head_output, axis=-1, keepdims=True) + 1e-06)
        * head_gain
    )
    gla_rows = normed_heads.transpose(0, 2, 1, 3).reshape(token_count, head_count * DV)
    gla_act = (gla_rows * jax.nn.silu(out_gate.astype(jnp.float32))).astype(jnp.bfloat16)
    contract = (((1,), (1,)), ((), ()))
    conv_term = lax.dot_general(
        pointwise_full, conv_act, contract, preferred_element_type=jnp.float32
    )
    summed = lax.psum_scatter(
        (
            conv_term
            + lax.dot_general(gla_out_full, gla_act, contract, preferred_element_type=jnp.float32)
        ).astype(jnp.bfloat16),
        "tp",
        scatter_dimension=0,
        tiled=True,
    ).astype(jnp.float32)
    return (tok_rows.astype(jnp.float32) + summed.T).astype(jnp.bfloat16)[None]


def shards(*args):
    if fits(args[0], args[2], args[4], args[6]):
        return by_segments(*args)
    return by_tokens(*args)


def solution(mesh):
    by_rows = P(("sp", "fs"), "tp")
    return jax.shard_map(
        shards,
        mesh=mesh,
        in_specs=(P("fs", "sp", "tp"), P())
        + (by_rows,) * 8
        + (P(), P(), P(), P("fs", "sp", "tp"), P(), P(), P()),
        out_specs=P("fs", "sp", "tp"),
        check_vma=False,
    )
```
